32 devices in a mesh: kv: 8 (over z, y), tp: 4 (over x, core).
Axes of the slice: x: 2, y: 2, z: 4, core: 2. Of those that a mesh axis runs over, the one named last changes fastest.
Arguments:
- tokens: bfloat16 [16, 16, 4096], replicated, may hold values from -6 to 6
- gain_pre: float32 [4096], replicated, may hold values from 0.1 to 1.9
- w_query: bfloat16 [4096, 2048], P('kv', 'tp'), may hold values from -0.09375 to 0.09375
- w_key: bfloat16 [4096, 2048], P('kv', 'tp'), may hold values from -0.09375 to 0.09375
- w_value: bfloat16 [4096, 2048], P('kv', 'tp'), may hold values from -0.09375 to 0.09375
- w_forget: bfloat16 [4096, 16], replicated, may hold values from -0.09375 to 0.09375
- b_forget: float32 [16], replicated
- w_out: bfloat16 [2048, 4096], P('tp', 'kv'), may hold values from -0.125 to 0.125
- gain_post: float32 [4096], P(('kv', 'tp')), may hold values from 0.1 to 1.9
- key_cache: bfloat16 [16, 1024, 16, 128], P(None, 'kv', 'tp'), may hold values from -6 to 6
- value_cache: bfloat16 [16, 1024, 16, 128], P(None, 'kv', 'tp'), may hold values from -6 to 6
- cum_cache: float32 [16, 1024, 16], P(None, 'kv', 'tp'), may hold values from -402 to 0, as said below
- lengths: int32 [16], replicated, may hold values from 512 to 992
- accepted: int32 [16], replicated, may hold values from 0 to 16
- parent: int32 [16, 16], replicated, may hold values from -1 to 14, as said below
Outputs:
- mixed: bfloat16 [16, 16, 4096], P(None, None, ('kv', 'tp'))
- key_out: bfloat16 [16, 1024, 16, 128], P(None, 'kv', 'tp')
- value_out: bfloat16 [16, 1024, 16, 128], P(None, 'kv', 'tp')
- cum_out: float32 [16, 1024, 16], P(None, 'kv', 'tp')
The draws below stay inside these ranges and needn't reach their ends.
Inputs may be any that keep to these rules, and one draw needn't show every extreme that they name: parent[s, 0] is -1 and parent[s, i] lies between -1 and i - 1. `cum_cache`: along the positions of each sequence and head the values never rise. lengths + accepted + 16 never exceeds 1024.
All inputs are finite; a program needn't handle non-finite values.
Results may differ from the reference program's by a relative error of at most 0.03.
Values may be sent and summed in bfloat16 or wider, within the bound.
A program may use at most 64 MiB of HBM per device.

```python
import jax
import jax.numpy as jnp
from jax import lax

D = 4096
HEADS = 16
HD = 128
PROP = 16
SEQS = 16
POS_DEV = 128
HW = 2048
CACHE_LEN = 1024
SHARDS = 8
GROUPS = 4


def fast_heads(key):
    share = 0.5
    return jax.random.bernoulli(jax.random.fold_in(key, 11), share, (HEADS,))


def draw_b_forget(key, part):
    fast = fast_heads(key)
    spread = jax.random.uniform(jax.random.fold_in(key, 12), (HEADS,), jnp.float32)
    return jnp.where(fast, 0.5 + 1.5 * spread, 2.5 + 1.5 * spread).astype(jnp.float32)


def draw_cum_cache(key, part):
    fast = fast_heads(key)
    slow_rate = jax.random.uniform(jax.random.fold_in(key, 21), (SEQS, HEADS), jnp.float32, 0.3, 1.2) / CACHE_LEN
    fast_rate = 1.0 / jax.random.uniform(jax.random.fold_in(key, 22), (SEQS, HEADS), jnp.float32, 40.0, 100.0)
    rates = jnp.where(fast[None, :], fast_rate, slow_rate)
    factor_pos = jnp.exp(jax.random.uniform(jax.random.fold_in(key, 23), (SEQS, CACHE_LEN, HEADS), jnp.float32, jnp.log(0.6), jnp.log(1.6)))
    factor_block = jnp.exp(jax.random.uniform(jax.random.fold_in(key, 24), (SEQS, CACHE_LEN // POS_DEV, HEADS), jnp.float32, jnp.log(0.5), jnp.log(2.0)))
    factor_block = jnp.repeat(factor_block, POS_DEV, axis=1)
    decrements = -rates[:, None, :] * factor_pos * factor_block
    offsets = jax.random.uniform(jax.random.fold_in(key, 25), (SEQS, 1, HEADS), jnp.float32, -300.0, 0.0)
    return (offsets + jnp.cumsum(decrements, axis=1)).astype(jnp.float32)


def draw_parent(key, part):
    limits = jnp.arange(PROP, dtype=jnp.int32)[None, :]
    return jax.random.randint(key, (SEQS, PROP), -1, limits, dtype=jnp.int32)


def place_ends(entries, stream_key, least, largest):
    longest = entries.shape.index(max(entries.shape))
    spots = []
    for shift in (0, 1):
        where = [jax.random.randint(jax.random.fold_in(stream_key, axis), (), 0, length) for axis, length in enumerate(entries.shape)]
        where[longest] = (where[longest] + shift) % entries.shape[longest]
        spots.append(tuple(where))
    return entries.at[spots[0]].set(least).at[spots[1]].set(largest)


def shard_levels(key, extent, split, low, largest):
    def one(position, blocks):
        draws = jax.random.uniform(jax.random.fold_in(jax.random.fold_in(key, 6), position), (blocks,), jnp.float32, low / len(split), largest / len(split))
        return jnp.repeat(jnp.exp(draws), extent[position] // blocks).reshape((-1,) + (1,) * (len(extent) - position - 1))

    factor_of = one(*split[0])
    for cut in split[1:]:
        factor_of = factor_of * one(*cut)
    return factor_of


def normal_values(key, shape, width, most, split=(), kind=jnp.bfloat16):
    gain = shard_levels(key, shape, split, -0.22, 0.18) if split else 1.0
    drawn = jax.random.normal(key, shape, jnp.float32) * width * gain
    return jnp.minimum(jnp.maximum(drawn, -most), most).astype(kind)


def setup_inputs(seed: int = 0) -> dict:
    key_of = jax.random.split(jax.random.key(seed), 16)
    tokens = normal_values(key_of[0], (SEQS, PROP, D), 1.0, 6.0)
    gain_pre = jnp.clip(1.0 + 0.18 * jax.random.normal(key_of[1], (D,), jnp.float32), 0.1, 1.9)
    w_query = normal_values(key_of[2], (D, HW), D ** -0.5, 0.09375, ((0, 8), (1, 4)))
    w_key = normal_values(key_of[3], (D, HW), D ** -0.5, 0.09375, ((0, 8), (1, 4)))
    w_value = normal_values(key_of[4], (D, HW), D ** -0.5, 0.09375, ((0, 8), (1, 4)))
    w_forget = normal_values(key_of[5], (D, HEADS), D ** -0.5, 0.09375)
    b_forget = draw_b_forget(jax.random.fold_in(key_of[15], 71), 0)
    w_out = normal_values(key_of[7], (HW, D), HW ** -0.5, 0.125, ((0, 4), (1, 8)))
    gain_post = jnp.clip(1.0 + 0.18 * jax.random.normal(key_of[8], (D,), jnp.float32), 0.1, 1.9)
    key_cache = normal_values(key_of[9], (SEQS, CACHE_LEN, HEADS, HD), 1.0, 6.0, ((1, 8), (2, 4)))
    value_cache = normal_values(key_of[10], (SEQS, CACHE_LEN, HEADS, HD), 1.0, 6.0, ((1, 8), (2, 4)))
    cum_cache = draw_cum_cache(jax.random.fold_in(key_of[15], 71), 0)
    lengths = place_ends(jax.random.randint(key_of[12], (SEQS,), CACHE_LEN // 2, CACHE_LEN - 2 * PROP + 1), jax.random.fold_in(key_of[12], 1), CACHE_LEN // 2, CACHE_LEN - 2 * PROP).astype(jnp.int32)
    accepted = place_ends(jax.random.randint(key_of[13], (SEQS,), 0, PROP + 1), jax.random.fold_in(key_of[13], 1), 0, PROP).astype(jnp.int32)
    parent = draw_parent(jax.random.fold_in(key_of[15], 71), 0)
    return {"tokens": tokens, "gain_pre": gain_pre, "w_query": w_query, "w_key": w_key, "w_value": w_value, "w_forget": w_forget, "b_forget": b_forget, "w_out": w_out, "gain_post": gain_post, "key_cache": key_cache, "value_cache": value_cache, "cum_cache": cum_cache, "lengths": lengths, "accepted": accepted, "parent": parent}


epsilon = 1e-06
floor_value = -1e+30

def ancestry(parent_ids, members):
    identity = jnp.eye(members, dtype=jnp.float32)
    parent_hot = (parent_ids[:, :, None] == jnp.arange(members, dtype=jnp.int32)[None, None, :]).astype(jnp.float32)
    ancestors = jnp.minimum(identity[None] + parent_hot, 1.0)
    for sweep in range(max(1, (members - 1).bit_length())):
        ancestors = jnp.minimum(jnp.einsum('bij,bjk->bik', ancestors, ancestors, precision=lax.Precision.HIGHEST), 1.0)
    return ancestors

def reference(tokens, gain_pre, w_query, w_key, w_value, w_forget, b_forget, w_out, gain_post, key_cache, value_cache, cum_cache, lengths, accepted, parent):
    num_seqs = tokens.shape[0]
    scale = HD ** (-0.5)
    tok_float = tokens.astype(jnp.float32)
    normed = (tok_float * lax.rsqrt(lax.optimization_barrier(jnp.mean(tok_float * tok_float, -1, keepdims=True)) + epsilon) * gain_pre.astype(jnp.float32)).astype(jnp.bfloat16)
    flat = normed.reshape(num_seqs * PROP, D)
    query = jnp.dot(flat, w_query, preferred_element_type=jnp.float32).astype(jnp.bfloat16).reshape(num_seqs, PROP, HEADS, HD)
    key_new = jnp.dot(flat, w_key, preferred_element_type=jnp.float32).astype(jnp.bfloat16).reshape(num_seqs, PROP, HEADS, HD)
    value_new = jnp.dot(flat, w_value, preferred_element_type=jnp.float32).astype(jnp.bfloat16).reshape(num_seqs, PROP, HEADS, HD)
    log_forget = jax.nn.log_sigmoid(jnp.dot(flat, w_forget, preferred_element_type=jnp.float32) + b_forget.astype(jnp.float32)).reshape(num_seqs, PROP, HEADS)
    ancestors = ancestry(parent, PROP)
    path = jnp.einsum('bij,bjh->bih', ancestors, log_forget, precision=lax.Precision.HIGHEST)
    valid = (lengths + accepted).astype(jnp.int32)
    last_index = jnp.broadcast_to((valid - 1).astype(jnp.int32)[:, None, None], (num_seqs, 1, HEADS))
    last_cum = jnp.take_along_axis(cum_cache, last_index, axis=1)[:, 0, :]
    query_float = query.astype(jnp.float32)
    key_blocks = jnp.swapaxes(key_cache.reshape(num_seqs, SHARDS, POS_DEV, HEADS, HD), 0, 1)
    value_blocks = jnp.swapaxes(value_cache.reshape(num_seqs, SHARDS, POS_DEV, HEADS, HD), 0, 1)
    cum_blocks = jnp.swapaxes(cum_cache.reshape(num_seqs, SHARDS, POS_DEV, HEADS), 0, 1)
    starts = (jnp.arange(SHARDS, dtype=jnp.int32) * POS_DEV).astype(jnp.int32)

    def add_block(carry, item):
        run_max, run_total, run_values = carry
        block_keys, block_vals, block_cum, start = item
        positions = start + jnp.arange(POS_DEV, dtype=jnp.int32)
        live = (positions[None, :] < valid[:, None])[:, None, None, :]
        score = jnp.einsum('bihd,bkhd->bihk', query_float, block_keys.astype(jnp.float32)) * scale + path[..., None] - jnp.swapaxes(block_cum, 1, 2)[:, None]
        block_max = lax.optimization_barrier(jnp.max(jnp.where(live, score, floor_value), axis=-1))
        weight = jnp.exp(jnp.where(live, score - block_max[..., None], floor_value))
        block_total = lax.optimization_barrier(jnp.sum(weight, axis=-1))
        weight_low = lax.optimization_barrier(weight.astype(jnp.bfloat16)).astype(jnp.float32)
        block_values = jnp.einsum('bihk,bkhd->bihd', weight_low, block_vals.astype(jnp.float32))
        new_max = jnp.maximum(run_max, block_max)
        old_scale = jnp.exp(run_max - new_max)
        new_scale = jnp.exp(block_max - new_max)
        return ((new_max, run_total * old_scale + block_total * new_scale, run_values * old_scale[..., None] + block_values * new_scale[..., None]), None)
    init = (jnp.full((num_seqs, PROP, HEADS), floor_value, jnp.float32), jnp.zeros((num_seqs, PROP, HEADS), jnp.float32), jnp.zeros((num_seqs, PROP, HEADS, HD), jnp.float32))
    (cache_max, cache_total, cache_values), unused = lax.scan(add_block, init, (key_blocks, value_blocks, cum_blocks, starts))
    tree_mask = (ancestors > 0.5)[:, :, None, :]
    tree_score = jnp.einsum('bihd,bjhd->bihj', query_float, key_new.astype(jnp.float32)) * scale + path[..., None] - jnp.swapaxes(path, 1, 2)[:, None]
    tree_max = lax.optimization_barrier(jnp.max(jnp.where(tree_mask, tree_score, floor_value), axis=-1))
    tree_weight = jnp.exp(jnp.where(tree_mask, tree_score - tree_max[..., None], floor_value))
    tree_total = lax.optimization_barrier(jnp.sum(tree_weight, axis=-1))
    tree_low = lax.optimization_barrier(tree_weight.astype(jnp.bfloat16)).astype(jnp.float32)
    tree_values = jnp.einsum('bihj,bjhd->bihd', tree_low, value_new.astype(jnp.float32))
    shifted = cache_max + last_cum[:, None, :]
    top = jnp.maximum(shifted, tree_max)
    cache_scale = jnp.exp(shifted - top)
    tree_scale = jnp.exp(tree_max - top)
    attended = ((cache_values * cache_scale[..., None] + tree_values * tree_scale[..., None]) / (cache_total * cache_scale + tree_total * tree_scale)[..., None]).astype(jnp.bfloat16)
    attended = attended.reshape(num_seqs * PROP, GROUPS, HW // GROUPS).astype(jnp.float32)
    group_out = jnp.einsum('tgc,gcd->gtd', attended, w_out.reshape(GROUPS, HW // GROUPS, D).astype(jnp.float32))
    group_out = lax.optimization_barrier(group_out.astype(jnp.bfloat16)).astype(jnp.float32)
    mixed_sum = lax.optimization_barrier(jnp.sum(group_out, axis=0))
    mixed = (mixed_sum * lax.rsqrt(lax.optimization_barrier(jnp.mean(mixed_sum * mixed_sum, -1, keepdims=True)) + epsilon) * gain_post.astype(jnp.float32)).astype(jnp.bfloat16).reshape(num_seqs, PROP, D)
    zero_index = jnp.zeros((), jnp.int32)

    def write_rows(cache_rows, new_rows, start):
        return lax.dynamic_update_slice(cache_rows, new_rows, (start.astype(jnp.int32), zero_index, zero_index))
    key_out = jax.vmap(write_rows)(key_cache, key_new, valid)
    value_out = jax.vmap(write_rows)(value_cache, value_new, valid)
    cum_new = last_cum[:, None, :] + path

    def write_cum(cache_rows, new_rows, start):
        return lax.dynamic_update_slice(cache_rows, new_rows, (start.astype(jnp.int32), zero_index))
    cum_out = jax.vmap(write_cum)(cum_cache, cum_new, valid)
    return (mixed, key_out, value_out, cum_out)
```

```python
import functools

import jax
import jax.numpy as jnp
from jax import lax
from jax.experimental import pallas as pl
from jax.experimental.pallas import tpu as pltpu
from jax.sharding import PartitionSpec as P

epsilon = 1e-06
floor_value = -1e30


def merged(part, axis, combine):
    gathered = jax.tree.map(lambda a: lax.all_gather(a, axis), part)

    def take(source):
        return jax.tree.map(lambda a: lax.dynamic_index_in_dim(a, source, 0, False), gathered)

    return lax.fori_loop(
        1, lax.axis_size(axis), lambda source, state: combine(state, take(source)), take(0)
    )


def ancestry(parent_ids, members):
    identity = jnp.eye(members, dtype=jnp.float32)
    parent_hot = (
        parent_ids[:, :, None] == jnp.arange(members, dtype=jnp.int32)[None, None, :]
    ).astype(jnp.float32)
    ancestors = jnp.minimum(identity[None] + parent_hot, 1.0)
    for sweep in range(max(1, (members - 1).bit_length())):
        ancestors = jnp.minimum(
            jnp.einsum("bij,bjk->bik", ancestors, ancestors, precision=lax.Precision.HIGHEST), 1.0
        )
    return ancestors


def combine_parts(first, second):
    new_max = jnp.maximum(first[0], second[0])
    first_scale = jnp.exp(first[0] - new_max)
    second_scale = jnp.exp(second[0] - new_max)
    return (
        new_max,
        first[1] * first_scale + second[1] * second_scale,
        first[2] * first_scale[..., None] + second[2] * second_scale[..., None],
        jnp.maximum(first[3], second[3]),
    )


def finish_rows(cache_max, cache_total, cache_values, last_rows, tree_max, tree_total, tree_values):
    shifted = cache_max + last_rows
    top = jnp.maximum(shifted, tree_max)
    cache_scale = jnp.exp(shifted - top)
    tree_scale = jnp.exp(tree_max - top)
    attended = (
        (cache_values * cache_scale[..., None] + tree_values * tree_scale[..., None])
        / (cache_total * cache_scale + tree_total * tree_scale)[..., None]
    ).astype(jnp.bfloat16)
    return attended.reshape(attended.shape[0], attended.shape[1] * attended.shape[2])


def per_device(
    tokens,
    gain_pre,
    w_query,
    w_key,
    w_value,
    w_forget,
    b_forget,
    w_out,
    gain_post,
    key_cache,
    value_cache,
    cum_cache,
    lengths,
    accepted,
    parent,
):
    num_seqs, proposals, model_width = tokens.shape
    kv_rank = lax.axis_index("kv")
    tp_rank = lax.axis_index("tp")
    span = key_cache.shape[1]
    heads_local = key_cache.shape[2]
    head_dim = key_cache.shape[3]
    scale = head_dim ** (-0.5)
    all_rows = num_seqs * proposals
    tok_float = tokens.astype(jnp.float32)
    normed = (
        tok_float
        * lax.rsqrt(jnp.mean(tok_float * tok_float, -1, keepdims=True) + epsilon)
        * gain_pre
    ).astype(jnp.bfloat16)
    flat = normed.reshape(all_rows, model_width)
    weight_rows = w_query.shape[0]
    local_rows = lax.dynamic_slice_in_dim(flat, kv_rank * weight_rows, weight_rows, 1)
    query_part = jnp.dot(local_rows, w_query, preferred_element_type=jnp.float32)
    key_part = jnp.dot(local_rows, w_key, preferred_element_type=jnp.float32)
    value_part = jnp.dot(local_rows, w_value, preferred_element_type=jnp.float32)
    summed = (
        lax.psum(query_part.astype(jnp.bfloat16), "kv").astype(jnp.float32),
        lax.psum(key_part.astype(jnp.bfloat16), "kv").astype(jnp.float32),
        lax.psum(value_part.astype(jnp.bfloat16), "kv").astype(jnp.float32),
    )
    query_flat = summed[0].astype(jnp.bfloat16)
    key_flat = summed[1].astype(jnp.bfloat16)
    value_flat = summed[2].astype(jnp.bfloat16)
    query = query_flat.reshape(num_seqs, proposals, heads_local, head_dim)
    key_new = key_flat.reshape(num_seqs, proposals, heads_local, head_dim)
    value_new = value_flat.reshape(num_seqs, proposals, heads_local, head_dim)
    forget_cols = lax.dynamic_slice_in_dim(w_forget, tp_rank * heads_local, heads_local, 1)
    forget_bias = lax.dynamic_slice_in_dim(b_forget, tp_rank * heads_local, heads_local, 0)
    log_forget = jax.nn.log_sigmoid(
        jnp.dot(flat, forget_cols, preferred_element_type=jnp.float32) + forget_bias
    ).reshape(num_seqs, proposals, heads_local)
    ancestors = ancestry(parent, proposals)
    path = jnp.einsum("bij,bjh->bih", ancestors, log_forget, precision=lax.Precision.HIGHEST)
    valid = lengths + accepted
    positions = kv_rank * span + jnp.arange(span, dtype=jnp.int32)
    live = (positions[None, :] < valid[:, None])[:, None, None, :]
    score = (
        jnp.einsum("bihd,bkhd->bihk", query, key_cache, preferred_element_type=jnp.float32) * scale
        + path[..., None]
        - jnp.swapaxes(cum_cache, 1, 2)[:, None]
    )
    block_max = jnp.max(jnp.where(live, score, floor_value), axis=-1)
    weight = jnp.exp(jnp.where(live, score - block_max[..., None], floor_value))
    block_total = jnp.sum(weight, axis=-1)
    block_values = jnp.einsum(
        "bihk,bkhd->bihd",
        weight.astype(jnp.bfloat16),
        value_cache,
        preferred_element_type=jnp.float32,
    )
    owner = positions[None, :] == (valid - 1)[:, None]
    candidate = jnp.max(jnp.where(owner[:, :, None], cum_cache, floor_value), axis=1)
    tree_mask = (ancestors > 0.5)[:, :, None, :]
    tree_score = (
        jnp.einsum("bihd,bjhd->bihj", query, key_new, preferred_element_type=jnp.float32) * scale
        + path[..., None]
        - jnp.swapaxes(path, 1, 2)[:, None]
    )
    tree_max = jnp.max(jnp.where(tree_mask, tree_score, floor_value), axis=-1)
    tree_weight = jnp.exp(jnp.where(tree_mask, tree_score - tree_max[..., None], floor_value))
    tree_total = jnp.sum(tree_weight, axis=-1)
    tree_values = jnp.einsum(
        "bihj,bjhd->bihd",
        tree_weight.astype(jnp.bfloat16),
        value_new,
        preferred_element_type=jnp.float32,
    )
    tree_max_rows = tree_max.reshape(all_rows, heads_local)
    tree_total_rows = tree_total.reshape(all_rows, heads_local)
    tree_values_rows = tree_values.reshape(all_rows, heads_local, head_dim)
    cache_max, cache_total, cache_values, last_cum = merged(
        (block_max, block_total, block_values, candidate), "kv", combine_parts
    )
    last_rows = jnp.broadcast_to(last_cum[:, None, :], (num_seqs, proposals, heads_local)).reshape(
        all_rows, heads_local
    )
    attended = finish_rows(
        cache_max.reshape(all_rows, heads_local),
        cache_total.reshape(all_rows, heads_local),
        cache_values.reshape(all_rows, heads_local, head_dim),
        last_rows,
        tree_max_rows,
        tree_total_rows,
        tree_values_rows,
    )
    mixed_part = jnp.dot(attended, w_out, preferred_element_type=jnp.float32)
    mixed_sum = lax.psum_scatter(
        mixed_part.astype(jnp.bfloat16), "tp", scatter_dimension=1, tiled=True
    ).astype(jnp.float32)
    squares = lax.psum(jnp.sum(mixed_sum * mixed_sum, axis=1), ("kv", "tp"))
    mixed = (mixed_sum * lax.rsqrt(squares / model_width + epsilon)[:, None] * gain_post).astype(
        jnp.bfloat16
    )
    mixed = mixed.reshape(num_seqs, proposals, mixed_sum.shape[1])
    relative = positions[None, :] - valid[:, None]
    select = relative[:, :, None] == jnp.arange(proposals, dtype=jnp.int32)[None, None, :]
    written = (relative >= 0) & (relative < proposals)
    placed_keys = jnp.einsum(
        "bkj,bjhd->bkhd", select.astype(jnp.bfloat16), key_new, preferred_element_type=jnp.float32
    ).astype(jnp.bfloat16)
    placed_values = jnp.einsum(
        "bkj,bjhd->bkhd", select.astype(jnp.bfloat16), value_new, preferred_element_type=jnp.float32
    ).astype(jnp.bfloat16)
    key_out = jnp.where(written[:, :, None, None], placed_keys, key_cache)
    value_out = jnp.where(written[:, :, None, None], placed_values, value_cache)
    cum_new = last_cum[:, None, :] + path
    placed_cum = jnp.einsum(
        "bkj,bjh->bkh", select.astype(jnp.float32), cum_new, precision=lax.Precision.HIGHEST
    )
    cum_out = jnp.where(written[:, :, None], placed_cum, cum_cache)
    return (mixed, key_out, value_out, cum_out)


MESH = pl.DeviceIdType.MESH
HI = lax.Precision.HIGHEST
F32 = jnp.float32
BF = jnp.bfloat16


def iota(shape, dim):
    return lax.broadcasted_iota(jnp.int32, shape, dim)


def hot(mask):
    return jnp.where(mask, 1.0, 0.0).astype(F32)


def dot_hi(a, b, dims=(((1,), (0,)), ((), ()))):
    return lax.dot_general(a, b, dims, precision=HI, preferred_element_type=F32)


NT = (((1,), (1,)), ((), ()))


def layer_kernel(
    n,
    nt,
    num_seqs,
    prop,
    heads,
    hd,
    span,
    tok,
    gain,
    wq,
    wk,
    wv,
    wft,
    bias,
    wo,
    gpost,
    kc,
    vc,
    cum,
    lens,
    accs,
    parent,
    mixed_out,
    k_out,
    v_out,
    cum_out,
    tokv,
    normed,
    wv3,
    wov,
    kcv,
    vcv,
    part,
    rs_recv,
    qkv,
    st_send,
    val_send,
    st_recv,
    val_recv,
    cand_send,
    cand_recv,
    brow,
    anc,
    tpath,
    ptile,
    att,
    o_send,
    o_recv,
    sq_send,
    sq_recv,
    sq2_send,
    sq2_recv,
    loc,
    ssem,
    rsem,
    tssem,
    trsem,
):
    me = lax.axis_index("kv")
    mt = lax.axis_index("tp")
    rows = num_seqs * prop
    width = tok.shape[1]
    hw = heads * hd
    kdim = wq.shape[0]
    cols = heads * span
    sp = num_seqs // n
    R = sp * prop
    hp = heads * prop
    L = sp * hp
    scale = hd ** (-0.5)
    base = me * span
    heads_all = wft.shape[0]

    barrier = pltpu.get_barrier_semaphore()

    def greet(d, c):
        pl.semaphore_signal(
            barrier, inc=1, device_id={"kv": lax.rem(me + d, n)}, device_id_type=MESH
        )
        return c

    def greet_t(d, c):
        pl.semaphore_signal(
            barrier, inc=1, device_id={"tp": lax.rem(mt + d, nt)}, device_id_type=MESH
        )
        return c

    lax.fori_loop(1, n, greet, 0)
    lax.fori_loop(1, nt, greet_t, 0)

    in_tok = pltpu.make_async_copy(tok, tokv, loc.at[0])
    in_w = [pltpu.make_async_copy(w, wv3.at[i], loc.at[1 + i]) for i, w in enumerate((wq, wk, wv))]
    in_kc = pltpu.make_async_copy(kc, kcv, loc.at[4])
    in_vc = pltpu.make_async_copy(vc, vcv, loc.at[5])
    in_wo = pltpu.make_async_copy(wo, wov, loc.at[6])
    in_tok.start()
    for c in in_w:
        c.start()
    in_kc.start()
    in_vc.start()
    in_wo.start()

    def to_kv(ph, d, src, dst, sign=1):
        peer = lax.rem(me + sign * d + n, n)
        return pltpu.make_async_remote_copy(
            src_ref=src,
            dst_ref=dst,
            send_sem=ssem.at[ph, d],
            recv_sem=rsem.at[ph, d],
            device_id={"kv": peer},
            device_id_type=MESH,
        )

    def to_tp(ph, d, src, dst):
        peer = lax.rem(mt + d, nt)
        return pltpu.make_async_remote_copy(
            src_ref=src,
            dst_ref=dst,
            send_sem=tssem.at[ph, d],
            recv_sem=trsem.at[ph, d],
            device_id={"tp": peer},
            device_id_type=MESH,
        )

    def up(d):
        return lax.rem(me + d, n)

    def down(d):
        return lax.rem(me - d + n, n)

    def rrow(i):
        return pl.ds(pl.multiple_of(i * R, R), R)

    def rs_copy(ph, d):
        return to_kv(ph, d, part.at[ph, rrow(up(d))], rs_recv.at[ph, d])

    def ag_copy(ph, d):
        return to_kv(3 + ph, d, qkv.at[ph, rrow(me)], qkv.at[ph, rrow(me)])

    def ag_wait(ph, d):
        to_kv(3 + ph, d, qkv.at[ph, rrow(me)], qkv.at[ph, rrow(down(d))]).wait_recv()

    def stat_copy(d):
        return to_kv(6, d, st_send.at[d], st_recv.at[d], -1)

    def val_copy(d):
        return to_kv(7, d, val_send.at[d], val_recv.at[d], -1)

    def cand_copy(d):
        return to_kv(8, d, cand_send, cand_recv.at[d])

    def att_copy(d):
        return to_kv(9, d, att.at[rrow(me)], att.at[rrow(me)])

    def att_wait(d):
        to_kv(9, d, att.at[rrow(me)], att.at[rrow(down(d))]).wait_recv()

    def sq_copy(d):
        return to_kv(10, d, sq_send, sq_recv.at[d])

    def each(count, fn):
        def body(d, c):
            fn(d)
            return c

        lax.fori_loop(1, count, body, 0)

    in_tok.wait()
    nb = prop

    def norm_rows(i, c):
        sl = pl.ds(pl.multiple_of(i * nb, nb), nb)
        t = tokv[sl, :].astype(F32)
        inv = lax.rsqrt(jnp.mean(t * t, axis=-1, keepdims=True) + epsilon)
        normed[sl, :] = (t * inv * gain[...]).astype(BF)
        return c

    lax.fori_loop(0, rows // nb, norm_rows, 0)
    local = normed[:, pl.ds(pl.multiple_of(me * kdim, kdim), kdim)]
    pl.semaphore_wait(barrier, n - 1 + nt - 1)
    for ph in range(3):
        in_w[ph].wait()
        part[ph] = jnp.dot(local, wv3[ph], preferred_element_type=F32).astype(BF)
        each(n, lambda d: rs_copy(ph, d).start())

    r64 = num_seqs * heads
    c64 = cum[...]
    srow = iota((r64, span), 0) // heads
    lane = iota((r64, span), 1)
    rel64 = jnp.zeros((r64, span), jnp.int32)
    rel16 = jnp.zeros((num_seqs, cols), jnp.int32)
    s16 = iota((num_seqs, cols), 0)
    for s in range(num_seqs):
        rel_s = lens[s] + accs[s] - base
        rel64 = jnp.where(srow == s, rel_s, rel64)
        rel16 = jnp.where(s16 == s, rel_s, rel16)
    cand = jnp.max(jnp.where(lane == rel64 - 1, c64, floor_value), axis=1, keepdims=True)
    diag = iota((r64, 128), 0) == iota((r64, 128), 1)
    cand_lane = jnp.sum(jnp.where(diag, cand, 0.0), axis=0, keepdims=True)
    cand_send[...] = jnp.broadcast_to(cand_lane, (8, 128))
    each(n, lambda d: cand_copy(d).start())

    spread = hot(iota((span, cols), 1) // heads == iota((span, cols), 0))
    e1 = dot_hi(c64, spread)
    e1 = jnp.where(iota((r64, cols), 0) % heads == iota((r64, cols), 1) % heads, e1, 0.0)
    take = hot(iota((num_seqs, r64), 1) // heads == iota((num_seqs, r64), 0))
    cflat = dot_hi(take, e1)
    brow[...] = jnp.where(iota((num_seqs, cols), 1) // heads < rel16, -cflat, floor_value)

    ri = iota((rows, rows), 0)
    ci = iota((rows, rows), 1)
    pick = hot(iota((rows, num_seqs), 0) // prop == iota((rows, num_seqs), 1))
    pb = dot_hi(pick, parent[...].astype(F32))
    pcol = jnp.sum(
        jnp.where(iota((rows, prop), 1) == iota((rows, prop), 0) % prop, pb, 0.0),
        axis=1,
        keepdims=True,
    )
    target = jnp.where(pcol >= 0.0, (ri // prop * prop).astype(F32) + pcol, -1.0)
    a = jnp.where((ri == ci) | (ci.astype(F32) == target), 1.0, 0.0)
    for sweep in range(max(1, (prop - 1).bit_length())):
        low = a.astype(BF)
        a = jnp.minimum(jnp.dot(low, low, preferred_element_type=F32), 1.0)
    anc[...] = a
    lf = lax.dot_general(wft[...], normed[...], NT, preferred_element_type=F32)
    bcol = jnp.zeros((heads_all, rows), F32)
    for h in range(heads_all):
        bcol = jnp.where(iota((heads_all, rows), 0) == h, bias[h], bcol)
    z = lf + bcol
    lf = jnp.minimum(z, 0.0) - jnp.log1p(jnp.exp(-jnp.abs(z)))
    path_t = dot_hi(lf, a, NT)
    rep = hot(iota((r64, heads_all), 1) == mt * heads + iota((r64, heads_all), 0) % heads)
    pm = dot_hi(rep, path_t)
    pm = jnp.where(iota((r64, rows), 1) // prop == iota((r64, rows), 0) // heads, pm, 0.0)
    fold = hot(iota((rows, 128), 0) % prop == iota((rows, 128), 1) % prop)
    pt = dot_hi(pm, fold)
    ptile[...] = pt
    ptm = jnp.where((iota((r64, 128), 1) // prop) % heads == iota((r64, 128), 0) % heads, pt, 0.0)
    tpath[...] = dot_hi(take, ptm)

    def reduce_part(ph):
        total = part[ph, rrow(me)].astype(F32)
        for d in range(1, n):
            rs_copy(ph, d).wait_recv()
            total = total + rs_recv[ph, d].astype(F32)
        qkv[ph, rrow(me)] = total.astype(BF)
        each(n, lambda d: ag_copy(ph, d).start())

    for ph in range(3):
        reduce_part(ph)

    in_kc.wait()
    in_vc.wait()
    same_head = iota((hp, cols), 0) // prop == iota((hp, cols), 1) % heads
    diag_l = iota((L, L), 0) == iota((L, L), 1)

    def heads_of(ph, s):
        block = qkv[ph, pl.ds(pl.multiple_of(s * prop, prop), prop), :]
        return jnp.concatenate([block[:, h * hd : (h + 1) * hd] for h in range(heads)], axis=0)

    def block_part(src):
        maxes, totals, values = [], [], []
        for j in range(sp):
            s = src * sp + j
            q = heads_of(0, s)
            sc = lax.dot_general(q, kcv[s], NT, preferred_element_type=F32) * scale
            sc = jnp.where(same_head, sc + brow[pl.ds(s, 1), :], floor_value)
            m = jnp.max(sc, axis=1, keepdims=True)
            w = jnp.exp(sc - m)
            maxes.append(m)
            totals.append(jnp.sum(w, axis=1, keepdims=True))
            values.append(
                jnp.dot(w.astype(BF), vcv[s], preferred_element_type=F32).astype(BF)
            )
        m = jnp.concatenate(maxes, axis=0)
        t = jnp.concatenate(totals, axis=0)
        m_lane = jnp.sum(jnp.where(diag_l, m, 0.0), axis=0, keepdims=True)
        t_lane = jnp.sum(jnp.where(diag_l, t, 0.0), axis=0, keepdims=True)
        stats = jnp.where(iota((8, L), 0) == 0, m_lane, t_lane)
        return stats, jnp.concatenate(values, axis=0)

    def remote_block(d):
        ag_wait(0, d)
        stats, values = block_part(down(d))
        st_send[d] = stats
        val_send[d] = values
        stat_copy(d).start()
        val_copy(d).start()

    each(n, remote_block)
    stats, values = block_part(me)
    st_recv[0] = stats
    val_recv[0] = values

    fold_h = iota((rows, hp), 0)
    tmax, ttot, tval = [], [], []
    for j in range(sp):
        s = me * sp + j
        q = heads_of(0, s)
        k = heads_of(1, s)
        v = heads_of(2, s)
        arows = anc[pl.ds(pl.multiple_of(s * prop, prop), prop), :]
        sel = hot(fold_h == s * prop + iota((rows, hp), 1) % prop).astype(BF)
        am = jnp.dot(arows.astype(BF), sel, preferred_element_type=F32)
        am = jnp.concatenate([am] * heads, axis=0)
        mask = (am > 0.5) & (iota((hp, hp), 0) // prop == iota((hp, hp), 1) // prop)
        sc = lax.dot_general(q, k, NT, preferred_element_type=F32) * scale
        sc = jnp.where(mask, sc - tpath[pl.ds(s, 1), 0:hp], floor_value)
        m = jnp.max(sc, axis=1, keepdims=True)
        w = jnp.where(mask, jnp.exp(sc - m), 0.0)
        tmax.append(m)
        ttot.append(jnp.sum(w, axis=1, keepdims=True))
        tval.append(jnp.dot(w.astype(BF), v, preferred_element_type=F32))
    tree_max = jnp.concatenate(tmax, axis=0)
    tree_tot = jnp.concatenate(ttot, axis=0)
    tree_val = jnp.concatenate(tval, axis=0)

    last_lane = cand_send[...]
    for d in range(1, n):
        cand_copy(d).wait_recv()
        last_lane = jnp.maximum(last_lane, cand_recv[d])
    last_col = jnp.sum(jnp.where(diag, last_lane[0:1], 0.0), axis=1, keepdims=True)
    own_rows = iota((L, 128), 0)
    own_pick = iota((L, 128), 1) == (me * sp + own_rows // hp) * heads + (own_rows % hp) // prop
    last_own = jnp.sum(jnp.where(own_pick, last_lane[0:1], 0.0), axis=1, keepdims=True)

    shifted_path = ptile[...]
    for b in range((span - 1).bit_length()):
        moved = pltpu.roll(shifted_path, 1 << b, 1)
        shifted_path = jnp.where((rel64 >> b) & 1 == 1, moved, shifted_path)
    off = lane - rel64
    cum_out[...] = jnp.where((off >= 0) & (off < prop), last_col + shifted_path, cum[...])

    for d in range(1, n):
        stat_copy(d).wait_recv()
    top = st_recv[0]
    for d in range(1, n):
        top = jnp.maximum(top, st_recv[d])
    top = top[0:1]

    def col(x):
        return jnp.sum(jnp.where(diag_l, x, 0.0), axis=1, keepdims=True)

    cache_tot = jnp.zeros((1, L), F32)
    scales = []
    for d in range(n):
        sd = jnp.exp(st_recv[d, 0:1] - top)
        scales.append(col(sd))
        cache_tot = cache_tot + st_recv[d, 1:2] * sd
    shifted = col(top) + last_own
    both = jnp.maximum(shifted, tree_max)
    cscale = jnp.exp(shifted - both)
    tscale = jnp.exp(tree_max - both)
    denom = col(cache_tot) * cscale + tree_tot * tscale
    vals = jnp.zeros((L, hd), F32)
    for d in range(n):
        if d > 0:
            val_copy(d).wait_recv()
        vals = vals + val_recv[d].astype(F32) * scales[d]
    attended = ((vals * cscale + tree_val * tscale) / denom).astype(BF)
    for j in range(sp):
        for h in range(heads):
            att[pl.ds(pl.multiple_of(me * R + j * prop, prop), prop), h * hd : (h + 1) * hd] = (
                attended[j * hp + h * prop : j * hp + (h + 1) * prop]
            )
    each(n, lambda d: att_copy(d).start())
    each(n, lambda d: ag_wait(1, d))
    each(n, lambda d: ag_wait(2, d))
    out_k = pltpu.make_async_copy(qkv.at[1], k_out, loc.at[7])
    out_v = pltpu.make_async_copy(qkv.at[2], v_out, loc.at[8])
    out_k.start()
    out_v.start()
    in_wo.wait()
    each(n, att_wait)
    full = jnp.dot(att[...], wov[...], preferred_element_type=F32).astype(BF)
    oc = o_send.shape[2]
    for t in range(nt):
        o_send[t] = full[:, t * oc : (t + 1) * oc]

    def o_copy(d):
        return to_tp(0, d, o_send.at[lax.rem(mt + d, nt)], o_recv.at[d])

    def sq2_copy(d):
        return to_tp(1, d, sq2_send, sq2_recv.at[d])

    each(nt, lambda d: o_copy(d).start())
    mixed = o_send[mt].astype(F32)
    for d in range(1, nt):
        o_copy(d).wait_recv()
        mixed = mixed + o_recv[d].astype(F32)
    sq_send[...] = dot_hi(jnp.ones((8, oc), F32), mixed * mixed, NT)
    each(n, lambda d: sq_copy(d).start())
    sq = sq_send[...]
    for d in range(1, n):
        sq_copy(d).wait_recv()
        sq = sq + sq_recv[d]
    sq2_send[...] = sq
    each(nt, lambda d: sq2_copy(d).start())
    for d in range(1, nt):
        sq2_copy(d).wait_recv()
        sq = sq + sq2_recv[d]
    ssum = dot_hi(sq, jnp.full((8, oc), 0.125, F32), (((0,), (0,)), ((), ())))
    mixed_out[...] = (mixed * lax.rsqrt(ssum / width + epsilon) * gpost[...]).astype(BF)

    def drain(d):
        for ph in range(3):
            rs_copy(ph, d).wait_send()
            ag_copy(ph, d).wait_send()
        stat_copy(d).wait_send()
        val_copy(d).wait_send()
        cand_copy(d).wait_send()
        att_copy(d).wait_send()
        sq_copy(d).wait_send()

    each(n, drain)

    def drain_t(d):
        o_copy(d).wait_send()
        sq2_copy(d).wait_send()

    each(nt, drain_t)
    out_k.wait()
    out_v.wait()


def write_kernel(num_seqs, prop, heads, hd, span, kc, vc, kn, vn, lens, accs, k_out, v_out, buf, sin, sout):
    base = lax.axis_index("kv") * span
    hp = heads * prop
    cols = heads * span
    win = hp + 16
    srcs, dsts, news = (kc, vc), (k_out, v_out), (kn, vn)
    for s in range(num_seqs):
        for i in range(2):
            pltpu.make_async_copy(srcs[i].at[s], buf.at[i, s], sin.at[i, s]).start()
    m = iota((win, hp), 1)
    diff = iota((win, hp), 0) - (m % prop * heads + m // prop)
    edge = iota((win, hd), 0)
    for s in range(num_seqs):
        first = (lens[s] + accs[s] - base) * heads
        start = pl.multiple_of(jnp.clip(first // 16 * 16, 0, cols - win), 16)
        sel = hot(diff == first - start).astype(BF)
        here = edge - (first - start)
        inside = (here >= 0) & (here < hp)
        for i in range(2):
            new = news[i][s * prop : (s + 1) * prop, :]
            new = jnp.concatenate([new[:, h * hd : (h + 1) * hd] for h in range(heads)], axis=0)
            placed = jnp.dot(sel, new, preferred_element_type=F32)
            pltpu.make_async_copy(srcs[i].at[s], buf.at[i, s], sin.at[i, s]).wait()
            old = buf[i, s, pl.ds(start, win), :].astype(F32)
            buf[i, s, pl.ds(start, win), :] = jnp.where(inside, placed, old).astype(BF)
            pltpu.make_async_copy(buf.at[i, s], dsts[i].at[s], sout.at[i, s]).start()
    for s in range(num_seqs):
        for i in range(2):
            pltpu.make_async_copy(buf.at[i, s], dsts[i].at[s], sout.at[i, s]).wait()


def fast_device(
    n,
    nt,
    tokens,
    gain_pre,
    w_query,
    w_key,
    w_value,
    w_forget,
    b_forget,
    w_out,
    gain_post,
    key_cache,
    value_cache,
    cum_cache,
    lengths,
    accepted,
    parent,
):
    num_seqs, prop, width = tokens.shape
    span, heads, hd = key_cache.shape[1:]
    rows = num_seqs * prop
    hw = heads * hd
    cols = heads * span
    sp = num_seqs // n
    R = sp * prop
    L = sp * heads * prop
    oc = gain_post.shape[0]
    kc = key_cache.reshape(num_seqs, cols, hd)
    vc = value_cache.reshape(num_seqs, cols, hd)
    cum = jnp.swapaxes(cum_cache, 1, 2).reshape(num_seqs * heads, span)
    anyspec = pl.BlockSpec(memory_space=pl.ANY)
    vmem = pl.BlockSpec(memory_space=pltpu.VMEM)
    smem = pl.BlockSpec(memory_space=pltpu.SMEM)
    V = pltpu.VMEM
    D = pltpu.SemaphoreType.DMA
    mixed, k_new, v_new, cum_new = pl.pallas_call(
        functools.partial(layer_kernel, n, nt, num_seqs, prop, heads, hd, span),
        out_shape=(
            jax.ShapeDtypeStruct((rows, oc), BF),
            jax.ShapeDtypeStruct((rows, hw), BF),
            jax.ShapeDtypeStruct((rows, hw), BF),
            jax.ShapeDtypeStruct(cum.shape, F32),
        ),
        in_specs=[
            anyspec,
            vmem,
            anyspec,
            anyspec,
            anyspec,
            vmem,
            smem,
            anyspec,
            vmem,
            anyspec,
            anyspec,
            vmem,
            smem,
            smem,
            vmem,
        ],
        out_specs=(vmem, anyspec, anyspec, vmem),
        scratch_shapes=[
            V((rows, width), BF),
            V((rows, width), BF),
            V((3,) + w_query.shape, BF),
            V(w_out.shape, BF),
            V(kc.shape, BF),
            V(vc.shape, BF),
            V((3, rows, hw), BF),
            V((3, n, R, hw), BF),
            V((3, rows, hw), BF),
            V((n, 8, L), F32),
            V((n, L, hd), BF),
            V((n, 8, L), F32),
            V((n, L, hd), BF),
            V((8, 128), F32),
            V((n, 8, 128), F32),
            V((num_seqs, cols), F32),
            V((rows, rows), F32),
            V((num_seqs, 128), F32),
            V((num_seqs * heads, 128), F32),
            V((rows, hw), BF),
            V((nt, rows, oc), BF),
            V((nt, rows, oc), BF),
            V((8, rows), F32),
            V((n, 8, rows), F32),
            V((8, rows), F32),
            V((nt, 8, rows), F32),
            D((9,)),
            D((11, n)),
            D((11, n)),
            D((2, nt)),
            D((2, nt)),
        ],
        compiler_params=pltpu.CompilerParams(
            collective_id=0, has_side_effects=True, vmem_limit_bytes=50 * 1024 * 1024
        ),
        name="layer",
    )(
        tokens.reshape(rows, width),
        gain_pre.reshape(1, width),
        w_query,
        w_key,
        w_value,
        w_forget.T,
        b_forget,
        w_out,
        gain_post.reshape(1, oc),
        kc,
        vc,
        cum,
        lengths,
        accepted,
        parent,
    )
    key_out, value_out = pl.pallas_call(
        functools.partial(write_kernel, num_seqs, prop, heads, hd, span),
        out_shape=(
            jax.ShapeDtypeStruct(kc.shape, BF),
            jax.ShapeDtypeStruct(vc.shape, BF),
        ),
        in_specs=[anyspec, anyspec, vmem, vmem, smem, smem],
        out_specs=(anyspec, anyspec),
        scratch_shapes=[
            V((2,) + kc.shape, BF),
            D((2, num_seqs)),
            D((2, num_seqs)),
        ],
        compiler_params=pltpu.CompilerParams(vmem_limit_bytes=16 * 1024 * 1024),
        name="cache_write",
    )(kc, vc, k_new, v_new, lengths, accepted)
    cum_out = jnp.swapaxes(cum_new.reshape(num_seqs, heads, span), 1, 2)
    return (
        mixed.reshape(num_seqs, prop, oc),
        key_out.reshape(key_cache.shape),
        value_out.reshape(value_cache.shape),
        cum_out,
    )


def choose(mesh):
    n, nt = mesh.shape["kv"], mesh.shape["tp"]

    def body(*args):
        tokens, key_cache = args[0], args[9]
        num_seqs, prop = tokens.shape[:2]
        span, heads = key_cache.shape[1:3]
        fits = (
            num_seqs % n == 0
            and (num_seqs // n) * heads * prop == 128
            and span == 128
            and num_seqs * heads <= 128
            and prop % 16 == 0
        )
        if fits:
            return fast_device(n, nt, *args)
        return per_device(*args)

    return body


def solution(mesh):
    return jax.shard_map(
        choose(mesh),
        mesh=mesh,
        in_specs=(
            P(),
            P(),
            P("kv", "tp"),
            P("kv", "tp"),
            P("kv", "tp"),
            P(),
            P(),
            P("tp", "kv"),
            P(("kv", "tp")),
            P(None, "kv", "tp", None),
            P(None, "kv", "tp", None),
            P(None, "kv", "tp"),
            P(),
            P(),
            P(),
        ),
        out_specs=(
            P(None, None, ("kv", "tp")),
            P(None, "kv", "tp", None),
            P(None, "kv", "tp", None),
            P(None, "kv", "tp"),
        ),
        check_vma=False,
    )
```

```python
import functools

import jax
import jax.numpy as jnp
from jax import lax
from jax.experimental import pallas as pl
from jax.experimental.pallas import tpu as pltpu
from jax.sharding import PartitionSpec as P

epsilon = 1e-06
floor_value = -1e30


def merged(part, axis, combine):
    gathered = jax.tree.map(lambda a: lax.all_gather(a, axis), part)

    def take(source):
        return jax.tree.map(lambda a: lax.dynamic_index_in_dim(a, source, 0, False), gathered)

    return lax.fori_loop(
        1, lax.axis_size(axis), lambda source, state: combine(state, take(source)), take(0)
    )


def ancestry(parent_ids, members):
    identity = jnp.eye(members, dtype=jnp.float32)
    parent_hot = (
        parent_ids[:, :, None] == jnp.arange(members, dtype=jnp.int32)[None, None, :]
    ).astype(jnp.float32)
    ancestors = jnp.minimum(identity[None] + parent_hot, 1.0)
    for sweep in range(max(1, (members - 1).bit_length())):
        ancestors = jnp.minimum(
            jnp.einsum("bij,bjk->bik", ancestors, ancestors, precision=lax.Precision.HIGHEST), 1.0
        )
    return ancestors


def combine_parts(first, second):
    new_max = jnp.maximum(first[0], second[0])
    first_scale = jnp.exp(first[0] - new_max)
    second_scale = jnp.exp(second[0] - new_max)
    return (
        new_max,
        first[1] * first_scale + second[1] * second_scale,
        first[2] * first_scale[..., None] + second[2] * second_scale[..., None],
        jnp.maximum(first[3], second[3]),
    )


def finish_rows(cache_max, cache_total, cache_values, last_rows, tree_max, tree_total, tree_values):
    shifted = cache_max + last_rows
    top = jnp.maximum(shifted, tree_max)
    cache_scale = jnp.exp(shifted - top)
    tree_scale = jnp.exp(tree_max - top)
    attended = (
        (cache_values * cache_scale[..., None] + tree_values * tree_scale[..., None])
        / (cache_total * cache_scale + tree_total * tree_scale)[..., None]
    ).astype(jnp.bfloat16)
    return attended.reshape(attended.shape[0], attended.shape[1] * attended.shape[2])


def per_device(
    tokens,
    gain_pre,
    w_query,
    w_key,
    w_value,
    w_forget,
    b_forget,
    w_out,
    gain_post,
    key_cache,
    value_cache,
    cum_cache,
    lengths,
    accepted,
    parent,
):
    num_seqs, proposals, model_width = tokens.shape
    kv_rank = lax.axis_index("kv")
    tp_rank = lax.axis_index("tp")
    span = key_cache.shape[1]
    heads_local = key_cache.shape[2]
    head_dim = key_cache.shape[3]
    scale = head_dim ** (-0.5)
    all_rows = num_seqs * proposals
    tok_float = tokens.astype(jnp.float32)
    normed = (
        tok_float
        * lax.rsqrt(jnp.mean(tok_float * tok_float, -1, keepdims=True) + epsilon)
        * gain_pre
    ).astype(jnp.bfloat16)
    flat = normed.reshape(all_rows, model_width)
    weight_rows = w_query.shape[0]
    local_rows = lax.dynamic_slice_in_dim(flat, kv_rank * weight_rows, weight_rows, 1)
    query_part = jnp.dot(local_rows, w_query, preferred_element_type=jnp.float32)
    key_part = jnp.dot(local_rows, w_key, preferred_element_type=jnp.float32)
    value_part = jnp.dot(local_rows, w_value, preferred_element_type=jnp.float32)
    summed = (
        lax.psum(query_part.astype(jnp.bfloat16), "kv").astype(jnp.float32),
        lax.psum(key_part.astype(jnp.bfloat16), "kv").astype(jnp.float32),
        lax.psum(value_part.astype(jnp.bfloat16), "kv").astype(jnp.float32),
    )
    query_flat = summed[0].astype(jnp.bfloat16)
    key_flat = summed[1].astype(jnp.bfloat16)
    value_flat = summed[2].astype(jnp.bfloat16)
    query = query_flat.reshape(num_seqs, proposals, heads_local, head_dim)
    key_new = key_flat.reshape(num_seqs, proposals, heads_local, head_dim)
    value_new = value_flat.reshape(num_seqs, proposals, heads_local, head_dim)
    forget_cols = lax.dynamic_slice_in_dim(w_forget, tp_rank * heads_local, heads_local, 1)
    forget_bias = lax.dynamic_slice_in_dim(b_forget, tp_rank * heads_local, heads_local, 0)
    log_forget = jax.nn.log_sigmoid(
        jnp.dot(flat, forget_cols, preferred_element_type=jnp.float32) + forget_bias
    ).reshape(num_seqs, proposals, heads_local)
    ancestors = ancestry(parent, proposals)
    path = jnp.einsum("bij,bjh->bih", ancestors, log_forget, precision=lax.Precision.HIGHEST)
    valid = lengths + accepted
    positions = kv_rank * span + jnp.arange(span, dtype=jnp.int32)
    live = (positions[None, :] < valid[:, None])[:, None, None, :]
    score = (
        jnp.einsum("bihd,bkhd->bihk", query, key_cache, preferred_element_type=jnp.float32) * scale
        + path[..., None]
        - jnp.swapaxes(cum_cache, 1, 2)[:, None]
    )
    block_max = jnp.max(jnp.where(live, score, floor_value), axis=-1)
    weight = jnp.exp(jnp.where(live, score - block_max[..., None], floor_value))
    block_total = jnp.sum(weight, axis=-1)
    block_values = jnp.einsum(
        "bihk,bkhd->bihd",
        weight.astype(jnp.bfloat16),
        value_cache,
        preferred_element_type=jnp.float32,
    )
    owner = positions[None, :] == (valid - 1)[:, None]
    candidate = jnp.max(jnp.where(owner[:, :, None], cum_cache, floor_value), axis=1)
    tree_mask = (ancestors > 0.5)[:, :, None, :]
    tree_score = (
        jnp.einsum("bihd,bjhd->bihj", query, key_new, preferred_element_type=jnp.float32) * scale
        + path[..., None]
        - jnp.swapaxes(path, 1, 2)[:, None]
    )
    tree_max = jnp.max(jnp.where(tree_mask, tree_score, floor_value), axis=-1)
    tree_weight = jnp.exp(jnp.where(tree_mask, tree_score - tree_max[..., None], floor_value))
    tree_total = jnp.sum(tree_weight, axis=-1)
    tree_values = jnp.einsum(
        "bihj,bjhd->bihd",
        tree_weight.astype(jnp.bfloat16),
        value_new,
        preferred_element_type=jnp.float32,
    )
    tree_max_rows = tree_max.reshape(all_rows, heads_local)
    tree_total_rows = tree_total.reshape(all_rows, heads_local)
    tree_values_rows = tree_values.reshape(all_rows, heads_local, head_dim)
    cache_max, cache_total, cache_values, last_cum = merged(
        (block_max, block_total, block_values, candidate), "kv", combine_parts
    )
    last_rows = jnp.broadcast_to(last_cum[:, None, :], (num_seqs, proposals, heads_local)).reshape(
        all_rows, heads_local
    )
    attended = finish_rows(
        cache_max.reshape(all_rows, heads_local),
        cache_total.reshape(all_rows, heads_local),
        cache_values.reshape(all_rows, heads_local, head_dim),
        last_rows,
        tree_max_rows,
        tree_total_rows,
        tree_values_rows,
    )
    mixed_part = jnp.dot(attended, w_out, preferred_element_type=jnp.float32)
    mixed_sum = lax.psum_scatter(
        mixed_part.astype(jnp.bfloat16), "tp", scatter_dimension=1, tiled=True
    ).astype(jnp.float32)
    squares = lax.psum(jnp.sum(mixed_sum * mixed_sum, axis=1), ("kv", "tp"))
    mixed = (mixed_sum * lax.rsqrt(squares / model_width + epsilon)[:, None] * gain_post).astype(
        jnp.bfloat16
    )
    mixed = mixed.reshape(num_seqs, proposals, mixed_sum.shape[1])
    relative = positions[None, :] - valid[:, None]
    select = relative[:, :, None] == jnp.arange(proposals, dtype=jnp.int32)[None, None, :]
    written = (relative >= 0) & (relative < proposals)
    placed_keys = jnp.einsum(
        "bkj,bjhd->bkhd", select.astype(jnp.bfloat16), key_new, preferred_element_type=jnp.float32
    ).astype(jnp.bfloat16)
    placed_values = jnp.einsum(
        "bkj,bjhd->bkhd", select.astype(jnp.bfloat16), value_new, preferred_element_type=jnp.float32
    ).astype(jnp.bfloat16)
    key_out = jnp.where(written[:, :, None, None], placed_keys, key_cache)
    value_out = jnp.where(written[:, :, None, None], placed_values, value_cache)
    cum_new = last_cum[:, None, :] + path
    placed_cum = jnp.einsum(
        "bkj,bjh->bkh", select.astype(jnp.float32), cum_new, precision=lax.Precision.HIGHEST
    )
    cum_out = jnp.where(written[:, :, None], placed_cum, cum_cache)
    return (mixed, key_out, value_out, cum_out)


MESH = pl.DeviceIdType.MESH
HI = lax.Precision.HIGHEST
F32 = jnp.float32
BF = jnp.bfloat16


def iota(shape, dim):
    return lax.broadcasted_iota(jnp.int32, shape, dim)


def hot(mask):
    return jnp.where(mask, 1.0, 0.0).astype(F32)


def dot_hi(a, b, dims=(((1,), (0,)), ((), ()))):
    return lax.dot_general(a, b, dims, precision=HI, preferred_element_type=F32)


NT = (((1,), (1,)), ((), ()))


def layer_kernel(
    n,
    nt,
    num_seqs,
    prop,
    heads,
    hd,
    span,
    tok,
    gain_h,
    wq,
    wk,
    wv,
    wft_h,
    bias_h,
    wo,
    gpost_h,
    kc,
    vc,
    cum_h,
    lens_h,
    accs_h,
    parent_h,
    mixed_out,
    kv_out,
    cum_out,
    tokv,
    normed,
    gain,
    wv3,
    wft,
    wov,
    gpost,
    kcv,
    vcv,
    cum,
    parent,
    bias,
    lens,
    accs,
    partq,
    rsq,
    part2,
    rs1,
    half,
    rs2,
    kvown,
    flat,
    kvflat,
    qall,
    st_send,
    val_send,
    st_recv,
    val_recv,
    cand_send,
    cand_recv,
    brow,
    anc,
    tpath,
    ptile,
    att,
    o_send,
    o_recv,
    sq_send,
    sq_recv,
    sq2_send,
    sq2_recv,
    loc,
    ssem,
    rsem,
    tssem,
    trsem,
):
    me = lax.axis_index("kv")
    mt = lax.axis_index("tp")
    rows = num_seqs * prop
    width = tok.shape[1]
    hw = heads * hd
    kdim = wq.shape[0]
    cols = heads * span
    sp = num_seqs // n
    R = sp * prop
    hp = heads * prop
    L = sp * hp
    scale = hd ** (-0.5)
    base = me * span
    heads_all = wft.shape[0]

    barrier = pltpu.get_barrier_semaphore()

    def greet(d, c):
        pl.semaphore_signal(
            barrier, inc=1, device_id={"kv": lax.rem(me + d, n)}, device_id_type=MESH
        )
        return c

    def greet_t(d, c):
        pl.semaphore_signal(
            barrier, inc=1, device_id={"tp": lax.rem(mt + d, nt)}, device_id_type=MESH
        )
        return c

    lax.fori_loop(1, n, greet, 0)
    lax.fori_loop(1, nt, greet_t, 0)

    pairs = (
        (tok, tokv),
        (gain_h, gain),
        (wq, wv3.at[0]),
        (wk, wv3.at[1]),
        (wv, wv3.at[2]),
        (cum_h, cum),
        (lens_h, lens),
        (accs_h, accs),
        (parent_h, parent),
        (bias_h, bias),
        (wft_h, wft),
        (kc, kcv),
        (vc, vcv),
        (wo, wov),
        (gpost_h, gpost),
    )
    ins = [pltpu.make_async_copy(a, b, loc.at[i]) for i, (a, b) in enumerate(pairs)]
    for c in ins:
        c.start()
    par = lax.rem(me, 2)
    mate = me + 1 - 2 * par
    nh = n // 2

    def to_kv(ph, d, src, dst, sign=1):
        peer = lax.rem(me + sign * d + n, n)
        return pltpu.make_async_remote_copy(
            src_ref=src,
            dst_ref=dst,
            send_sem=ssem.at[ph, d],
            recv_sem=rsem.at[ph, d],
            device_id={"kv": peer},
            device_id_type=MESH,
        )

    def to_tp(ph, d, src, dst):
        peer = lax.rem(mt + d, nt)
        return pltpu.make_async_remote_copy(
            src_ref=src,
            dst_ref=dst,
            send_sem=tssem.at[ph, d],
            recv_sem=trsem.at[ph, d],
            device_id={"tp": peer},
            device_id_type=MESH,
        )

    def up(d):
        return lax.rem(me + d, n)

    def down(d):
        return lax.rem(me - d + n, n)

    def rrow(i):
        return pl.ds(pl.multiple_of(i * R, R), R)

    def lrow(i):
        return pl.ds(pl.multiple_of(i * L, L), L)

    def to_peer(ph, d, peer, src, dst):
        return pltpu.make_async_remote_copy(
            src_ref=src,
            dst_ref=dst,
            send_sem=ssem.at[ph, d],
            recv_sem=rsem.at[ph, d],
            device_id={"kv": peer},
            device_id_type=MESH,
        )

    def rsq_copy(d):
        return to_kv(0, d, partq.at[rrow(up(d))], rsq.at[d])

    def rs1_copy():
        return to_peer(1, 0, mate, part2.at[1 - par], rs1)

    def rs2_copy(e):
        peer = up(2 * e)
        return to_peer(2, e, peer, half.at[peer // 2], rs2.at[e])

    def gather_along(ph, e, view):
        return to_peer(ph, 2 * e, up(2 * e), view(me), view(me))

    def gather_mate(ph, e, view):
        c = down(2 * e)
        return to_peer(ph, 2 * e + 1, mate, view(c), view(c))

    def gather_start(ph, view):
        each(nh, lambda e: gather_along(ph, e, view).start())
        gather_mate(ph, 0, view).start()

    def gather_pass(ph, view):
        def one(e):
            c = down(2 * e)
            to_peer(ph, 2 * e, me, view(c), view(c)).wait_recv()
            gather_mate(ph, e, view).start()

        each(nh, one)

    def mate_chunk(e):
        return lax.rem(mate - 2 * e + n, n)

    def gather_wait(ph, e, view):
        c = mate_chunk(e)
        to_peer(ph, 2 * e + 1, mate, view(c), view(c)).wait_recv()

    def gather_drain(ph, view):
        each(nh, lambda e: gather_along(ph, e, view).wait_send())
        for e in range(nh):
            gather_mate(ph, e, view).wait_send()

    def q_view(c):
        return qall.at[rrow(c)]

    def kv_view(c):
        return kvflat.at[:, lrow(c)]

    def att_view(c):
        return att.at[rrow(c)]

    def stat_copy(d):
        return to_kv(6, d, st_send.at[d], st_recv.at[d], -1)

    def val_copy(d):
        return to_kv(7, d, val_send.at[d], val_recv.at[d], -1)

    def cand_copy(d):
        return to_kv(8, d, cand_send, cand_recv.at[d])

    def sq_copy(d):
        return to_kv(10, d, sq_send, sq_recv.at[d])

    def each(count, fn):
        def body(d, c):
            fn(d)
            return c

        lax.fori_loop(1, count, body, 0)

    ins[0].wait()
    ins[1].wait()
    nb = prop

    def norm_rows(i, c):
        sl = pl.ds(pl.multiple_of(i * nb, nb), nb)
        t = tokv[sl, :].astype(F32)
        inv = lax.rsqrt(jnp.mean(t * t, axis=-1, keepdims=True) + epsilon)
        normed[sl, :] = (t * inv * gain[...]).astype(BF)
        return c

    lax.fori_loop(0, rows // nb, norm_rows, 0)
    local = normed[:, pl.ds(pl.multiple_of(me * kdim, kdim), kdim)]
    pl.semaphore_wait(barrier, n - 1 + nt - 1)
    ins[2].wait()
    partq[...] = jnp.dot(local, wv3[0], preferred_element_type=F32).astype(BF)
    each(n, lambda d: rsq_copy(d).start())
    for i in range(2):
        ins[3 + i].wait()
        both_rows = jnp.dot(local, wv3[1 + i], preferred_element_type=F32).astype(BF)
        for c in range(n):
            part2[c % 2, c // 2, :, i * hw : (i + 1) * hw] = both_rows[c * R : (c + 1) * R]
    for c in ins[5:11]:
        c.wait()

    r64 = num_seqs * heads
    c64 = cum[...]
    srow = iota((r64, span), 0) // heads
    lane = iota((r64, span), 1)
    rel64 = jnp.zeros((r64, span), jnp.int32)
    rel16 = jnp.zeros((num_seqs, cols), jnp.int32)
    s16 = iota((num_seqs, cols), 0)
    for s in range(num_seqs):
        rel_s = lens[s] + accs[s] - base
        rel64 = jnp.where(srow == s, rel_s, rel64)
        rel16 = jnp.where(s16 == s, rel_s, rel16)
    cand = jnp.max(jnp.where(lane == rel64 - 1, c64, floor_value), axis=1, keepdims=True)
    diag = iota((r64, 128), 0) == iota((r64, 128), 1)
    cand_lane = jnp.sum(jnp.where(diag, cand, 0.0), axis=0, keepdims=True)
    cand_send[...] = jnp.broadcast_to(cand_lane, (8, 128))
    each(n, lambda d: cand_copy(d).start())

    spread = hot(iota((span, cols), 1) // heads == iota((span, cols), 0))
    e1 = dot_hi(c64, spread)
    e1 = jnp.where(iota((r64, cols), 0) % heads == iota((r64, cols), 1) % heads, e1, 0.0)
    take = hot(iota((num_seqs, r64), 1) // heads == iota((num_seqs, r64), 0))
    cflat = dot_hi(take, e1)
    brow[...] = jnp.where(iota((num_seqs, cols), 1) // heads < rel16, -cflat, floor_value)

    ri = iota((rows, rows), 0)
    ci = iota((rows, rows), 1)
    pick = hot(iota((rows, num_seqs), 0) // prop == iota((rows, num_seqs), 1))
    pb = dot_hi(pick, parent[...].astype(F32))
    pcol = jnp.sum(
        jnp.where(iota((rows, prop), 1) == iota((rows, prop), 0) % prop, pb, 0.0),
        axis=1,
        keepdims=True,
    )
    target = jnp.where(pcol >= 0.0, (ri // prop * prop).astype(F32) + pcol, -1.0)
    a = jnp.where((ri == ci) | (ci.astype(F32) == target), 1.0, 0.0)
    for sweep in range(max(1, (prop - 1).bit_length())):
        low = a.astype(BF)
        a = jnp.minimum(jnp.dot(low, low, preferred_element_type=F32), 1.0)
    anc[...] = a
    lf = lax.dot_general(wft[...], normed[...], NT, preferred_element_type=F32)
    bcol = jnp.zeros((heads_all, rows), F32)
    for h in range(heads_all):
        bcol = jnp.where(iota((heads_all, rows), 0) == h, bias[h], bcol)
    z = lf + bcol
    lf = jnp.minimum(z, 0.0) - jnp.log1p(jnp.exp(-jnp.abs(z)))
    path_t = dot_hi(lf, a, NT)
    rep = hot(iota((r64, heads_all), 1) == mt * heads + iota((r64, heads_all), 0) % heads)
    pm = dot_hi(rep, path_t)
    pm = jnp.where(iota((r64, rows), 1) // prop == iota((r64, rows), 0) // heads, pm, 0.0)
    fold = hot(iota((rows, 128), 0) % prop == iota((rows, 128), 1) % prop)
    pt = dot_hi(pm, fold)
    ptile[...] = pt
    ptm = jnp.where((iota((r64, 128), 1) // prop) % heads == iota((r64, 128), 0) % heads, pt, 0.0)
    tpath[...] = dot_hi(take, ptm)

    own_q = partq[rrow(me)].astype(F32)
    for d in range(1, n):
        rsq_copy(d).wait_recv()
        own_q = own_q + rsq[d].astype(F32)
    qall[rrow(me)] = own_q.astype(BF)
    gather_start(3, q_view)
    rs1_copy().start()

    ins[11].wait()
    ins[12].wait()
    same_head = iota((hp, cols), 0) // prop == iota((hp, cols), 1) % heads
    diag_l = iota((L, L), 0) == iota((L, L), 1)

    def heads_of(block):
        return jnp.concatenate([block[:, h * hd : (h + 1) * hd] for h in range(heads)], axis=0)

    def block_part(src):
        maxes, totals, values = [], [], []
        for j in range(sp):
            s = src * sp + j
            q = heads_of(qall[pl.ds(pl.multiple_of(s * prop, prop), prop), :])
            sc = lax.dot_general(q, kcv[s], NT, preferred_element_type=F32) * scale
            sc = jnp.where(same_head, sc + brow[pl.ds(s, 1), :], floor_value)
            m = jnp.max(sc, axis=1, keepdims=True)
            w = jnp.exp(sc - m)
            maxes.append(m)
            totals.append(jnp.sum(w, axis=1, keepdims=True))
            values.append(
                jnp.dot(w.astype(BF), vcv[s], preferred_element_type=F32).astype(BF)
            )
        m = jnp.concatenate(maxes, axis=0)
        t = jnp.concatenate(totals, axis=0)
        m_lane = jnp.sum(jnp.where(diag_l, m, 0.0), axis=0, keepdims=True)
        t_lane = jnp.sum(jnp.where(diag_l, t, 0.0), axis=0, keepdims=True)
        stats = jnp.where(iota((8, L), 0) == 0, m_lane, t_lane)
        return stats, jnp.concatenate(values, axis=0)

    def remote_block(d):
        src = down(d)
        stats, values = block_part(src)
        st_send[d] = stats
        val_send[d] = values
        stat_copy(d).start()
        val_copy(d).start()

    stats, values = block_part(me)
    st_recv[0] = stats
    val_recv[0] = values
    gather_pass(3, q_view)
    each(nh, lambda e: remote_block(2 * e))
    rs1_copy().wait_recv()
    for i in range(nh):
        half[i] = (part2[par, i].astype(F32) + rs1[i].astype(F32)).astype(BF)
    each(nh, lambda e: rs2_copy(e).start())

    def mate_block(e, c):
        gather_wait(3, e, q_view)
        remote_block(lax.rem(me - mate_chunk(e) + n, n))
        return c

    lax.fori_loop(0, nh, mate_block, 0)
    own_kv = half[me // 2].astype(F32)
    for e in range(1, nh):
        rs2_copy(e).wait_recv()
        own_kv = own_kv + rs2[e].astype(F32)
    kvown[...] = own_kv.astype(BF)
    for i in range(2):
        for h in range(heads):
            flat[pl.ds(h, R, stride=heads), :] = own_kv[:, i * hw + h * hd : i * hw + (h + 1) * hd]
        kvflat[i, lrow(me)] = flat[...].astype(BF)

    fold_h = iota((rows, hp), 0)
    tmax, ttot, tval = [], [], []
    for j in range(sp):
        s = me * sp + j
        q = heads_of(qall[pl.ds(pl.multiple_of(s * prop, prop), prop), :])
        k = heads_of(kvown[j * prop : (j + 1) * prop, 0:hw])
        v = heads_of(kvown[j * prop : (j + 1) * prop, hw : 2 * hw])
        arows = anc[pl.ds(pl.multiple_of(s * prop, prop), prop), :]
        sel = hot(fold_h == s * prop + iota((rows, hp), 1) % prop).astype(BF)
        am = jnp.dot(arows.astype(BF), sel, preferred_element_type=F32)
        am = jnp.concatenate([am] * heads, axis=0)
        mask = (am > 0.5) & (iota((hp, hp), 0) // prop == iota((hp, hp), 1) // prop)
        sc = lax.dot_general(q, k, NT, preferred_element_type=F32) * scale
        sc = jnp.where(mask, sc - tpath[pl.ds(s, 1), 0:hp], floor_value)
        m = jnp.max(sc, axis=1, keepdims=True)
        w = jnp.where(mask, jnp.exp(sc - m), 0.0)
        tmax.append(m)
        ttot.append(jnp.sum(w, axis=1, keepdims=True))
        tval.append(jnp.dot(w.astype(BF), v, preferred_element_type=F32))
    tree_max = jnp.concatenate(tmax, axis=0)
    tree_tot = jnp.concatenate(ttot, axis=0)
    tree_val = jnp.concatenate(tval, axis=0)

    last_lane = cand_send[...]
    for d in range(1, n):
        cand_copy(d).wait_recv()
        last_lane = jnp.maximum(last_lane, cand_recv[d])
    last_col = jnp.sum(jnp.where(diag, last_lane[0:1], 0.0), axis=1, keepdims=True)
    own_rows = iota((L, 128), 0)
    own_pick = iota((L, 128), 1) == (me * sp + own_rows // hp) * heads + (own_rows % hp) // prop
    last_own = jnp.sum(jnp.where(own_pick, last_lane[0:1], 0.0), axis=1, keepdims=True)

    shifted_path = ptile[...]
    for b in range((span - 1).bit_length()):
        moved = pltpu.roll(shifted_path, 1 << b, 1)
        shifted_path = jnp.where((rel64 >> b) & 1 == 1, moved, shifted_path)
    off = lane - rel64
    cum_out[...] = jnp.where((off >= 0) & (off < prop), last_col + shifted_path, cum[...])

    for d in range(1, n):
        stat_copy(d).wait_recv()
    top = st_recv[0]
    for d in range(1, n):
        top = jnp.maximum(top, st_recv[d])
    top = top[0:1]

    def col(x):
        return jnp.sum(jnp.where(diag_l, x, 0.0), axis=1, keepdims=True)

    cache_tot = jnp.zeros((1, L), F32)
    scales = []
    for d in range(n):
        sd = jnp.exp(st_recv[d, 0:1] - top)
        scales.append(col(sd))
        cache_tot = cache_tot + st_recv[d, 1:2] * sd
    shifted = col(top) + last_own
    both = jnp.maximum(shifted, tree_max)
    cscale = jnp.exp(shifted - both)
    tscale = jnp.exp(tree_max - both)
    denom = col(cache_tot) * cscale + tree_tot * tscale
    vals = jnp.zeros((L, hd), F32)
    for d in range(n):
        if d > 0:
            val_copy(d).wait_recv()
        vals = vals + val_recv[d].astype(F32) * scales[d]
    attended = ((vals * cscale + tree_val * tscale) / denom).astype(BF)
    for j in range(sp):
        for h in range(heads):
            att[pl.ds(pl.multiple_of(me * R + j * prop, prop), prop), h * hd : (h + 1) * hd] = (
                attended[j * hp + h * prop : j * hp + (h + 1) * prop]
            )
    gather_start(4, att_view)
    gather_start(5, kv_view)
    ins[13].wait()
    ins[14].wait()
    gather_pass(4, att_view)
    for e in range(nh):
        gather_wait(4, e, att_view)
    full = jnp.dot(att[...], wov[...], preferred_element_type=F32).astype(BF)
    oc = o_send.shape[2]
    for t in range(nt):
        o_send[t] = full[:, t * oc : (t + 1) * oc]

    def o_copy(d):
        return to_tp(0, d, o_send.at[lax.rem(mt + d, nt)], o_recv.at[d])

    def sq2_copy(d):
        return to_tp(1, d, sq2_send, sq2_recv.at[d])

    each(nt, lambda d: o_copy(d).start())
    gather_pass(5, kv_view)
    mixed = o_send[mt].astype(F32)
    for d in range(1, nt):
        o_copy(d).wait_recv()
        mixed = mixed + o_recv[d].astype(F32)
    sq_send[...] = dot_hi(jnp.ones((8, oc), F32), mixed * mixed, NT)
    each(n, lambda d: sq_copy(d).start())
    for e in range(nh):
        gather_wait(5, e, kv_view)
    out_kv = pltpu.make_async_copy(kvflat, kv_out, loc.at[15])
    out_kv.start()
    sq = sq_send[...]
    for d in range(1, n):
        sq_copy(d).wait_recv()
        sq = sq + sq_recv[d]
    sq2_send[...] = sq
    each(nt, lambda d: sq2_copy(d).start())
    for d in range(1, nt):
        sq2_copy(d).wait_recv()
        sq = sq + sq2_recv[d]
    ssum = dot_hi(sq, jnp.full((8, oc), 0.125, F32), (((0,), (0,)), ((), ())))
    mixed_out[...] = (mixed * lax.rsqrt(ssum / width + epsilon) * gpost[...]).astype(BF)

    def drain(d):
        rsq_copy(d).wait_send()
        stat_copy(d).wait_send()
        val_copy(d).wait_send()
        cand_copy(d).wait_send()
        sq_copy(d).wait_send()

    each(n, drain)
    rs1_copy().wait_send()
    each(nh, lambda e: rs2_copy(e).wait_send())
    gather_drain(3, q_view)
    gather_drain(4, att_view)
    gather_drain(5, kv_view)

    def drain_t(d):
        o_copy(d).wait_send()
        sq2_copy(d).wait_send()

    each(nt, drain_t)
    out_kv.wait()


def write_kernel(
    num_seqs,
    prop,
    span,
    kc,
    vc,
    kv_new,
    mixed,
    cum,
    lens_h,
    accs_h,
    k_out,
    v_out,
    mixed_out,
    cum_out,
    buf,
    fresh,
    lens,
    accs,
    sem,
    sin,
    sout,
):
    base = lax.axis_index("kv") * span
    small = [
        pltpu.make_async_copy(lens_h, lens, sem.at[0]),
        pltpu.make_async_copy(accs_h, accs, sem.at[1]),
        pltpu.make_async_copy(kv_new, fresh, sem.at[2]),
        pltpu.make_async_copy(mixed, mixed_out, sem.at[3]),
        pltpu.make_async_copy(cum, cum_out, sem.at[4]),
    ]
    cut = sin.shape[1]
    step = num_seqs // cut
    arrays = ((kc, k_out), (vc, v_out))

    def part(c):
        return pl.ds(c * step, step)

    def come(c, i):
        return pltpu.make_async_copy(arrays[i][0].at[part(c)], buf.at[i, part(c)], sin.at[i, c])

    def leave(c, i):
        return pltpu.make_async_copy(buf.at[i, part(c)], arrays[i][1].at[part(c)], sout.at[i, c])

    for c in small[:3]:
        c.start()
    for c in range(cut):
        for i in range(2):
            come(c, i).start()
    for c in small[3:]:
        c.start()
    for c in small[:3]:
        c.wait()

    def place(i, s):
        rel = lens[s] + accs[s] - base
        whole = (rel >= 0) & (rel <= span - prop)
        partly = (rel > -prop) & (rel < span) & jnp.logical_not(whole)

        @pl.when(whole)
        def _():
            buf[i, s, pl.ds(rel, prop)] = fresh[i, s]

        @pl.when(partly)
        def _():
            def one(j, c):
                buf[i, s, pl.ds(rel + j, 1)] = fresh[i, s, pl.ds(j, 1)]
                return c

            lax.fori_loop(jnp.maximum(-rel, 0), jnp.minimum(span - rel, prop), one, 0)

    for c in range(cut):
        for i in range(2):
            come(c, i).wait()
            for s in range(c * step, (c + 1) * step):
                place(i, s)
            leave(c, i).start()
    for c in range(cut):
        for i in range(2):
            leave(c, i).wait()
    for c in small[3:]:
        c.wait()


def fast_device(
    n,
    nt,
    tokens,
    gain_pre,
    w_query,
    w_key,
    w_value,
    w_forget,
    b_forget,
    w_out,
    gain_post,
    key_cache,
    value_cache,
    cum_cache,
    lengths,
    accepted,
    parent,
):
    num_seqs, prop, width = tokens.shape
    span, heads, hd = key_cache.shape[1:]
    rows = num_seqs * prop
    hw = heads * hd
    cols = heads * span
    sp = num_seqs // n
    R = sp * prop
    L = sp * heads * prop
    oc = gain_post.shape[0]
    kc = key_cache.reshape(num_seqs, cols, hd)
    vc = value_cache.reshape(num_seqs, cols, hd)
    cum = jnp.swapaxes(cum_cache, 1, 2).reshape(num_seqs * heads, span)
    vmem = pl.BlockSpec(memory_space=pltpu.VMEM)
    V = pltpu.VMEM
    D = pltpu.SemaphoreType.DMA
    hbm = pl.BlockSpec(memory_space=pltpu.HBM)
    S = pltpu.SMEM
    nh = n // 2
    mixed, kv_new, cum_new = pl.pallas_call(
        functools.partial(layer_kernel, n, nt, num_seqs, prop, heads, hd, span),
        out_shape=(
            jax.ShapeDtypeStruct((rows, oc), BF),
            jax.ShapeDtypeStruct((2, rows * heads, hd), BF),
            jax.ShapeDtypeStruct(cum.shape, F32),
        ),
        in_specs=[hbm] * 15,
        out_specs=(vmem, hbm, vmem),
        scratch_shapes=[
            V((rows, width), BF),
            V((rows, width), BF),
            V((1, width), F32),
            V((3,) + w_query.shape, BF),
            V(w_forget.T.shape, BF),
            V(w_out.shape, BF),
            V((1, oc), F32),
            V(kc.shape, BF),
            V(vc.shape, BF),
            V(cum.shape, F32),
            V(parent.shape, jnp.int32),
            S(b_forget.shape, F32),
            S(lengths.shape, jnp.int32),
            S(accepted.shape, jnp.int32),
            V((rows, hw), BF),
            V((n, R, hw), BF),
            V((2, nh, R, 2 * hw), BF),
            V((nh, R, 2 * hw), BF),
            V((nh, R, 2 * hw), BF),
            V((nh, R, 2 * hw), BF),
            V((R, 2 * hw), BF),
            V((L, hd), F32),
            V((2, rows * heads, hd), BF),
            V((rows, hw), BF),
            V((n, 8, L), F32),
            V((n, L, hd), BF),
            V((n, 8, L), F32),
            V((n, L, hd), BF),
            V((8, 128), F32),
            V((n, 8, 128), F32),
            V((num_seqs, cols), F32),
            V((rows, rows), F32),
            V((num_seqs, 128), F32),
            V((num_seqs * heads, 128), F32),
            V((rows, hw), BF),
            V((nt, rows, oc), BF),
            V((nt, rows, oc), BF),
            V((8, rows), F32),
            V((n, 8, rows), F32),
            V((8, rows), F32),
            V((nt, 8, rows), F32),
            D((16,)),
            D((11, n)),
            D((11, n)),
            D((2, nt)),
            D((2, nt)),
        ],
        compiler_params=pltpu.CompilerParams(
            collective_id=0, has_side_effects=True, vmem_limit_bytes=67043328
        ),
        name="layer",
    )(
        tokens.reshape(rows, width),
        gain_pre.reshape(1, width),
        w_query,
        w_key,
        w_value,
        w_forget.T,
        b_forget,
        w_out,
        gain_post.reshape(1, oc),
        kc,
        vc,
        cum,
        lengths,
        accepted,
        parent,
    )
    key_out, value_out, mixed, cum_new = pl.pallas_call(
        functools.partial(write_kernel, num_seqs, prop, span),
        out_shape=(
            jax.ShapeDtypeStruct(key_cache.shape, BF),
            jax.ShapeDtypeStruct(value_cache.shape, BF),
            jax.ShapeDtypeStruct(mixed.shape, BF),
            jax.ShapeDtypeStruct(cum_new.shape, F32),
        ),
        in_specs=[hbm] * 7,
        out_specs=(hbm,) * 4,
        scratch_shapes=[
            V((2,) + key_cache.shape, BF),
            V((2, num_seqs, prop, heads, hd), BF),
            S(lengths.shape, jnp.int32),
            S(accepted.shape, jnp.int32),
            D((5,)),
            D((2, 4)),
            D((2, 4)),
        ],
        compiler_params=pltpu.CompilerParams(vmem_limit_bytes=67043328),
        name="cache_write",
    )(
        key_cache,
        value_cache,
        kv_new.reshape(2, num_seqs, prop, heads, hd),
        mixed,
        cum_new,
        lengths,
        accepted,
    )
    cum_out = jnp.swapaxes(cum_new.reshape(num_seqs, heads, span), 1, 2)
    return (
        mixed.reshape(num_seqs, prop, oc),
        key_out,
        value_out,
        cum_out,
    )


def choose(mesh):
    n, nt = mesh.shape["kv"], mesh.shape["tp"]

    def body(*args):
        tokens, key_cache = args[0], args[9]
        num_seqs, prop = tokens.shape[:2]
        span, heads = key_cache.shape[1:3]
        fits = (
            num_seqs % n == 0
            and n % 2 == 0
            and num_seqs % 4 == 0
            and (num_seqs // n) * heads * prop == 128
            and span == 128
            and num_seqs * heads <= 128
            and prop % 16 == 0
        )
        if fits:
            return fast_device(n, nt, *args)
        return per_device(*args)

    return body


def solution(mesh):
    return jax.shard_map(
        choose(mesh),
        mesh=mesh,
        in_specs=(
            P(),
            P(),
            P("kv", "tp"),
            P("kv", "tp"),
            P("kv", "tp"),
            P(),
            P(),
            P("tp", "kv"),
            P(("kv", "tp")),
            P(None, "kv", "tp", None),
            P(None, "kv", "tp", None),
            P(None, "kv", "tp"),
            P(),
            P(),
            P(),
        ),
        out_specs=(
            P(None, None, ("kv", "tp")),
            P(None, "kv", "tp", None),
            P(None, "kv", "tp", None),
            P(None, "kv", "tp"),
        ),
        check_vma=False,
    )
```

```python
import functools

import jax
import jax.numpy as jnp
from jax import lax
from jax.experimental import pallas as pl
from jax.experimental.pallas import tpu as pltpu
from jax.sharding import PartitionSpec as P

epsilon = 1e-06
floor_value = -1e30


def merged(part, axis, combine):
    gathered = jax.tree.map(lambda a: lax.all_gather(a, axis), part)

    def take(source):
        return jax.tree.map(lambda a: lax.dynamic_index_in_dim(a, source, 0, False), gathered)

    return lax.fori_loop(
        1, lax.axis_size(axis), lambda source, state: combine(state, take(source)), take(0)
    )


def ancestry(parent_ids, members):
    identity = jnp.eye(members, dtype=jnp.float32)
    parent_hot = (
        parent_ids[:, :, None] == jnp.arange(members, dtype=jnp.int32)[None, None, :]
    ).astype(jnp.float32)
    ancestors = jnp.minimum(identity[None] + parent_hot, 1.0)
    for sweep in range(max(1, (members - 1).bit_length())):
        ancestors = jnp.minimum(
            jnp.einsum("bij,bjk->bik", ancestors, ancestors, precision=lax.Precision.HIGHEST), 1.0
        )
    return ancestors


def combine_parts(first, second):
    new_max = jnp.maximum(first[0], second[0])
    first_scale = jnp.exp(first[0] - new_max)
    second_scale = jnp.exp(second[0] - new_max)
    return (
        new_max,
        first[1] * first_scale + second[1] * second_scale,
        first[2] * first_scale[..., None] + second[2] * second_scale[..., None],
        jnp.maximum(first[3], second[3]),
    )


def finish_rows(cache_max, cache_total, cache_values, last_rows, tree_max, tree_total, tree_values):
    shifted = cache_max + last_rows
    top = jnp.maximum(shifted, tree_max)
    cache_scale = jnp.exp(shifted - top)
    tree_scale = jnp.exp(tree_max - top)
    attended = (
        (cache_values * cache_scale[..., None] + tree_values * tree_scale[..., None])
        / (cache_total * cache_scale + tree_total * tree_scale)[..., None]
    ).astype(jnp.bfloat16)
    return attended.reshape(attended.shape[0], attended.shape[1] * attended.shape[2])


def per_device(
    tokens,
    gain_pre,
    w_query,
    w_key,
    w_value,
    w_forget,
    b_forget,
    w_out,
    gain_post,
    key_cache,
    value_cache,
    cum_cache,
    lengths,
    accepted,
    parent,
):
    num_seqs, proposals, model_width = tokens.shape
    kv_rank = lax.axis_index("kv")
    tp_rank = lax.axis_index("tp")
    span = key_cache.shape[1]
    heads_local = key_cache.shape[2]
    head_dim = key_cache.shape[3]
    scale = head_dim ** (-0.5)
    all_rows = num_seqs * proposals
    tok_float = tokens.astype(jnp.float32)
    normed = (
        tok_float
        * lax.rsqrt(jnp.mean(tok_float * tok_float, -1, keepdims=True) + epsilon)
        * gain_pre
    ).astype(jnp.bfloat16)
    flat = normed.reshape(all_rows, model_width)
    weight_rows = w_query.shape[0]
    local_rows = lax.dynamic_slice_in_dim(flat, kv_rank * weight_rows, weight_rows, 1)
    query_part = jnp.dot(local_rows, w_query, preferred_element_type=jnp.float32)
    key_part = jnp.dot(local_rows, w_key, preferred_element_type=jnp.float32)
    value_part = jnp.dot(local_rows, w_value, preferred_element_type=jnp.float32)
    summed = (
        lax.psum(query_part.astype(jnp.bfloat16), "kv").astype(jnp.float32),
        lax.psum(key_part.astype(jnp.bfloat16), "kv").astype(jnp.float32),
        lax.psum(value_part.astype(jnp.bfloat16), "kv").astype(jnp.float32),
    )
    query_flat = summed[0].astype(jnp.bfloat16)
    key_flat = summed[1].astype(jnp.bfloat16)
    value_flat = summed[2].astype(jnp.bfloat16)
    query = query_flat.reshape(num_seqs, proposals, heads_local, head_dim)
    key_new = key_flat.reshape(num_seqs, proposals, heads_local, head_dim)
    value_new = value_flat.reshape(num_seqs, proposals, heads_local, head_dim)
    forget_cols = lax.dynamic_slice_in_dim(w_forget, tp_rank * heads_local, heads_local, 1)
    forget_bias = lax.dynamic_slice_in_dim(b_forget, tp_rank * heads_local, heads_local, 0)
    log_forget = jax.nn.log_sigmoid(
        jnp.dot(flat, forget_cols, preferred_element_type=jnp.float32) + forget_bias
    ).reshape(num_seqs, proposals, heads_local)
    ancestors = ancestry(parent, proposals)
    path = jnp.einsum("bij,bjh->bih", ancestors, log_forget, precision=lax.Precision.HIGHEST)
    valid = lengths + accepted
    positions = kv_rank * span + jnp.arange(span, dtype=jnp.int32)
    live = (positions[None, :] < valid[:, None])[:, None, None, :]
    score = (
        jnp.einsum("bihd,bkhd->bihk", query, key_cache, preferred_element_type=jnp.float32) * scale
        + path[..., None]
        - jnp.swapaxes(cum_cache, 1, 2)[:, None]
    )
    block_max = jnp.max(jnp.where(live, score, floor_value), axis=-1)
    weight = jnp.exp(jnp.where(live, score - block_max[..., None], floor_value))
    block_total = jnp.sum(weight, axis=-1)
    block_values = jnp.einsum(
        "bihk,bkhd->bihd",
        weight.astype(jnp.bfloat16),
        value_cache,
        preferred_element_type=jnp.float32,
    )
    owner = positions[None, :] == (valid - 1)[:, None]
    candidate = jnp.max(jnp.where(owner[:, :, None], cum_cache, floor_value), axis=1)
    tree_mask = (ancestors > 0.5)[:, :, None, :]
    tree_score = (
        jnp.einsum("bihd,bjhd->bihj", query, key_new, preferred_element_type=jnp.float32) * scale
        + path[..., None]
        - jnp.swapaxes(path, 1, 2)[:, None]
    )
    tree_max = jnp.max(jnp.where(tree_mask, tree_score, floor_value), axis=-1)
    tree_weight = jnp.exp(jnp.where(tree_mask, tree_score - tree_max[..., None], floor_value))
    tree_total = jnp.sum(tree_weight, axis=-1)
    tree_values = jnp.einsum(
        "bihj,bjhd->bihd",
        tree_weight.astype(jnp.bfloat16),
        value_new,
        preferred_element_type=jnp.float32,
    )
    tree_max_rows = tree_max.reshape(all_rows, heads_local)
    tree_total_rows = tree_total.reshape(all_rows, heads_local)
    tree_values_rows = tree_values.reshape(all_rows, heads_local, head_dim)
    cache_max, cache_total, cache_values, last_cum = merged(
        (block_max, block_total, block_values, candidate), "kv", combine_parts
    )
    last_rows = jnp.broadcast_to(last_cum[:, None, :], (num_seqs, proposals, heads_local)).reshape(
        all_rows, heads_local
    )
    attended = finish_rows(
        cache_max.reshape(all_rows, heads_local),
        cache_total.reshape(all_rows, heads_local),
        cache_values.reshape(all_rows, heads_local, head_dim),
        last_rows,
        tree_max_rows,
        tree_total_rows,
        tree_values_rows,
    )
    mixed_part = jnp.dot(attended, w_out, preferred_element_type=jnp.float32)
    mixed_sum = lax.psum_scatter(
        mixed_part.astype(jnp.bfloat16), "tp", scatter_dimension=1, tiled=True
    ).astype(jnp.float32)
    squares = lax.psum(jnp.sum(mixed_sum * mixed_sum, axis=1), ("kv", "tp"))
    mixed = (mixed_sum * lax.rsqrt(squares / model_width + epsilon)[:, None] * gain_post).astype(
        jnp.bfloat16
    )
    mixed = mixed.reshape(num_seqs, proposals, mixed_sum.shape[1])
    relative = positions[None, :] - valid[:, None]
    select = relative[:, :, None] == jnp.arange(proposals, dtype=jnp.int32)[None, None, :]
    written = (relative >= 0) & (relative < proposals)
    placed_keys = jnp.einsum(
        "bkj,bjhd->bkhd", select.astype(jnp.bfloat16), key_new, preferred_element_type=jnp.float32
    ).astype(jnp.bfloat16)
    placed_values = jnp.einsum(
        "bkj,bjhd->bkhd", select.astype(jnp.bfloat16), value_new, preferred_element_type=jnp.float32
    ).astype(jnp.bfloat16)
    key_out = jnp.where(written[:, :, None, None], placed_keys, key_cache)
    value_out = jnp.where(written[:, :, None, None], placed_values, value_cache)
    cum_new = last_cum[:, None, :] + path
    placed_cum = jnp.einsum(
        "bkj,bjh->bkh", select.astype(jnp.float32), cum_new, precision=lax.Precision.HIGHEST
    )
    cum_out = jnp.where(written[:, :, None], placed_cum, cum_cache)
    return (mixed, key_out, value_out, cum_out)


MESH = pl.DeviceIdType.MESH
HI = lax.Precision.HIGHEST
F32 = jnp.float32
BF = jnp.bfloat16


def iota(shape, dim):
    return lax.broadcasted_iota(jnp.int32, shape, dim)


def hot(mask):
    return jnp.where(mask, 1.0, 0.0).astype(F32)


def dot_hi(a, b, dims=(((1,), (0,)), ((), ()))):
    return lax.dot_general(a, b, dims, precision=HI, preferred_element_type=F32)


NT = (((1,), (1,)), ((), ()))


def layer_kernel(
    n,
    nt,
    num_seqs,
    prop,
    heads,
    hd,
    span,
    tok,
    gain_h,
    wq,
    wk,
    wv,
    wft_h,
    bias_h,
    wo,
    gpost_h,
    kc,
    vc,
    cum_h,
    lens_h,
    accs_h,
    parent_h,
    mixed_out,
    kv_out,
    cum_out,
    tokv,
    normed,
    slab,
    invs,
    gain,
    wv3,
    wft,
    wov,
    gpost,
    kcv,
    vcv,
    cum,
    parent,
    bias,
    lens,
    accs,
    partq,
    rsq,
    part2,
    rs1,
    half,
    rs2,
    kvown,
    flat,
    kvflat,
    qall,
    st_send,
    val_send,
    st_recv,
    val_recv,
    cand_send,
    cand_recv,
    brow,
    anc,
    tpath,
    ptile,
    att,
    o_send,
    o_recv,
    sq_send,
    sq_recv,
    sq2_send,
    sq2_recv,
    loc,
    ssem,
    rsem,
    tssem,
    trsem,
):
    me = lax.axis_index("kv")
    mt = lax.axis_index("tp")
    rows = num_seqs * prop
    width = tok.shape[1]
    hw = heads * hd
    kdim = wq.shape[0]
    cols = heads * span
    sp = num_seqs // n
    R = sp * prop
    hp = heads * prop
    L = sp * hp
    scale = hd ** (-0.5)
    base = me * span
    heads_all = wft.shape[0]

    barrier = pltpu.get_barrier_semaphore()

    def greet(d, c):
        pl.semaphore_signal(
            barrier, inc=1, device_id={"kv": lax.rem(me + d, n)}, device_id_type=MESH
        )
        return c

    def greet_t(d, c):
        pl.semaphore_signal(
            barrier, inc=1, device_id={"tp": lax.rem(mt + d, nt)}, device_id_type=MESH
        )
        return c

    lax.fori_loop(1, n, greet, 0)
    lax.fori_loop(1, nt, greet_t, 0)

    pairs = (
        (tok, tokv),
        (gain_h, gain),
        (wq, wv3.at[0]),
        (wk, wv3.at[1]),
        (wv, wv3.at[2]),
        (cum_h, cum),
        (lens_h, lens),
        (accs_h, accs),
        (parent_h, parent),
        (bias_h, bias),
        (wft_h, wft),
        (kc, kcv),
        (vc, vcv),
        (wo, wov),
        (gpost_h, gpost),
    )
    ins = [pltpu.make_async_copy(a, b, loc.at[i]) for i, (a, b) in enumerate(pairs)]
    pieces = 4
    piece = rows // pieces
    tok_in = [
        pltpu.make_async_copy(
            tok.at[pl.ds(i * piece, piece)], tokv.at[pl.ds(i * piece, piece)], loc.at[16 + i]
        )
        for i in range(pieces)
    ]
    for c in tok_in[:1] + ins[1:2] + tok_in[1:] + ins[2:5]:
        c.start()
    par = lax.rem(me, 2)
    mate = me + 1 - 2 * par
    nh = n // 2

    def to_kv(ph, d, src, dst, sign=1):
        peer = lax.rem(me + sign * d + n, n)
        return pltpu.make_async_remote_copy(
            src_ref=src,
            dst_ref=dst,
            send_sem=ssem.at[ph, d],
            recv_sem=rsem.at[ph, d],
            device_id={"kv": peer},
            device_id_type=MESH,
        )

    def to_tp(ph, d, src, dst):
        peer = lax.rem(mt + d, nt)
        return pltpu.make_async_remote_copy(
            src_ref=src,
            dst_ref=dst,
            send_sem=tssem.at[ph, d],
            recv_sem=trsem.at[ph, d],
            device_id={"tp": peer},
            device_id_type=MESH,
        )

    def up(d):
        return lax.rem(me + d, n)

    def down(d):
        return lax.rem(me - d + n, n)

    def rrow(i):
        return pl.ds(pl.multiple_of(i * R, R), R)

    def lrow(i):
        return pl.ds(pl.multiple_of(i * L, L), L)

    def to_peer(ph, d, peer, src, dst):
        return pltpu.make_async_remote_copy(
            src_ref=src,
            dst_ref=dst,
            send_sem=ssem.at[ph, d],
            recv_sem=rsem.at[ph, d],
            device_id={"kv": peer},
            device_id_type=MESH,
        )

    def rsq_copy(d):
        return to_kv(0, d, partq.at[rrow(up(d))], rsq.at[d])

    def rs1_copy():
        return to_peer(1, 0, mate, part2.at[1 - par], rs1)

    def rs2_copy(e):
        peer = up(2 * e)
        return to_peer(2, e, peer, half.at[peer // 2], rs2.at[e])

    def gather_along(ph, e, view):
        return to_peer(ph, 2 * e, up(2 * e), view(me), view(me))

    def gather_mate(ph, e, view):
        c = down(2 * e)
        return to_peer(ph, 2 * e + 1, mate, view(c), view(c))

    def gather_start(ph, view):
        each(nh, lambda e: gather_along(ph, e, view).start())
        gather_mate(ph, 0, view).start()

    def gather_pass(ph, view):
        def one(e):
            c = down(2 * e)
            to_peer(ph, 2 * e, me, view(c), view(c)).wait_recv()
            gather_mate(ph, e, view).start()

        each(nh, one)

    def mate_chunk(e):
        return lax.rem(mate - 2 * e + n, n)

    def gather_wait(ph, e, view):
        c = mate_chunk(e)
        to_peer(ph, 2 * e + 1, mate, view(c), view(c)).wait_recv()

    def gather_drain(ph, view):
        each(nh, lambda e: gather_along(ph, e, view).wait_send())
        for e in range(nh):
            gather_mate(ph, e, view).wait_send()

    def q_view(c):
        return qall.at[rrow(c)]

    def k_view(c):
        return kvflat.at[0, lrow(c)]

    def v_view(c):
        return kvflat.at[1, lrow(c)]

    def att_view(c):
        return att.at[rrow(c)]

    def stat_copy(d):
        return to_kv(6, d, st_send.at[d], st_recv.at[d], -1)

    def val_copy(d):
        return to_kv(7, d, val_send.at[d], val_recv.at[d], -1)

    def cand_copy(d):
        return to_kv(8, d, cand_send, cand_recv.at[d])

    def sq_copy(d):
        return to_kv(10, d, sq_send, sq_recv.at[d])

    def each(count, fn):
        def body(d, c):
            fn(d)
            return c

        lax.fori_loop(1, count, body, 0)

    nb = min(2 * prop, piece)
    mine = pl.ds(pl.multiple_of(me * kdim, kdim), kdim)
    ins[1].wait()

    def norm_rows(i, c):
        sl = pl.ds(pl.multiple_of(i * nb, nb), nb)
        t = tokv[sl, :].astype(F32)
        inv = lax.rsqrt(jnp.mean(t * t, axis=-1, keepdims=True) + epsilon)
        invs[sl, :] = jnp.broadcast_to(inv, (nb, 128))
        slab[sl, :] = (tokv[sl, mine].astype(F32) * inv * gain[:, mine]).astype(BF)
        return c

    for p in range(pieces):
        tok_in[p].wait()
        lax.fori_loop(p * piece // nb, (p + 1) * piece // nb, norm_rows, 0)
    for c in ins[5:]:
        c.start()
    local = slab[...]
    pl.semaphore_wait(barrier, n - 1 + nt - 1)
    ins[2].wait()
    partq[...] = jnp.dot(local, wv3[0], preferred_element_type=F32).astype(BF)
    each(n, lambda d: rsq_copy(d).start())
    for i in range(2):
        ins[3 + i].wait()
        both_rows = jnp.dot(local, wv3[1 + i], preferred_element_type=F32).astype(BF)
        for c in range(n):
            part2[c % 2, c // 2, :, i * hw : (i + 1) * hw] = both_rows[c * R : (c + 1) * R]
    def norm_rest(i, c):
        sl = pl.ds(pl.multiple_of(i * nb, nb), nb)
        inv = invs[sl, 0:1]
        normed[sl, :] = (tokv[sl, :].astype(F32) * inv * gain[...]).astype(BF)
        return c

    lax.fori_loop(0, rows // nb, norm_rest, 0)
    for c in ins[5:11]:
        c.wait()

    r64 = num_seqs * heads
    c64 = cum[...]
    srow = iota((r64, span), 0) // heads
    lane = iota((r64, span), 1)
    rel64 = jnp.zeros((r64, span), jnp.int32)
    rel16 = jnp.zeros((num_seqs, cols), jnp.int32)
    s16 = iota((num_seqs, cols), 0)
    for s in range(num_seqs):
        rel_s = lens[s] + accs[s] - base
        rel64 = jnp.where(srow == s, rel_s, rel64)
        rel16 = jnp.where(s16 == s, rel_s, rel16)
    cand = jnp.max(jnp.where(lane == rel64 - 1, c64, floor_value), axis=1, keepdims=True)
    diag = iota((r64, 128), 0) == iota((r64, 128), 1)
    cand_lane = jnp.sum(jnp.where(diag, cand, 0.0), axis=0, keepdims=True)
    cand_send[...] = jnp.broadcast_to(cand_lane, (8, 128))
    each(n, lambda d: cand_copy(d).start())

    spread = hot(iota((span, cols), 1) // heads == iota((span, cols), 0))
    e1 = dot_hi(c64, spread)
    e1 = jnp.where(iota((r64, cols), 0) % heads == iota((r64, cols), 1) % heads, e1, 0.0)
    take = hot(iota((num_seqs, r64), 1) // heads == iota((num_seqs, r64), 0))
    cflat = dot_hi(take, e1)
    brow[...] = jnp.where(iota((num_seqs, cols), 1) // heads < rel16, -cflat, floor_value)

    ri = iota((rows, rows), 0)
    ci = iota((rows, rows), 1)
    pick = hot(iota((rows, num_seqs), 0) // prop == iota((rows, num_seqs), 1))
    pb = dot_hi(pick, parent[...].astype(F32))
    pcol = jnp.sum(
        jnp.where(iota((rows, prop), 1) == iota((rows, prop), 0) % prop, pb, 0.0),
        axis=1,
        keepdims=True,
    )
    target = jnp.where(pcol >= 0.0, (ri // prop * prop).astype(F32) + pcol, -1.0)
    a = jnp.where((ri == ci) | (ci.astype(F32) == target), 1.0, 0.0)
    for sweep in range(max(1, (prop - 1).bit_length())):
        low = a.astype(BF)
        a = jnp.minimum(jnp.dot(low, low, preferred_element_type=F32), 1.0)
    anc[...] = a
    lf = lax.dot_general(wft[...], normed[...], NT, preferred_element_type=F32)
    bcol = jnp.zeros((heads_all, rows), F32)
    for h in range(heads_all):
        bcol = jnp.where(iota((heads_all, rows), 0) == h, bias[h], bcol)
    z = lf + bcol
    lf = jnp.minimum(z, 0.0) - jnp.log1p(jnp.exp(-jnp.abs(z)))
    path_t = dot_hi(lf, a, NT)
    rep = hot(iota((r64, heads_all), 1) == mt * heads + iota((r64, heads_all), 0) % heads)
    pm = dot_hi(rep, path_t)
    pm = jnp.where(iota((r64, rows), 1) // prop == iota((r64, rows), 0) // heads, pm, 0.0)
    fold = hot(iota((rows, 128), 0) % prop == iota((rows, 128), 1) % prop)
    pt = dot_hi(pm, fold)
    ptile[...] = pt
    ptm = jnp.where((iota((r64, 128), 1) // prop) % heads == iota((r64, 128), 0) % heads, pt, 0.0)
    tpath[...] = dot_hi(take, ptm)

    own_q = partq[rrow(me)].astype(F32)
    for d in range(1, n):
        rsq_copy(d).wait_recv()
        own_q = own_q + rsq[d].astype(F32)
    qall[rrow(me)] = own_q.astype(BF)
    gather_start(3, q_view)
    rs1_copy().start()

    ins[11].wait()
    ins[12].wait()
    same_head = iota((hp, cols), 0) // prop == iota((hp, cols), 1) % heads
    diag_l = iota((L, L), 0) == iota((L, L), 1)

    def heads_of(block):
        return jnp.concatenate([block[:, h * hd : (h + 1) * hd] for h in range(heads)], axis=0)

    def block_part(src):
        maxes, totals, values = [], [], []
        for j in range(sp):
            s = src * sp + j
            q = heads_of(qall[pl.ds(pl.multiple_of(s * prop, prop), prop), :])
            sc = lax.dot_general(q, kcv[s], NT, preferred_element_type=F32) * scale
            sc = jnp.where(same_head, sc + brow[pl.ds(s, 1), :], floor_value)
            m = jnp.max(sc, axis=1, keepdims=True)
            w = jnp.exp(sc - m)
            maxes.append(m)
            totals.append(jnp.sum(w, axis=1, keepdims=True))
            values.append(
                jnp.dot(w.astype(BF), vcv[s], preferred_element_type=F32).astype(BF)
            )
        m = jnp.concatenate(maxes, axis=0)
        t = jnp.concatenate(totals, axis=0)
        m_lane = jnp.sum(jnp.where(diag_l, m, 0.0), axis=0, keepdims=True)
        t_lane = jnp.sum(jnp.where(diag_l, t, 0.0), axis=0, keepdims=True)
        stats = jnp.where(iota((8, L), 0) == 0, m_lane, t_lane)
        return stats, jnp.concatenate(values, axis=0)

    def remote_block(d):
        src = down(d)
        stats, values = block_part(src)
        st_send[d] = stats
        val_send[d] = values
        stat_copy(d).start()
        val_copy(d).start()

    stats, values = block_part(me)
    st_recv[0] = stats
    val_recv[0] = values
    gather_pass(3, q_view)
    each(nh, lambda e: remote_block(2 * e))
    rs1_copy().wait_recv()
    for i in range(nh):
        half[i] = (part2[par, i].astype(F32) + rs1[i].astype(F32)).astype(BF)
    each(nh, lambda e: rs2_copy(e).start())

    def mate_block(e, c):
        gather_wait(3, e, q_view)
        remote_block(lax.rem(me - mate_chunk(e) + n, n))
        return c

    lax.fori_loop(0, nh, mate_block, 0)
    own_kv = half[me // 2].astype(F32)
    for e in range(1, nh):
        rs2_copy(e).wait_recv()
        own_kv = own_kv + rs2[e].astype(F32)
    kvown[...] = own_kv.astype(BF)
    for i in range(2):
        for h in range(heads):
            flat[pl.ds(h, R, stride=heads), :] = own_kv[:, i * hw + h * hd : i * hw + (h + 1) * hd]
        kvflat[i, lrow(me)] = flat[...].astype(BF)
    gather_start(5, k_view)

    fold_h = iota((rows, hp), 0)
    tmax, ttot, tval = [], [], []
    for j in range(sp):
        s = me * sp + j
        q = heads_of(qall[pl.ds(pl.multiple_of(s * prop, prop), prop), :])
        k = heads_of(kvown[j * prop : (j + 1) * prop, 0:hw])
        v = heads_of(kvown[j * prop : (j + 1) * prop, hw : 2 * hw])
        arows = anc[pl.ds(pl.multiple_of(s * prop, prop), prop), :]
        sel = hot(fold_h == s * prop + iota((rows, hp), 1) % prop).astype(BF)
        am = jnp.dot(arows.astype(BF), sel, preferred_element_type=F32)
        am = jnp.concatenate([am] * heads, axis=0)
        mask = (am > 0.5) & (iota((hp, hp), 0) // prop == iota((hp, hp), 1) // prop)
        sc = lax.dot_general(q, k, NT, preferred_element_type=F32) * scale
        sc = jnp.where(mask, sc - tpath[pl.ds(s, 1), 0:hp], floor_value)
        m = jnp.max(sc, axis=1, keepdims=True)
        w = jnp.where(mask, jnp.exp(sc - m), 0.0)
        tmax.append(m)
        ttot.append(jnp.sum(w, axis=1, keepdims=True))
        tval.append(jnp.dot(w.astype(BF), v, preferred_element_type=F32))
    tree_max = jnp.concatenate(tmax, axis=0)
    tree_tot = jnp.concatenate(ttot, axis=0)
    tree_val = jnp.concatenate(tval, axis=0)

    last_lane = cand_send[...]
    for d in range(1, n):
        cand_copy(d).wait_recv()
        last_lane = jnp.maximum(last_lane, cand_recv[d])
    last_col = jnp.sum(jnp.where(diag, last_lane[0:1], 0.0), axis=1, keepdims=True)
    own_rows = iota((L, 128), 0)
    own_pick = iota((L, 128), 1) == (me * sp + own_rows // hp) * heads + (own_rows % hp) // prop
    last_own = jnp.sum(jnp.where(own_pick, last_lane[0:1], 0.0), axis=1, keepdims=True)

    shifted_path = ptile[...]
    for b in range((span - 1).bit_length()):
        moved = pltpu.roll(shifted_path, 1 << b, 1)
        shifted_path = jnp.where((rel64 >> b) & 1 == 1, moved, shifted_path)
    off = lane - rel64
    cum_out[...] = jnp.where((off >= 0) & (off < prop), last_col + shifted_path, cum[...])

    for d in range(1, n):
        stat_copy(d).wait_recv()
    top = st_recv[0]
    for d in range(1, n):
        top = jnp.maximum(top, st_recv[d])
    top = top[0:1]

    def col(x):
        return jnp.sum(jnp.where(diag_l, x, 0.0), axis=1, keepdims=True)

    cache_tot = jnp.zeros((1, L), F32)
    scales = []
    for d in range(n):
        sd = jnp.exp(st_recv[d, 0:1] - top)
        scales.append(col(sd))
        cache_tot = cache_tot + st_recv[d, 1:2] * sd
    shifted = col(top) + last_own
    both = jnp.maximum(shifted, tree_max)
    cscale = jnp.exp(shifted - both)
    tscale = jnp.exp(tree_max - both)
    denom = col(cache_tot) * cscale + tree_tot * tscale
    vals = jnp.zeros((L, hd), F32)
    for d in range(n):
        if d > 0:
            val_copy(d).wait_recv()
        vals = vals + val_recv[d].astype(F32) * scales[d]
    attended = ((vals * cscale + tree_val * tscale) / denom).astype(BF)
    for j in range(sp):
        for h in range(heads):
            att[pl.ds(pl.multiple_of(me * R + j * prop, prop), prop), h * hd : (h + 1) * hd] = (
                attended[j * hp + h * prop : j * hp + (h + 1) * prop]
            )
    gather_start(4, att_view)
    gather_start(11, v_view)
    ins[13].wait()
    ins[14].wait()
    gather_pass(5, k_view)
    gather_pass(4, att_view)
    for e in range(nh):
        gather_wait(4, e, att_view)
    full = jnp.dot(att[...], wov[...], preferred_element_type=F32).astype(BF)
    oc = o_send.shape[2]
    for t in range(nt):
        o_send[t] = full[:, t * oc : (t + 1) * oc]

    def o_copy(d):
        return to_tp(0, d, o_send.at[lax.rem(mt + d, nt)], o_recv.at[d])

    def sq2_copy(d):
        return to_tp(1, d, sq2_send, sq2_recv.at[d])

    each(nt, lambda d: o_copy(d).start())
    gather_pass(11, v_view)
    mixed = o_send[mt].astype(F32)
    for d in range(1, nt):
        o_copy(d).wait_recv()
        mixed = mixed + o_recv[d].astype(F32)
    sq_send[...] = dot_hi(jnp.ones((8, oc), F32), mixed * mixed, NT)[0:1]
    each(n, lambda d: sq_copy(d).start())
    sq = sq_send[...]
    for d in range(1, n):
        sq_copy(d).wait_recv()
        sq = sq + sq_recv[d]
    sq2_send[...] = sq
    each(nt, lambda d: sq2_copy(d).start())
    for e in range(nh):
        gather_wait(5, e, k_view)
        gather_wait(11, e, v_view)
    out_kv = pltpu.make_async_copy(kvflat, kv_out, loc.at[15])
    out_kv.start()
    for d in range(1, nt):
        sq2_copy(d).wait_recv()
        sq = sq + sq2_recv[d]
    ssum = dot_hi(jnp.broadcast_to(sq, (8, rows)), jnp.full((8, oc), 0.125, F32), (((0,), (0,)), ((), ())))
    mixed_out[...] = (mixed * lax.rsqrt(ssum / width + epsilon) * gpost[...]).astype(BF)

    def drain(d):
        rsq_copy(d).wait_send()
        stat_copy(d).wait_send()
        val_copy(d).wait_send()
        cand_copy(d).wait_send()
        sq_copy(d).wait_send()

    each(n, drain)
    rs1_copy().wait_send()
    each(nh, lambda e: rs2_copy(e).wait_send())
    gather_drain(3, q_view)
    gather_drain(4, att_view)
    gather_drain(5, k_view)
    gather_drain(11, v_view)

    def drain_t(d):
        o_copy(d).wait_send()
        sq2_copy(d).wait_send()

    each(nt, drain_t)
    out_kv.wait()


def write_kernel(
    num_seqs,
    prop,
    span,
    kc,
    vc,
    kv_new,
    mixed,
    cum,
    lens_h,
    accs_h,
    k_out,
    v_out,
    mixed_out,
    cum_out,
    buf,
    fresh,
    lens,
    accs,
    sem,
    sin,
    sout,
):
    base = lax.axis_index("kv") * span
    small = [
        pltpu.make_async_copy(lens_h, lens, sem.at[0]),
        pltpu.make_async_copy(accs_h, accs, sem.at[1]),
        pltpu.make_async_copy(kv_new, fresh, sem.at[2]),
        pltpu.make_async_copy(mixed, mixed_out, sem.at[3]),
        pltpu.make_async_copy(cum, cum_out, sem.at[4]),
    ]
    cut = sin.shape[1]
    step = num_seqs // cut
    arrays = ((kc, k_out), (vc, v_out))

    def part(c):
        return pl.ds(c * step, step)

    def come(c, i):
        return pltpu.make_async_copy(arrays[i][0].at[part(c)], buf.at[i, part(c)], sin.at[i, c])

    def leave(c, i):
        return pltpu.make_async_copy(buf.at[i, part(c)], arrays[i][1].at[part(c)], sout.at[i, c])

    for c in small[:3]:
        c.start()
    for c in range(cut):
        for i in range(2):
            come(c, i).start()
    for c in small[3:]:
        c.start()
    for c in small[:3]:
        c.wait()

    def place(i, s):
        rel = lens[s] + accs[s] - base
        whole = (rel >= 0) & (rel <= span - prop)
        partly = (rel > -prop) & (rel < span) & jnp.logical_not(whole)

        @pl.when(whole)
        def _():
            buf[i, s, pl.ds(rel, prop)] = fresh[i, s]

        @pl.when(partly)
        def _():
            def one(j, c):
                buf[i, s, pl.ds(rel + j, 1)] = fresh[i, s, pl.ds(j, 1)]
                return c

            lax.fori_loop(jnp.maximum(-rel, 0), jnp.minimum(span - rel, prop), one, 0)

    for c in range(cut):
        for i in range(2):
            come(c, i).wait()
            for s in range(c * step, (c + 1) * step):
                place(i, s)
            leave(c, i).start()
    for c in range(cut):
        for i in range(2):
            leave(c, i).wait()
    for c in small[3:]:
        c.wait()


def fast_device(
    n,
    nt,
    tokens,
    gain_pre,
    w_query,
    w_key,
    w_value,
    w_forget,
    b_forget,
    w_out,
    gain_post,
    key_cache,
    value_cache,
    cum_cache,
    lengths,
    accepted,
    parent,
):
    num_seqs, prop, width = tokens.shape
    span, heads, hd = key_cache.shape[1:]
    rows = num_seqs * prop
    hw = heads * hd
    cols = heads * span
    sp = num_seqs // n
    R = sp * prop
    L = sp * heads * prop
    oc = gain_post.shape[0]
    kc = key_cache.reshape(num_seqs, cols, hd)
    vc = value_cache.reshape(num_seqs, cols, hd)
    cum = jnp.swapaxes(cum_cache, 1, 2).reshape(num_seqs * heads, span)
    vmem = pl.BlockSpec(memory_space=pltpu.VMEM)
    V = pltpu.VMEM
    D = pltpu.SemaphoreType.DMA
    hbm = pl.BlockSpec(memory_space=pltpu.HBM)
    S = pltpu.SMEM
    nh = n // 2
    mixed, kv_new, cum_new = pl.pallas_call(
        functools.partial(layer_kernel, n, nt, num_seqs, prop, heads, hd, span),
        out_shape=(
            jax.ShapeDtypeStruct((rows, oc), BF),
            jax.ShapeDtypeStruct((2, rows * heads, hd), BF),
            jax.ShapeDtypeStruct(cum.shape, F32),
        ),
        in_specs=[hbm] * 15,
        out_specs=(vmem, hbm, vmem),
        scratch_shapes=[
            V((rows, width), BF),
            V((rows, width), BF),
            V((rows, w_query.shape[0]), BF),
            V((rows, 128), F32),
            V((1, width), F32),
            V((3,) + w_query.shape, BF),
            V(w_forget.T.shape, BF),
            V(w_out.shape, BF),
            V((1, oc), F32),
            V(kc.shape, BF),
            V(vc.shape, BF),
            V(cum.shape, F32),
            V(parent.shape, jnp.int32),
            S(b_forget.shape, F32),
            S(lengths.shape, jnp.int32),
            S(accepted.shape, jnp.int32),
            V((rows, hw), BF),
            V((n, R, hw), BF),
            V((2, nh, R, 2 * hw), BF),
            V((nh, R, 2 * hw), BF),
            V((nh, R, 2 * hw), BF),
            V((nh, R, 2 * hw), BF),
            V((R, 2 * hw), BF),
            V((L, hd), F32),
            V((2, rows * heads, hd), BF),
            V((rows, hw), BF),
            V((n, 8, L), F32),
            V((n, L, hd), BF),
            V((n, 8, L), F32),
            V((n, L, hd), BF),
            V((8, 128), F32),
            V((n, 8, 128), F32),
            V((num_seqs, cols), F32),
            V((rows, rows), F32),
            V((num_seqs, 128), F32),
            V((num_seqs * heads, 128), F32),
            V((rows, hw), BF),
            V((nt, rows, oc), BF),
            V((nt, rows, oc), BF),
            V((1, rows), F32),
            V((n, 1, rows), F32),
            V((1, rows), F32),
            V((nt, 1, rows), F32),
            D((20,)),
            D((12, n)),
            D((12, n)),
            D((2, nt)),
            D((2, nt)),
        ],
        compiler_params=pltpu.CompilerParams(
            collective_id=0, has_side_effects=True, vmem_limit_bytes=67043328
        ),
        name="layer",
    )(
        tokens.reshape(rows, width),
        gain_pre.reshape(1, width),
        w_query,
        w_key,
        w_value,
        w_forget.T,
        b_forget,
        w_out,
        gain_post.reshape(1, oc),
        kc,
        vc,
        cum,
        lengths,
        accepted,
        parent,
    )
    key_out, value_out, mixed, cum_new = pl.pallas_call(
        functools.partial(write_kernel, num_seqs, prop, span),
        out_shape=(
            jax.ShapeDtypeStruct(key_cache.shape, BF),
            jax.ShapeDtypeStruct(value_cache.shape, BF),
            jax.ShapeDtypeStruct(mixed.shape, BF),
            jax.ShapeDtypeStruct(cum_new.shape, F32),
        ),
        in_specs=[hbm] * 7,
        out_specs=(hbm,) * 4,
        scratch_shapes=[
            V((2,) + key_cache.shape, BF),
            V((2, num_seqs, prop, heads, hd), BF),
            S(lengths.shape, jnp.int32),
            S(accepted.shape, jnp.int32),
            D((5,)),
            D((2, 4)),
            D((2, 4)),
        ],
        compiler_params=pltpu.CompilerParams(vmem_limit_bytes=67043328),
        name="cache_write",
    )(
        key_cache,
        value_cache,
        kv_new.reshape(2, num_seqs, prop, heads, hd),
        mixed,
        cum_new,
        lengths,
        accepted,
    )
    cum_out = jnp.swapaxes(cum_new.reshape(num_seqs, heads, span), 1, 2)
    return (
        mixed.reshape(num_seqs, prop, oc),
        key_out,
        value_out,
        cum_out,
    )


def choose(mesh):
    n, nt = mesh.shape["kv"], mesh.shape["tp"]

    def body(*args):
        tokens, key_cache = args[0], args[9]
        num_seqs, prop = tokens.shape[:2]
        span, heads = key_cache.shape[1:3]
        fits = (
            num_seqs % n == 0
            and n % 2 == 0
            and num_seqs % 4 == 0
            and (num_seqs // n) * heads * prop == 128
            and span == 128
            and num_seqs * heads <= 128
            and prop % 16 == 0
        )
        if fits:
            return fast_device(n, nt, *args)
        return per_device(*args)

    return body


def solution(mesh):
    return jax.shard_map(
        choose(mesh),
        mesh=mesh,
        in_specs=(
            P(),
            P(),
            P("kv", "tp"),
            P("kv", "tp"),
            P("kv", "tp"),
            P(),
            P(),
            P("tp", "kv"),
            P(("kv", "tp")),
            P(None, "kv", "tp", None),
            P(None, "kv", "tp", None),
            P(None, "kv", "tp"),
            P(),
            P(),
            P(),
        ),
        out_specs=(
            P(None, None, ("kv", "tp")),
            P(None, "kv", "tp", None),
            P(None, "kv", "tp", None),
            P(None, "kv", "tp"),
        ),
        check_vma=False,
    )
```

```python
import functools

import jax
import jax.numpy as jnp
from jax import lax
from jax.experimental import pallas as pl
from jax.experimental.pallas import tpu as pltpu
from jax.sharding import PartitionSpec as P

epsilon = 1e-06
floor_value = -1e30


def merged(part, axis, combine):
    gathered = jax.tree.map(lambda a: lax.all_gather(a, axis), part)

    def take(source):
        return jax.tree.map(lambda a: lax.dynamic_index_in_dim(a, source, 0, False), gathered)

    return lax.fori_loop(
        1, lax.axis_size(axis), lambda source, state: combine(state, take(source)), take(0)
    )


def ancestry(parent_ids, members):
    identity = jnp.eye(members, dtype=jnp.float32)
    parent_hot = (
        parent_ids[:, :, None] == jnp.arange(members, dtype=jnp.int32)[None, None, :]
    ).astype(jnp.float32)
    ancestors = jnp.minimum(identity[None] + parent_hot, 1.0)
    for sweep in range(max(1, (members - 1).bit_length())):
        ancestors = jnp.minimum(
            jnp.einsum("bij,bjk->bik", ancestors, ancestors, precision=lax.Precision.HIGHEST), 1.0
        )
    return ancestors


def combine_parts(first, second):
    new_max = jnp.maximum(first[0], second[0])
    first_scale = jnp.exp(first[0] - new_max)
    second_scale = jnp.exp(second[0] - new_max)
    return (
        new_max,
        first[1] * first_scale + second[1] * second_scale,
        first[2] * first_scale[..., None] + second[2] * second_scale[..., None],
        jnp.maximum(first[3], second[3]),
    )


def finish_rows(cache_max, cache_total, cache_values, last_rows, tree_max, tree_total, tree_values):
    shifted = cache_max + last_rows
    top = jnp.maximum(shifted, tree_max)
    cache_scale = jnp.exp(shifted - top)
    tree_scale = jnp.exp(tree_max - top)
    attended = (
        (cache_values * cache_scale[..., None] + tree_values * tree_scale[..., None])
        / (cache_total * cache_scale + tree_total * tree_scale)[..., None]
    ).astype(jnp.bfloat16)
    return attended.reshape(attended.shape[0], attended.shape[1] * attended.shape[2])


def per_device(
    tokens,
    gain_pre,
    w_query,
    w_key,
    w_value,
    w_forget,
    b_forget,
    w_out,
    gain_post,
    key_cache,
    value_cache,
    cum_cache,
    lengths,
    accepted,
    parent,
):
    num_seqs, proposals, model_width = tokens.shape
    kv_rank = lax.axis_index("kv")
    tp_rank = lax.axis_index("tp")
    span = key_cache.shape[1]
    heads_local = key_cache.shape[2]
    head_dim = key_cache.shape[3]
    scale = head_dim ** (-0.5)
    all_rows = num_seqs * proposals
    tok_float = tokens.astype(jnp.float32)
    normed = (
        tok_float
        * lax.rsqrt(jnp.mean(tok_float * tok_float, -1, keepdims=True) + epsilon)
        * gain_pre
    ).astype(jnp.bfloat16)
    flat = normed.reshape(all_rows, model_width)
    weight_rows = w_query.shape[0]
    local_rows = lax.dynamic_slice_in_dim(flat, kv_rank * weight_rows, weight_rows, 1)
    query_part = jnp.dot(local_rows, w_query, preferred_element_type=jnp.float32)
    key_part = jnp.dot(local_rows, w_key, preferred_element_type=jnp.float32)
    value_part = jnp.dot(local_rows, w_value, preferred_element_type=jnp.float32)
    summed = (
        lax.psum(query_part.astype(jnp.bfloat16), "kv").astype(jnp.float32),
        lax.psum(key_part.astype(jnp.bfloat16), "kv").astype(jnp.float32),
        lax.psum(value_part.astype(jnp.bfloat16), "kv").astype(jnp.float32),
    )
    query_flat = summed[0].astype(jnp.bfloat16)
    key_flat = summed[1].astype(jnp.bfloat16)
    value_flat = summed[2].astype(jnp.bfloat16)
    query = query_flat.reshape(num_seqs, proposals, heads_local, head_dim)
    key_new = key_flat.reshape(num_seqs, proposals, heads_local, head_dim)
    value_new = value_flat.reshape(num_seqs, proposals, heads_local, head_dim)
    forget_cols = lax.dynamic_slice_in_dim(w_forget, tp_rank * heads_local, heads_local, 1)
    forget_bias = lax.dynamic_slice_in_dim(b_forget, tp_rank * heads_local, heads_local, 0)
    log_forget = jax.nn.log_sigmoid(
        jnp.dot(flat, forget_cols, preferred_element_type=jnp.float32) + forget_bias
    ).reshape(num_seqs, proposals, heads_local)
    ancestors = ancestry(parent, proposals)
    path = jnp.einsum("bij,bjh->bih", ancestors, log_forget, precision=lax.Precision.HIGHEST)
    valid = lengths + accepted
    positions = kv_rank * span + jnp.arange(span, dtype=jnp.int32)
    live = (positions[None, :] < valid[:, None])[:, None, None, :]
    score = (
        jnp.einsum("bihd,bkhd->bihk", query, key_cache, preferred_element_type=jnp.float32) * scale
        + path[..., None]
        - jnp.swapaxes(cum_cache, 1, 2)[:, None]
    )
    block_max = jnp.max(jnp.where(live, score, floor_value), axis=-1)
    weight = jnp.exp(jnp.where(live, score - block_max[..., None], floor_value))
    block_total = jnp.sum(weight, axis=-1)
    block_values = jnp.einsum(
        "bihk,bkhd->bihd",
        weight.astype(jnp.bfloat16),
        value_cache,
        preferred_element_type=jnp.float32,
    )
    owner = positions[None, :] == (valid - 1)[:, None]
    candidate = jnp.max(jnp.where(owner[:, :, None], cum_cache, floor_value), axis=1)
    tree_mask = (ancestors > 0.5)[:, :, None, :]
    tree_score = (
        jnp.einsum("bihd,bjhd->bihj", query, key_new, preferred_element_type=jnp.float32) * scale
        + path[..., None]
        - jnp.swapaxes(path, 1, 2)[:, None]
    )
    tree_max = jnp.max(jnp.where(tree_mask, tree_score, floor_value), axis=-1)
    tree_weight = jnp.exp(jnp.where(tree_mask, tree_score - tree_max[..., None], floor_value))
    tree_total = jnp.sum(tree_weight, axis=-1)
    tree_values = jnp.einsum(
        "bihj,bjhd->bihd",
        tree_weight.astype(jnp.bfloat16),
        value_new,
        preferred_element_type=jnp.float32,
    )
    tree_max_rows = tree_max.reshape(all_rows, heads_local)
    tree_total_rows = tree_total.reshape(all_rows, heads_local)
    tree_values_rows = tree_values.reshape(all_rows, heads_local, head_dim)
    cache_max, cache_total, cache_values, last_cum = merged(
        (block_max, block_total, block_values, candidate), "kv", combine_parts
    )
    last_rows = jnp.broadcast_to(last_cum[:, None, :], (num_seqs, proposals, heads_local)).reshape(
        all_rows, heads_local
    )
    attended = finish_rows(
        cache_max.reshape(all_rows, heads_local),
        cache_total.reshape(all_rows, heads_local),
        cache_values.reshape(all_rows, heads_local, head_dim),
        last_rows,
        tree_max_rows,
        tree_total_rows,
        tree_values_rows,
    )
    mixed_part = jnp.dot(attended, w_out, preferred_element_type=jnp.float32)
    mixed_sum = lax.psum_scatter(
        mixed_part.astype(jnp.bfloat16), "tp", scatter_dimension=1, tiled=True
    ).astype(jnp.float32)
    squares = lax.psum(jnp.sum(mixed_sum * mixed_sum, axis=1), ("kv", "tp"))
    mixed = (mixed_sum * lax.rsqrt(squares / model_width + epsilon)[:, None] * gain_post).astype(
        jnp.bfloat16
    )
    mixed = mixed.reshape(num_seqs, proposals, mixed_sum.shape[1])
    relative = positions[None, :] - valid[:, None]
    select = relative[:, :, None] == jnp.arange(proposals, dtype=jnp.int32)[None, None, :]
    written = (relative >= 0) & (relative < proposals)
    placed_keys = jnp.einsum(
        "bkj,bjhd->bkhd", select.astype(jnp.bfloat16), key_new, preferred_element_type=jnp.float32
    ).astype(jnp.bfloat16)
    placed_values = jnp.einsum(
        "bkj,bjhd->bkhd", select.astype(jnp.bfloat16), value_new, preferred_element_type=jnp.float32
    ).astype(jnp.bfloat16)
    key_out = jnp.where(written[:, :, None, None], placed_keys, key_cache)
    value_out = jnp.where(written[:, :, None, None], placed_values, value_cache)
    cum_new = last_cum[:, None, :] + path
    placed_cum = jnp.einsum(
        "bkj,bjh->bkh", select.astype(jnp.float32), cum_new, precision=lax.Precision.HIGHEST
    )
    cum_out = jnp.where(written[:, :, None], placed_cum, cum_cache)
    return (mixed, key_out, value_out, cum_out)


MESH = pl.DeviceIdType.MESH
HI = lax.Precision.HIGHEST
F32 = jnp.float32
BF = jnp.bfloat16


def iota(shape, dim):
    return lax.broadcasted_iota(jnp.int32, shape, dim)


def hot(mask):
    return jnp.where(mask, 1.0, 0.0).astype(F32)


def dot_hi(a, b, dims=(((1,), (0,)), ((), ()))):
    return lax.dot_general(a, b, dims, precision=HI, preferred_element_type=F32)


NT = (((1,), (1,)), ((), ()))


def layer_kernel(
    n,
    nt,
    num_seqs,
    prop,
    heads,
    hd,
    span,
    tok,
    gain_h,
    wq,
    wk,
    wv,
    wft_h,
    bias_h,
    wo,
    gpost_h,
    kc,
    vc,
    cum_h,
    lens_h,
    accs_h,
    parent_h,
    mixed_out,
    kv_out,
    cum_out,
    tokv,
    normed,
    slab,
    invs,
    gain,
    wv3,
    wft,
    wov,
    gpost,
    kcv,
    vcv,
    cum,
    parent,
    bias,
    lens,
    accs,
    partq,
    rsq,
    part2,
    rs1,
    half,
    rs2,
    kvown,
    flat,
    kvflat,
    qall,
    st_send,
    val_send,
    st_recv,
    val_recv,
    cand_send,
    cand_recv,
    brow,
    anc,
    tpath,
    ptile,
    att,
    o_send,
    o_recv,
    sq_send,
    sq_recv,
    sq2_send,
    sq2_recv,
    loc,
    ssem,
    rsem,
    tssem,
    trsem,
):
    me = lax.axis_index("kv")
    mt = lax.axis_index("tp")
    rows = num_seqs * prop
    width = tok.shape[1]
    hw = heads * hd
    kdim = wq.shape[0]
    cols = heads * span
    sp = num_seqs // n
    R = sp * prop
    hp = heads * prop
    L = sp * hp
    scale = hd ** (-0.5)
    base = me * span
    heads_all = wft.shape[0]

    barrier = pltpu.get_barrier_semaphore()

    def greet(d, c):
        pl.semaphore_signal(
            barrier, inc=1, device_id={"kv": lax.rem(me + d, n)}, device_id_type=MESH
        )
        return c

    def greet_t(d, c):
        pl.semaphore_signal(
            barrier, inc=1, device_id={"tp": lax.rem(mt + d, nt)}, device_id_type=MESH
        )
        return c

    lax.fori_loop(1, n, greet, 0)
    lax.fori_loop(1, nt, greet_t, 0)

    pairs = (
        (tok, tokv),
        (gain_h, gain),
        (wq, wv3.at[0]),
        (wk, wv3.at[1]),
        (wv, wv3.at[2]),
        (cum_h, cum),
        (lens_h, lens),
        (accs_h, accs),
        (parent_h, parent),
        (bias_h, bias),
        (wft_h, wft),
        (kc, kcv),
        (vc, vcv),
        (wo, wov),
        (gpost_h, gpost),
    )
    ins = [None] + [
        pltpu.make_async_copy(a, b, loc.at[i]) for i, (a, b) in enumerate(pairs) if i > 0
    ]
    pieces = 4
    piece = rows // pieces
    tok_in = [
        pltpu.make_async_copy(
            tok.at[pl.ds(i * piece, piece)], tokv.at[pl.ds(i * piece, piece)], loc.at[16 + i]
        )
        for i in range(pieces)
    ]
    for c in tok_in[:1] + ins[1:2] + tok_in[1:] + ins[2:5]:
        c.start()
    par = lax.rem(me, 2)
    mate = me + 1 - 2 * par
    nh = n // 2

    def to_kv(ph, d, src, dst, sign=1):
        peer = lax.rem(me + sign * d + n, n)
        return pltpu.make_async_remote_copy(
            src_ref=src,
            dst_ref=dst,
            send_sem=ssem.at[ph, d],
            recv_sem=rsem.at[ph, d],
            device_id={"kv": peer},
            device_id_type=MESH,
        )

    def to_tp(ph, d, src, dst):
        peer = lax.rem(mt + d, nt)
        return pltpu.make_async_remote_copy(
            src_ref=src,
            dst_ref=dst,
            send_sem=tssem.at[ph, d],
            recv_sem=trsem.at[ph, d],
            device_id={"tp": peer},
            device_id_type=MESH,
        )

    def up(d):
        return lax.rem(me + d, n)

    def down(d):
        return lax.rem(me - d + n, n)

    def rrow(i):
        return pl.ds(pl.multiple_of(i * R, R), R)

    def lrow(i):
        return pl.ds(pl.multiple_of(i * L, L), L)

    def to_peer(ph, d, peer, src, dst):
        return pltpu.make_async_remote_copy(
            src_ref=src,
            dst_ref=dst,
            send_sem=ssem.at[ph, d],
            recv_sem=rsem.at[ph, d],
            device_id={"kv": peer},
            device_id_type=MESH,
        )

    def rsq_copy(d):
        return to_kv(0, d, partq.at[rrow(up(d))], rsq.at[d])

    def rs1_copy():
        return to_peer(1, 0, mate, part2.at[1 - par], rs1)

    def rs2_copy(e):
        peer = up(2 * e)
        return to_peer(2, e, peer, half.at[peer // 2], rs2.at[e])

    def gather_along(ph, e, view):
        return to_peer(ph, 2 * e, up(2 * e), view(me), view(me))

    def gather_mate(ph, e, view):
        c = down(2 * e)
        return to_peer(ph, 2 * e + 1, mate, view(c), view(c))

    def gather_start(ph, view):
        each(nh, lambda e: gather_along(ph, e, view).start())
        gather_mate(ph, 0, view).start()

    def gather_pass(ph, view):
        def one(e):
            c = down(2 * e)
            to_peer(ph, 2 * e, me, view(c), view(c)).wait_recv()
            gather_mate(ph, e, view).start()

        each(nh, one)

    def mate_chunk(e):
        return lax.rem(mate - 2 * e + n, n)

    def gather_wait(ph, e, view):
        c = mate_chunk(e)
        to_peer(ph, 2 * e + 1, mate, view(c), view(c)).wait_recv()

    def gather_drain(ph, view):
        each(nh, lambda e: gather_along(ph, e, view).wait_send())
        for e in range(nh):
            gather_mate(ph, e, view).wait_send()

    def q_view(c):
        return qall.at[rrow(c)]

    def k_view(c):
        return kvflat.at[0, lrow(c)]

    def v_view(c):
        return kvflat.at[1, lrow(c)]

    def att_view(c):
        return att.at[rrow(c)]

    def stat_copy(d):
        return to_kv(6, d, st_send.at[d], st_recv.at[d], -1)

    def val_copy(d):
        return to_kv(7, d, val_send.at[d], val_recv.at[d], -1)

    def cand_copy(d):
        return to_kv(8, d, cand_send, cand_recv.at[d])

    def sq_copy(d):
        return to_kv(10, d, sq_send, sq_recv.at[d])

    def each(count, fn):
        def body(d, c):
            fn(d)
            return c

        lax.fori_loop(1, count, body, 0)

    nb = min(2 * prop, piece)
    mine = pl.ds(pl.multiple_of(me * kdim, kdim), kdim)
    ins[1].wait()

    def norm_rows(i, c):
        sl = pl.ds(pl.multiple_of(i * nb, nb), nb)
        t = tokv[sl, :].astype(F32)
        inv = lax.rsqrt(jnp.mean(t * t, axis=-1, keepdims=True) + epsilon)
        invs[sl, :] = jnp.broadcast_to(inv, (nb, 128))
        slab[sl, :] = (tokv[sl, mine].astype(F32) * inv * gain[:, mine]).astype(BF)
        return c

    for p in range(pieces):
        tok_in[p].wait()
        lax.fori_loop(p * piece // nb, (p + 1) * piece // nb, norm_rows, 0)
    for c in ins[5:]:
        c.start()
    local = slab[...]
    pl.semaphore_wait(barrier, n - 1 + nt - 1)
    ins[2].wait()
    partq[...] = jnp.dot(local, wv3[0], preferred_element_type=F32).astype(BF)
    each(n, lambda d: rsq_copy(d).start())
    for i in range(2):
        ins[3 + i].wait()
        both_rows = jnp.dot(local, wv3[1 + i], preferred_element_type=F32).astype(BF)
        for c in range(n):
            part2[c % 2, c // 2, :, i * hw : (i + 1) * hw] = both_rows[c * R : (c + 1) * R]
    rs1_copy().start()

    def norm_rest(i, c):
        sl = pl.ds(pl.multiple_of(i * nb, nb), nb)
        inv = invs[sl, 0:1]
        normed[sl, :] = (tokv[sl, :].astype(F32) * inv * gain[...]).astype(BF)
        return c

    lax.fori_loop(0, rows // nb, norm_rest, 0)
    for c in ins[5:11]:
        c.wait()

    r64 = num_seqs * heads
    c64 = cum[...]
    srow = iota((r64, span), 0) // heads
    lane = iota((r64, span), 1)
    rel64 = jnp.zeros((r64, span), jnp.int32)
    rel16 = jnp.zeros((num_seqs, cols), jnp.int32)
    s16 = iota((num_seqs, cols), 0)
    for s in range(num_seqs):
        rel_s = lens[s] + accs[s] - base
        rel64 = jnp.where(srow == s, rel_s, rel64)
        rel16 = jnp.where(s16 == s, rel_s, rel16)
    cand = jnp.max(jnp.where(lane == rel64 - 1, c64, floor_value), axis=1, keepdims=True)
    diag = iota((r64, 128), 0) == iota((r64, 128), 1)
    cand_lane = jnp.sum(jnp.where(diag, cand, 0.0), axis=0, keepdims=True)
    cand_send[...] = jnp.broadcast_to(cand_lane, (8, 128))
    each(n, lambda d: cand_copy(d).start())

    spread = hot(iota((span, cols), 1) // heads == iota((span, cols), 0))
    e1 = dot_hi(c64, spread)
    e1 = jnp.where(iota((r64, cols), 0) % heads == iota((r64, cols), 1) % heads, e1, 0.0)
    take = hot(iota((num_seqs, r64), 1) // heads == iota((num_seqs, r64), 0))
    cflat = dot_hi(take, e1)
    brow[...] = jnp.where(iota((num_seqs, cols), 1) // heads < rel16, -cflat, floor_value)

    ri = iota((rows, rows), 0)
    ci = iota((rows, rows), 1)
    pick = hot(iota((rows, num_seqs), 0) // prop == iota((rows, num_seqs), 1))
    pb = dot_hi(pick, parent[...].astype(F32))
    pcol = jnp.sum(
        jnp.where(iota((rows, prop), 1) == iota((rows, prop), 0) % prop, pb, 0.0),
        axis=1,
        keepdims=True,
    )
    target = jnp.where(pcol >= 0.0, (ri // prop * prop).astype(F32) + pcol, -1.0)
    a = jnp.where((ri == ci) | (ci.astype(F32) == target), 1.0, 0.0)
    for sweep in range(max(1, (prop - 1).bit_length())):
        low = a.astype(BF)
        a = jnp.minimum(jnp.dot(low, low, preferred_element_type=F32), 1.0)
    anc[...] = a
    lf = lax.dot_general(wft[...], normed[...], NT, preferred_element_type=F32)
    bcol = jnp.zeros((heads_all, rows), F32)
    for h in range(heads_all):
        bcol = jnp.where(iota((heads_all, rows), 0) == h, bias[h], bcol)
    z = lf + bcol
    lf = jnp.minimum(z, 0.0) - jnp.log1p(jnp.exp(-jnp.abs(z)))
    path_t = dot_hi(lf, a, NT)
    rep = hot(iota((r64, heads_all), 1) == mt * heads + iota((r64, heads_all), 0) % heads)
    pm = dot_hi(rep, path_t)
    pm = jnp.where(iota((r64, rows), 1) // prop == iota((r64, rows), 0) // heads, pm, 0.0)
    fold = hot(iota((rows, 128), 0) % prop == iota((rows, 128), 1) % prop)
    pt = dot_hi(pm, fold)
    ptile[...] = pt
    ptm = jnp.where((iota((r64, 128), 1) // prop) % heads == iota((r64, 128), 0) % heads, pt, 0.0)
    tpath[...] = dot_hi(take, ptm)

    own_q = partq[rrow(me)].astype(F32)
    for d in range(1, n):
        rsq_copy(d).wait_recv()
        own_q = own_q + rsq[d].astype(F32)
    qall[rrow(me)] = own_q.astype(BF)
    gather_start(3, q_view)
    rs1_copy().wait_recv()
    for i in range(nh):
        half[i] = (part2[par, i].astype(F32) + rs1[i].astype(F32)).astype(BF)
    each(nh, lambda e: rs2_copy(e).start())

    ins[11].wait()
    ins[12].wait()
    same_head = iota((hp, cols), 0) // prop == iota((hp, cols), 1) % heads
    diag_l = iota((L, L), 0) == iota((L, L), 1)

    def heads_of(block):
        return jnp.concatenate([block[:, h * hd : (h + 1) * hd] for h in range(heads)], axis=0)

    def block_part(src):
        maxes, totals, values = [], [], []
        for j in range(sp):
            s = src * sp + j
            q = heads_of(qall[pl.ds(pl.multiple_of(s * prop, prop), prop), :])
            sc = lax.dot_general(q, kcv[s], NT, preferred_element_type=F32) * scale
            sc = jnp.where(same_head, sc + brow[pl.ds(s, 1), :], floor_value)
            m = jnp.max(sc, axis=1, keepdims=True)
            w = jnp.exp(sc - m)
            maxes.append(m)
            totals.append(jnp.sum(w, axis=1, keepdims=True))
            values.append(
                jnp.dot(w.astype(BF), vcv[s], preferred_element_type=F32).astype(BF)
            )
        m = jnp.concatenate(maxes, axis=0)
        t = jnp.concatenate(totals, axis=0)
        m_lane = jnp.sum(jnp.where(diag_l, m, 0.0), axis=0, keepdims=True)
        t_lane = jnp.sum(jnp.where(diag_l, t, 0.0), axis=0, keepdims=True)
        stats = jnp.where(iota((8, L), 0) == 0, m_lane, t_lane)
        return stats, jnp.concatenate(values, axis=0)

    def remote_block(d):
        src = down(d)
        stats, values = block_part(src)
        st_send[d] = stats
        val_send[d] = values
        stat_copy(d).start()
        val_copy(d).start()

    stats, values = block_part(me)
    st_recv[0] = stats
    val_recv[0] = values
    gather_pass(3, q_view)
    each(nh, lambda e: remote_block(2 * e))

    def mate_block(e, c):
        gather_wait(3, e, q_view)
        remote_block(lax.rem(me - mate_chunk(e) + n, n))
        return c

    lax.fori_loop(0, nh, mate_block, 0)
    own_kv = half[me // 2].astype(F32)
    for e in range(1, nh):
        rs2_copy(e).wait_recv()
        own_kv = own_kv + rs2[e].astype(F32)
    kvown[...] = own_kv.astype(BF)
    for i in range(2):
        for h in range(heads):
            flat[pl.ds(h, R, stride=heads), :] = own_kv[:, i * hw + h * hd : i * hw + (h + 1) * hd]
        kvflat[i, lrow(me)] = flat[...].astype(BF)
    gather_start(5, k_view)

    fold_h = iota((rows, hp), 0)
    tmax, ttot, tval = [], [], []
    for j in range(sp):
        s = me * sp + j
        q = heads_of(qall[pl.ds(pl.multiple_of(s * prop, prop), prop), :])
        k = heads_of(kvown[j * prop : (j + 1) * prop, 0:hw])
        v = heads_of(kvown[j * prop : (j + 1) * prop, hw : 2 * hw])
        arows = anc[pl.ds(pl.multiple_of(s * prop, prop), prop), :]
        sel = hot(fold_h == s * prop + iota((rows, hp), 1) % prop).astype(BF)
        am = jnp.dot(arows.astype(BF), sel, preferred_element_type=F32)
        am = jnp.concatenate([am] * heads, axis=0)
        mask = (am > 0.5) & (iota((hp, hp), 0) // prop == iota((hp, hp), 1) // prop)
        sc = lax.dot_general(q, k, NT, preferred_element_type=F32) * scale
        sc = jnp.where(mask, sc - tpath[pl.ds(s, 1), 0:hp], floor_value)
        m = jnp.max(sc, axis=1, keepdims=True)
        w = jnp.where(mask, jnp.exp(sc - m), 0.0)
        tmax.append(m)
        ttot.append(jnp.sum(w, axis=1, keepdims=True))
        tval.append(jnp.dot(w.astype(BF), v, preferred_element_type=F32))
    tree_max = jnp.concatenate(tmax, axis=0)
    tree_tot = jnp.concatenate(ttot, axis=0)
    tree_val = jnp.concatenate(tval, axis=0)

    last_lane = cand_send[...]
    for d in range(1, n):
        cand_copy(d).wait_recv()
        last_lane = jnp.maximum(last_lane, cand_recv[d])
    last_col = jnp.sum(jnp.where(diag, last_lane[0:1], 0.0), axis=1, keepdims=True)
    own_rows = iota((L, 128), 0)
    own_pick = iota((L, 128), 1) == (me * sp + own_rows // hp) * heads + (own_rows % hp) // prop
    last_own = jnp.sum(jnp.where(own_pick, last_lane[0:1], 0.0), axis=1, keepdims=True)

    shifted_path = ptile[...]
    for b in range((span - 1).bit_length()):
        moved = pltpu.roll(shifted_path, 1 << b, 1)
        shifted_path = jnp.where((rel64 >> b) & 1 == 1, moved, shifted_path)
    off = lane - rel64
    cum_out[...] = jnp.where((off >= 0) & (off < prop), last_col + shifted_path, cum[...])

    for d in range(1, n):
        stat_copy(d).wait_recv()
    top = st_recv[0]
    for d in range(1, n):
        top = jnp.maximum(top, st_recv[d])
    top = top[0:1]

    def col(x):
        return jnp.sum(jnp.where(diag_l, x, 0.0), axis=1, keepdims=True)

    cache_tot = jnp.zeros((1, L), F32)
    scales = []
    for d in range(n):
        sd = jnp.exp(st_recv[d, 0:1] - top)
        scales.append(col(sd))
        cache_tot = cache_tot + st_recv[d, 1:2] * sd
    shifted = col(top) + last_own
    both = jnp.maximum(shifted, tree_max)
    cscale = jnp.exp(shifted - both)
    tscale = jnp.exp(tree_max - both)
    denom = col(cache_tot) * cscale + tree_tot * tscale
    vals = jnp.zeros((L, hd), F32)
    for d in range(n):
        if d > 0:
            val_copy(d).wait_recv()
        vals = vals + val_recv[d].astype(F32) * scales[d]
    attended = ((vals * cscale + tree_val * tscale) / denom).astype(BF)
    for j in range(sp):
        for h in range(heads):
            att[pl.ds(pl.multiple_of(me * R + j * prop, prop), prop), h * hd : (h + 1) * hd] = (
                attended[j * hp + h * prop : j * hp + (h + 1) * prop]
            )
    gather_start(4, att_view)
    ins[13].wait()
    ins[14].wait()
    gather_pass(4, att_view)
    gather_start(11, v_view)
    gather_pass(5, k_view)
    for e in range(nh):
        gather_wait(4, e, att_view)
    full = jnp.dot(att[...], wov[...], preferred_element_type=F32).astype(BF)
    oc = o_send.shape[2]
    for t in range(nt):
        o_send[t] = full[:, t * oc : (t + 1) * oc]

    def o_copy(d):
        return to_tp(0, d, o_send.at[lax.rem(mt + d, nt)], o_recv.at[d])

    def sq2_copy(d):
        return to_tp(1, d, sq2_send, sq2_recv.at[d])

    each(nt, lambda d: o_copy(d).start())
    gather_pass(11, v_view)
    mixed = o_send[mt].astype(F32)
    for d in range(1, nt):
        o_copy(d).wait_recv()
        mixed = mixed + o_recv[d].astype(F32)
    sq_send[...] = dot_hi(jnp.ones((8, oc), F32), mixed * mixed, NT)[0:1]
    each(n, lambda d: sq_copy(d).start())
    sq = sq_send[...]
    for d in range(1, n):
        sq_copy(d).wait_recv()
        sq = sq + sq_recv[d]
    sq2_send[...] = sq
    each(nt, lambda d: sq2_copy(d).start())
    for e in range(nh):
        gather_wait(5, e, k_view)
        gather_wait(11, e, v_view)
    out_kv = pltpu.make_async_copy(kvflat, kv_out, loc.at[15])
    out_kv.start()
    for d in range(1, nt):
        sq2_copy(d).wait_recv()
        sq = sq + sq2_recv[d]
    ssum = dot_hi(jnp.broadcast_to(sq, (8, rows)), jnp.full((8, oc), 0.125, F32), (((0,), (0,)), ((), ())))
    mixed_out[...] = (mixed * lax.rsqrt(ssum / width + epsilon) * gpost[...]).astype(BF)

    def drain(d):
        rsq_copy(d).wait_send()
        stat_copy(d).wait_send()
        val_copy(d).wait_send()
        cand_copy(d).wait_send()
        sq_copy(d).wait_send()

    each(n, drain)
    rs1_copy().wait_send()
    each(nh, lambda e: rs2_copy(e).wait_send())
    gather_drain(3, q_view)
    gather_drain(4, att_view)
    gather_drain(5, k_view)
    gather_drain(11, v_view)

    def drain_t(d):
        o_copy(d).wait_send()
        sq2_copy(d).wait_send()

    each(nt, drain_t)
    out_kv.wait()


def write_kernel(
    num_seqs,
    prop,
    span,
    kc,
    vc,
    kv_new,
    mixed,
    cum,
    lens_h,
    accs_h,
    k_out,
    v_out,
    mixed_out,
    cum_out,
    buf,
    fresh,
    lens,
    accs,
    sem,
    sin,
    sout,
):
    base = lax.axis_index("kv") * span
    small = [
        pltpu.make_async_copy(lens_h, lens, sem.at[0]),
        pltpu.make_async_copy(accs_h, accs, sem.at[1]),
        pltpu.make_async_copy(kv_new, fresh, sem.at[2]),
        pltpu.make_async_copy(mixed, mixed_out, sem.at[3]),
        pltpu.make_async_copy(cum, cum_out, sem.at[4]),
    ]
    cut = sin.shape[1]
    step = num_seqs // cut
    arrays = ((kc, k_out), (vc, v_out))

    def part(c):
        return pl.ds(c * step, step)

    def come(c, i):
        return pltpu.make_async_copy(arrays[i][0].at[part(c)], buf.at[i, part(c)], sin.at[i, c])

    def leave(c, i):
        return pltpu.make_async_copy(buf.at[i, part(c)], arrays[i][1].at[part(c)], sout.at[i, c])

    for c in small[:3]:
        c.start()
    for c in range(cut):
        for i in range(2):
            come(c, i).start()
    for c in small[3:]:
        c.start()
    for c in small[:3]:
        c.wait()

    def place(i, s):
        rel = lens[s] + accs[s] - base
        whole = (rel >= 0) & (rel <= span - prop)
        partly = (rel > -prop) & (rel < span) & jnp.logical_not(whole)

        @pl.when(whole)
        def _():
            buf[i, s, pl.ds(rel, prop)] = fresh[i, s]

        @pl.when(partly)
        def _():
            def one(j, c):
                buf[i, s, pl.ds(rel + j, 1)] = fresh[i, s, pl.ds(j, 1)]
                return c

            lax.fori_loop(jnp.maximum(-rel, 0), jnp.minimum(span - rel, prop), one, 0)

    for c in range(cut):
        for i in range(2):
            come(c, i).wait()
            for s in range(c * step, (c + 1) * step):
                place(i, s)
            leave(c, i).start()
    for c in range(cut):
        for i in range(2):
            leave(c, i).wait()
    for c in small[3:]:
        c.wait()


def fast_device(
    n,
    nt,
    tokens,
    gain_pre,
    w_query,
    w_key,
    w_value,
    w_forget,
    b_forget,
    w_out,
    gain_post,
    key_cache,
    value_cache,
    cum_cache,
    lengths,
    accepted,
    parent,
):
    num_seqs, prop, width = tokens.shape
    span, heads, hd = key_cache.shape[1:]
    rows = num_seqs * prop
    hw = heads * hd
    cols = heads * span
    sp = num_seqs // n
    R = sp * prop
    L = sp * heads * prop
    oc = gain_post.shape[0]
    kc = key_cache.reshape(num_seqs, cols, hd)
    vc = value_cache.reshape(num_seqs, cols, hd)
    cum = jnp.swapaxes(cum_cache, 1, 2).reshape(num_seqs * heads, span)
    vmem = pl.BlockSpec(memory_space=pltpu.VMEM)
    V = pltpu.VMEM
    D = pltpu.SemaphoreType.DMA
    hbm = pl.BlockSpec(memory_space=pltpu.HBM)
    S = pltpu.SMEM
    nh = n // 2
    mixed, kv_new, cum_new = pl.pallas_call(
        functools.partial(layer_kernel, n, nt, num_seqs, prop, heads, hd, span),
        out_shape=(
            jax.ShapeDtypeStruct((rows, oc), BF),
            jax.ShapeDtypeStruct((2, rows * heads, hd), BF),
            jax.ShapeDtypeStruct(cum.shape, F32),
        ),
        in_specs=[hbm] * 15,
        out_specs=(vmem, hbm, vmem),
        scratch_shapes=[
            V((rows, width), BF),
            V((rows, width), BF),
            V((rows, w_query.shape[0]), BF),
            V((rows, 128), F32),
            V((1, width), F32),
            V((3,) + w_query.shape, BF),
            V(w_forget.T.shape, BF),
            V(w_out.shape, BF),
            V((1, oc), F32),
            V(kc.shape, BF),
            V(vc.shape, BF),
            V(cum.shape, F32),
            V(parent.shape, jnp.int32),
            S(b_forget.shape, F32),
            S(lengths.shape, jnp.int32),
            S(accepted.shape, jnp.int32),
            V((rows, hw), BF),
            V((n, R, hw), BF),
            V((2, nh, R, 2 * hw), BF),
            V((nh, R, 2 * hw), BF),
            V((nh, R, 2 * hw), BF),
            V((nh, R, 2 * hw), BF),
            V((R, 2 * hw), BF),
            V((L, hd), F32),
            V((2, rows * heads, hd), BF),
            V((rows, hw), BF),
            V((n, 8, L), F32),
            V((n, L, hd), BF),
            V((n, 8, L), F32),
            V((n, L, hd), BF),
            V((8, 128), F32),
            V((n, 8, 128), F32),
            V((num_seqs, cols), F32),
            V((rows, rows), F32),
            V((num_seqs, 128), F32),
            V((num_seqs * heads, 128), F32),
            V((rows, hw), BF),
            V((nt, rows, oc), BF),
            V((nt, rows, oc), BF),
            V((1, rows), F32),
            V((n, 1, rows), F32),
            V((1, rows), F32),
            V((nt, 1, rows), F32),
            D((20,)),
            D((12, n)),
            D((12, n)),
            D((2, nt)),
            D((2, nt)),
        ],
        compiler_params=pltpu.CompilerParams(
            collective_id=0, has_side_effects=True, vmem_limit_bytes=67043328
        ),
        name="layer",
    )(
        tokens.reshape(rows, width),
        gain_pre.reshape(1, width),
        w_query,
        w_key,
        w_value,
        w_forget.T,
        b_forget,
        w_out,
        gain_post.reshape(1, oc),
        kc,
        vc,
        cum,
        lengths,
        accepted,
        parent,
    )
    key_out, value_out, mixed, cum_new = pl.pallas_call(
        functools.partial(write_kernel, num_seqs, prop, span),
        out_shape=(
            jax.ShapeDtypeStruct(key_cache.shape, BF),
            jax.ShapeDtypeStruct(value_cache.shape, BF),
            jax.ShapeDtypeStruct(mixed.shape, BF),
            jax.ShapeDtypeStruct(cum_new.shape, F32),
        ),
        in_specs=[hbm] * 7,
        out_specs=(hbm,) * 4,
        scratch_shapes=[
            V((2,) + key_cache.shape, BF),
            V((2, num_seqs, prop, heads, hd), BF),
            S(lengths.shape, jnp.int32),
            S(accepted.shape, jnp.int32),
            D((5,)),
            D((2, 4)),
            D((2, 4)),
        ],
        compiler_params=pltpu.CompilerParams(vmem_limit_bytes=67043328),
        name="cache_write",
    )(
        key_cache,
        value_cache,
        kv_new.reshape(2, num_seqs, prop, heads, hd),
        mixed,
        cum_new,
        lengths,
        accepted,
    )
    cum_out = jnp.swapaxes(cum_new.reshape(num_seqs, heads, span), 1, 2)
    return (
        mixed.reshape(num_seqs, prop, oc),
        key_out,
        value_out,
        cum_out,
    )


def choose(mesh):
    n, nt = mesh.shape["kv"], mesh.shape["tp"]

    def body(*args):
        tokens, key_cache = args[0], args[9]
        num_seqs, prop = tokens.shape[:2]
        span, heads = key_cache.shape[1:3]
        fits = (
            num_seqs % n == 0
            and n % 2 == 0
            and num_seqs % 4 == 0
            and (num_seqs // n) * heads * prop == 128
            and span == 128
            and num_seqs * heads <= 128
            and prop % 16 == 0
        )
        if fits:
            return fast_device(n, nt, *args)
        return per_device(*args)

    return body


def solution(mesh):
    return jax.shard_map(
        choose(mesh),
        mesh=mesh,
        in_specs=(
            P(),
            P(),
            P("kv", "tp"),
            P("kv", "tp"),
            P("kv", "tp"),
            P(),
            P(),
            P("tp", "kv"),
            P(("kv", "tp")),
            P(None, "kv", "tp", None),
            P(None, "kv", "tp", None),
            P(None, "kv", "tp"),
            P(),
            P(),
            P(),
        ),
        out_specs=(
            P(None, None, ("kv", "tp")),
            P(None, "kv", "tp", None),
            P(None, "kv", "tp", None),
            P(None, "kv", "tp"),
        ),
        check_vma=False,
    )
```

```python
import functools

import jax
import jax.numpy as jnp
from jax import lax
from jax.experimental import pallas as pl
from jax.experimental.pallas import tpu as pltpu
from jax.sharding import PartitionSpec as P

epsilon = 1e-06
floor_value = -1e30


def merged(part, axis, combine):
    gathered = jax.tree.map(lambda a: lax.all_gather(a, axis), part)

    def take(source):
        return jax.tree.map(lambda a: lax.dynamic_index_in_dim(a, source, 0, False), gathered)

    return lax.fori_loop(
        1, lax.axis_size(axis), lambda source, state: combine(state, take(source)), take(0)
    )


def ancestry(parent_ids, members):
    identity = jnp.eye(members, dtype=jnp.float32)
    parent_hot = (
        parent_ids[:, :, None] == jnp.arange(members, dtype=jnp.int32)[None, None, :]
    ).astype(jnp.float32)
    ancestors = jnp.minimum(identity[None] + parent_hot, 1.0)
    for sweep in range(max(1, (members - 1).bit_length())):
        ancestors = jnp.minimum(
            jnp.einsum("bij,bjk->bik", ancestors, ancestors, precision=lax.Precision.HIGHEST), 1.0
        )
    return ancestors


def combine_parts(first, second):
    new_max = jnp.maximum(first[0], second[0])
    first_scale = jnp.exp(first[0] - new_max)
    second_scale = jnp.exp(second[0] - new_max)
    return (
        new_max,
        first[1] * first_scale + second[1] * second_scale,
        first[2] * first_scale[..., None] + second[2] * second_scale[..., None],
        jnp.maximum(first[3], second[3]),
    )


def finish_rows(cache_max, cache_total, cache_values, last_rows, tree_max, tree_total, tree_values):
    shifted = cache_max + last_rows
    top = jnp.maximum(shifted, tree_max)
    cache_scale = jnp.exp(shifted - top)
    tree_scale = jnp.exp(tree_max - top)
    attended = (
        (cache_values * cache_scale[..., None] + tree_values * tree_scale[..., None])
        / (cache_total * cache_scale + tree_total * tree_scale)[..., None]
    ).astype(jnp.bfloat16)
    return attended.reshape(attended.shape[0], attended.shape[1] * attended.shape[2])


def per_device(
    tokens,
    gain_pre,
    w_query,
    w_key,
    w_value,
    w_forget,
    b_forget,
    w_out,
    gain_post,
    key_cache,
    value_cache,
    cum_cache,
    lengths,
    accepted,
    parent,
):
    num_seqs, proposals, model_width = tokens.shape
    kv_rank = lax.axis_index("kv")
    tp_rank = lax.axis_index("tp")
    span = key_cache.shape[1]
    heads_local = key_cache.shape[2]
    head_dim = key_cache.shape[3]
    scale = head_dim ** (-0.5)
    all_rows = num_seqs * proposals
    tok_float = tokens.astype(jnp.float32)
    normed = (
        tok_float
        * lax.rsqrt(jnp.mean(tok_float * tok_float, -1, keepdims=True) + epsilon)
        * gain_pre
    ).astype(jnp.bfloat16)
    flat = normed.reshape(all_rows, model_width)
    weight_rows = w_query.shape[0]
    local_rows = lax.dynamic_slice_in_dim(flat, kv_rank * weight_rows, weight_rows, 1)
    query_part = jnp.dot(local_rows, w_query, preferred_element_type=jnp.float32)
    key_part = jnp.dot(local_rows, w_key, preferred_element_type=jnp.float32)
    value_part = jnp.dot(local_rows, w_value, preferred_element_type=jnp.float32)
    summed = (
        lax.psum(query_part.astype(jnp.bfloat16), "kv").astype(jnp.float32),
        lax.psum(key_part.astype(jnp.bfloat16), "kv").astype(jnp.float32),
        lax.psum(value_part.astype(jnp.bfloat16), "kv").astype(jnp.float32),
    )
    query_flat = summed[0].astype(jnp.bfloat16)
    key_flat = summed[1].astype(jnp.bfloat16)
    value_flat = summed[2].astype(jnp.bfloat16)
    query = query_flat.reshape(num_seqs, proposals, heads_local, head_dim)
    key_new = key_flat.reshape(num_seqs, proposals, heads_local, head_dim)
    value_new = value_flat.reshape(num_seqs, proposals, heads_local, head_dim)
    forget_cols = lax.dynamic_slice_in_dim(w_forget, tp_rank * heads_local, heads_local, 1)
    forget_bias = lax.dynamic_slice_in_dim(b_forget, tp_rank * heads_local, heads_local, 0)
    log_forget = jax.nn.log_sigmoid(
        jnp.dot(flat, forget_cols, preferred_element_type=jnp.float32) + forget_bias
    ).reshape(num_seqs, proposals, heads_local)
    ancestors = ancestry(parent, proposals)
    path = jnp.einsum("bij,bjh->bih", ancestors, log_forget, precision=lax.Precision.HIGHEST)
    valid = lengths + accepted
    positions = kv_rank * span + jnp.arange(span, dtype=jnp.int32)
    live = (positions[None, :] < valid[:, None])[:, None, None, :]
    score = (
        jnp.einsum("bihd,bkhd->bihk", query, key_cache, preferred_element_type=jnp.float32) * scale
        + path[..., None]
        - jnp.swapaxes(cum_cache, 1, 2)[:, None]
    )
    block_max = jnp.max(jnp.where(live, score, floor_value), axis=-1)
    weight = jnp.exp(jnp.where(live, score - block_max[..., None], floor_value))
    block_total = jnp.sum(weight, axis=-1)
    block_values = jnp.einsum(
        "bihk,bkhd->bihd",
        weight.astype(jnp.bfloat16),
        value_cache,
        preferred_element_type=jnp.float32,
    )
    owner = positions[None, :] == (valid - 1)[:, None]
    candidate = jnp.max(jnp.where(owner[:, :, None], cum_cache, floor_value), axis=1)
    tree_mask = (ancestors > 0.5)[:, :, None, :]
    tree_score = (
        jnp.einsum("bihd,bjhd->bihj", query, key_new, preferred_element_type=jnp.float32) * scale
        + path[..., None]
        - jnp.swapaxes(path, 1, 2)[:, None]
    )
    tree_max = jnp.max(jnp.where(tree_mask, tree_score, floor_value), axis=-1)
    tree_weight = jnp.exp(jnp.where(tree_mask, tree_score - tree_max[..., None], floor_value))
    tree_total = jnp.sum(tree_weight, axis=-1)
    tree_values = jnp.einsum(
        "bihj,bjhd->bihd",
        tree_weight.astype(jnp.bfloat16),
        value_new,
        preferred_element_type=jnp.float32,
    )
    tree_max_rows = tree_max.reshape(all_rows, heads_local)
    tree_total_rows = tree_total.reshape(all_rows, heads_local)
    tree_values_rows = tree_values.reshape(all_rows, heads_local, head_dim)
    cache_max, cache_total, cache_values, last_cum = merged(
        (block_max, block_total, block_values, candidate), "kv", combine_parts
    )
    last_rows = jnp.broadcast_to(last_cum[:, None, :], (num_seqs, proposals, heads_local)).reshape(
        all_rows, heads_local
    )
    attended = finish_rows(
        cache_max.reshape(all_rows, heads_local),
        cache_total.reshape(all_rows, heads_local),
        cache_values.reshape(all_rows, heads_local, head_dim),
        last_rows,
        tree_max_rows,
        tree_total_rows,
        tree_values_rows,
    )
    mixed_part = jnp.dot(attended, w_out, preferred_element_type=jnp.float32)
    mixed_sum = lax.psum_scatter(
        mixed_part.astype(jnp.bfloat16), "tp", scatter_dimension=1, tiled=True
    ).astype(jnp.float32)
    squares = lax.psum(jnp.sum(mixed_sum * mixed_sum, axis=1), ("kv", "tp"))
    mixed = (mixed_sum * lax.rsqrt(squares / model_width + epsilon)[:, None] * gain_post).astype(
        jnp.bfloat16
    )
    mixed = mixed.reshape(num_seqs, proposals, mixed_sum.shape[1])
    relative = positions[None, :] - valid[:, None]
    select = relative[:, :, None] == jnp.arange(proposals, dtype=jnp.int32)[None, None, :]
    written = (relative >= 0) & (relative < proposals)
    placed_keys = jnp.einsum(
        "bkj,bjhd->bkhd", select.astype(jnp.bfloat16), key_new, preferred_element_type=jnp.float32
    ).astype(jnp.bfloat16)
    placed_values = jnp.einsum(
        "bkj,bjhd->bkhd", select.astype(jnp.bfloat16), value_new, preferred_element_type=jnp.float32
    ).astype(jnp.bfloat16)
    key_out = jnp.where(written[:, :, None, None], placed_keys, key_cache)
    value_out = jnp.where(written[:, :, None, None], placed_values, value_cache)
    cum_new = last_cum[:, None, :] + path
    placed_cum = jnp.einsum(
        "bkj,bjh->bkh", select.astype(jnp.float32), cum_new, precision=lax.Precision.HIGHEST
    )
    cum_out = jnp.where(written[:, :, None], placed_cum, cum_cache)
    return (mixed, key_out, value_out, cum_out)


MESH = pl.DeviceIdType.MESH
HI = lax.Precision.HIGHEST
F32 = jnp.float32
BF = jnp.bfloat16


def iota(shape, dim):
    return lax.broadcasted_iota(jnp.int32, shape, dim)


def hot(mask):
    return jnp.where(mask, 1.0, 0.0).astype(F32)


def dot_hi(a, b, dims=(((1,), (0,)), ((), ()))):
    return lax.dot_general(a, b, dims, precision=HI, preferred_element_type=F32)


NT = (((1,), (1,)), ((), ()))


def layer_kernel(
    n,
    nt,
    num_seqs,
    prop,
    heads,
    hd,
    span,
    tok,
    gain_h,
    wq,
    wk,
    wv,
    wft_h,
    bias_h,
    wo,
    gpost_h,
    kc,
    vc,
    cum_h,
    lens_h,
    accs_h,
    parent_h,
    mixed_out,
    kv_out,
    cum_out,
    tokv,
    normed,
    slab,
    invs,
    gain,
    wv3,
    wft,
    wov,
    gpost,
    kcv,
    vcv,
    cum,
    parent,
    bias,
    lens,
    accs,
    partq,
    rsq,
    part2,
    rs1,
    half,
    rs2,
    kvown,
    flat,
    kvflat,
    qall,
    st_send,
    val_send,
    st_recv,
    val_recv,
    cand_send,
    cand_recv,
    brow,
    anc,
    tpath,
    ptile,
    att,
    o_send,
    o_recv,
    sq_send,
    sq_recv,
    loc,
    ssem,
    rsem,
    tssem,
    trsem,
    qssem,
    qrsem,
):
    me = lax.axis_index("kv")
    mt = lax.axis_index("tp")
    rows = num_seqs * prop
    width = tok.shape[1]
    hw = heads * hd
    kdim = wq.shape[0]
    cols = heads * span
    sp = num_seqs // n
    R = sp * prop
    hp = heads * prop
    L = sp * hp
    scale = hd ** (-0.5)
    base = me * span
    heads_all = wft.shape[0]

    barrier = pltpu.get_barrier_semaphore()

    count = n * nt
    spot = me * nt + mt

    def place(d):
        other = lax.rem(spot + d, count)
        return {"kv": other // nt, "tp": lax.rem(other, nt)}

    def greet(d, c):
        pl.semaphore_signal(barrier, inc=1, device_id=place(d), device_id_type=MESH)
        return c

    lax.fori_loop(1, count, greet, 0)

    pairs = (
        (tok, tokv),
        (gain_h, gain),
        (wq, wv3.at[0]),
        (wk, wv3.at[1]),
        (wv, wv3.at[2]),
        (cum_h, cum),
        (lens_h, lens),
        (accs_h, accs),
        (parent_h, parent),
        (bias_h, bias),
        (wft_h, wft),
        (kc, kcv),
        (vc, vcv),
        (wo, wov),
        (gpost_h, gpost),
    )
    ins = [None] + [
        pltpu.make_async_copy(a, b, loc.at[i]) for i, (a, b) in enumerate(pairs) if i > 0
    ]
    pieces = 4
    piece = rows // pieces
    tok_in = [
        pltpu.make_async_copy(
            tok.at[pl.ds(i * piece, piece)], tokv.at[pl.ds(i * piece, piece)], loc.at[16 + i]
        )
        for i in range(pieces)
    ]
    for c in tok_in[:1] + ins[1:2] + tok_in[1:] + ins[2:5]:
        c.start()
    par = lax.rem(me, 2)
    mate = me + 1 - 2 * par
    nh = n // 2

    def to_kv(ph, d, src, dst, sign=1):
        peer = lax.rem(me + sign * d + n, n)
        return pltpu.make_async_remote_copy(
            src_ref=src,
            dst_ref=dst,
            send_sem=ssem.at[ph, d],
            recv_sem=rsem.at[ph, d],
            device_id={"kv": peer},
            device_id_type=MESH,
        )

    def to_tp(ph, d, src, dst):
        peer = lax.rem(mt + d, nt)
        return pltpu.make_async_remote_copy(
            src_ref=src,
            dst_ref=dst,
            send_sem=tssem.at[ph, d],
            recv_sem=trsem.at[ph, d],
            device_id={"tp": peer},
            device_id_type=MESH,
        )

    def up(d):
        return lax.rem(me + d, n)

    def down(d):
        return lax.rem(me - d + n, n)

    def rrow(i):
        return pl.ds(pl.multiple_of(i * R, R), R)

    def lrow(i):
        return pl.ds(pl.multiple_of(i * L, L), L)

    def to_peer(ph, d, peer, src, dst):
        return pltpu.make_async_remote_copy(
            src_ref=src,
            dst_ref=dst,
            send_sem=ssem.at[ph, d],
            recv_sem=rsem.at[ph, d],
            device_id={"kv": peer},
            device_id_type=MESH,
        )

    def rsq_copy(d):
        return to_kv(0, d, partq.at[rrow(up(d))], rsq.at[d])

    def rs1_copy():
        return to_peer(1, 0, mate, part2.at[1 - par], rs1)

    def rs2_copy(e):
        peer = up(2 * e)
        return to_peer(2, e, peer, half.at[peer // 2], rs2.at[e])

    def gather_along(ph, e, view):
        return to_peer(ph, 2 * e, up(2 * e), view(me), view(me))

    def gather_mate(ph, e, view):
        c = down(2 * e)
        return to_peer(ph, 2 * e + 1, mate, view(c), view(c))

    def gather_start(ph, view):
        each(nh, lambda e: gather_along(ph, e, view).start())
        gather_mate(ph, 0, view).start()

    def gather_pass(ph, view):
        def one(e):
            c = down(2 * e)
            to_peer(ph, 2 * e, me, view(c), view(c)).wait_recv()
            gather_mate(ph, e, view).start()

        each(nh, one)

    def mate_chunk(e):
        return lax.rem(mate - 2 * e + n, n)

    def gather_wait(ph, e, view):
        c = mate_chunk(e)
        to_peer(ph, 2 * e + 1, mate, view(c), view(c)).wait_recv()

    def gather_drain(ph, view):
        each(nh, lambda e: gather_along(ph, e, view).wait_send())
        for e in range(nh):
            gather_mate(ph, e, view).wait_send()

    def q_view(c):
        return qall.at[rrow(c)]

    def k_view(c):
        return kvflat.at[0, lrow(c)]

    def v_view(c):
        return kvflat.at[1, lrow(c)]

    def att_view(c):
        return att.at[rrow(c)]

    def stat_copy(d):
        return to_kv(6, d, st_send.at[d], st_recv.at[d], -1)

    def val_copy(d):
        return to_kv(7, d, val_send.at[d], val_recv.at[d], -1)

    def cand_copy(d):
        return to_kv(8, d, cand_send, cand_recv.at[d])

    def sq_copy(d):
        return pltpu.make_async_remote_copy(
            src_ref=sq_send,
            dst_ref=sq_recv.at[d],
            send_sem=qssem.at[d],
            recv_sem=qrsem.at[d],
            device_id=place(d),
            device_id_type=MESH,
        )

    def each(times, fn):
        def body(d, c):
            fn(d)
            return c

        lax.fori_loop(1, times, body, 0)

    nb = min(2 * prop, piece)
    mine = pl.ds(pl.multiple_of(me * kdim, kdim), kdim)
    ins[1].wait()

    def norm_rows(i, c):
        sl = pl.ds(pl.multiple_of(i * nb, nb), nb)
        t = tokv[sl, :].astype(F32)
        inv = lax.rsqrt(jnp.mean(t * t, axis=-1, keepdims=True) + epsilon)
        invs[sl, :] = jnp.broadcast_to(inv, (nb, 128))
        slab[sl, :] = (tokv[sl, mine].astype(F32) * inv * gain[:, mine]).astype(BF)
        return c

    for p in range(pieces):
        tok_in[p].wait()
        lax.fori_loop(p * piece // nb, (p + 1) * piece // nb, norm_rows, 0)
    for c in ins[5:]:
        c.start()
    local = slab[...]
    pl.semaphore_wait(barrier, count - 1)
    ins[2].wait()
    partq[...] = jnp.dot(local, wv3[0], preferred_element_type=F32).astype(BF)
    each(n, lambda d: rsq_copy(d).start())
    for i in range(2):
        ins[3 + i].wait()
        both_rows = jnp.dot(local, wv3[1 + i], preferred_element_type=F32).astype(BF)
        for c in range(n):
            part2[c % 2, c // 2, :, i * hw : (i + 1) * hw] = both_rows[c * R : (c + 1) * R]
    rs1_copy().start()

    def norm_rest(i, c):
        sl = pl.ds(pl.multiple_of(i * nb, nb), nb)
        inv = invs[sl, 0:1]
        normed[sl, :] = (tokv[sl, :].astype(F32) * inv * gain[...]).astype(BF)
        return c

    lax.fori_loop(0, rows // nb, norm_rest, 0)
    for c in ins[5:11]:
        c.wait()

    r64 = num_seqs * heads
    c64 = cum[...]
    srow = iota((r64, span), 0) // heads
    lane = iota((r64, span), 1)
    rel64 = jnp.zeros((r64, span), jnp.int32)
    rel16 = jnp.zeros((num_seqs, cols), jnp.int32)
    s16 = iota((num_seqs, cols), 0)
    for s in range(num_seqs):
        rel_s = lens[s] + accs[s] - base
        rel64 = jnp.where(srow == s, rel_s, rel64)
        rel16 = jnp.where(s16 == s, rel_s, rel16)
    cand = jnp.max(jnp.where(lane == rel64 - 1, c64, floor_value), axis=1, keepdims=True)
    diag = iota((r64, 128), 0) == iota((r64, 128), 1)
    cand_lane = jnp.sum(jnp.where(diag, cand, 0.0), axis=0, keepdims=True)
    cand_send[...] = jnp.broadcast_to(cand_lane, (8, 128))
    each(n, lambda d: cand_copy(d).start())

    spread = hot(iota((span, cols), 1) // heads == iota((span, cols), 0))
    e1 = dot_hi(c64, spread)
    e1 = jnp.where(iota((r64, cols), 0) % heads == iota((r64, cols), 1) % heads, e1, 0.0)
    take = hot(iota((num_seqs, r64), 1) // heads == iota((num_seqs, r64), 0))
    cflat = dot_hi(take, e1)
    brow[...] = jnp.where(iota((num_seqs, cols), 1) // heads < rel16, -cflat, floor_value)

    ri = iota((rows, rows), 0)
    ci = iota((rows, rows), 1)
    pick = hot(iota((rows, num_seqs), 0) // prop == iota((rows, num_seqs), 1))
    pb = dot_hi(pick, parent[...].astype(F32))
    pcol = jnp.sum(
        jnp.where(iota((rows, prop), 1) == iota((rows, prop), 0) % prop, pb, 0.0),
        axis=1,
        keepdims=True,
    )
    target = jnp.where(pcol >= 0.0, (ri // prop * prop).astype(F32) + pcol, -1.0)
    a = jnp.where((ri == ci) | (ci.astype(F32) == target), 1.0, 0.0)
    for sweep in range(max(1, (prop - 1).bit_length())):
        low = a.astype(BF)
        a = jnp.minimum(jnp.dot(low, low, preferred_element_type=F32), 1.0)
    anc[...] = a
    lf = lax.dot_general(wft[...], normed[...], NT, preferred_element_type=F32)
    bcol = jnp.zeros((heads_all, rows), F32)
    for h in range(heads_all):
        bcol = jnp.where(iota((heads_all, rows), 0) == h, bias[h], bcol)
    z = lf + bcol
    lf = jnp.minimum(z, 0.0) - jnp.log1p(jnp.exp(-jnp.abs(z)))
    path_t = dot_hi(lf, a, NT)
    rep = hot(iota((r64, heads_all), 1) == mt * heads + iota((r64, heads_all), 0) % heads)
    pm = dot_hi(rep, path_t)
    pm = jnp.where(iota((r64, rows), 1) // prop == iota((r64, rows), 0) // heads, pm, 0.0)
    fold = hot(iota((rows, 128), 0) % prop == iota((rows, 128), 1) % prop)
    pt = dot_hi(pm, fold)
    ptile[...] = pt
    ptm = jnp.where((iota((r64, 128), 1) // prop) % heads == iota((r64, 128), 0) % heads, pt, 0.0)
    tpath[...] = dot_hi(take, ptm)

    own_q = partq[rrow(me)].astype(F32)
    for d in range(1, n):
        rsq_copy(d).wait_recv()
        own_q = own_q + rsq[d].astype(F32)
    qall[rrow(me)] = own_q.astype(BF)
    gather_start(3, q_view)
    rs1_copy().wait_recv()
    for i in range(nh):
        half[i] = (part2[par, i].astype(F32) + rs1[i].astype(F32)).astype(BF)
    each(nh, lambda e: rs2_copy(e).start())

    ins[11].wait()
    ins[12].wait()
    same_head = iota((hp, cols), 0) // prop == iota((hp, cols), 1) % heads
    diag_l = iota((L, L), 0) == iota((L, L), 1)

    def heads_of(block):
        return jnp.concatenate([block[:, h * hd : (h + 1) * hd] for h in range(heads)], axis=0)

    def block_part(src):
        maxes, totals, values = [], [], []
        for j in range(sp):
            s = src * sp + j
            q = heads_of(qall[pl.ds(pl.multiple_of(s * prop, prop), prop), :])
            sc = lax.dot_general(q, kcv[s], NT, preferred_element_type=F32) * scale
            sc = jnp.where(same_head, sc + brow[pl.ds(s, 1), :], floor_value)
            m = jnp.max(sc, axis=1, keepdims=True)
            w = jnp.exp(sc - m)
            maxes.append(m)
            totals.append(jnp.sum(w, axis=1, keepdims=True))
            values.append(
                jnp.dot(w.astype(BF), vcv[s], preferred_element_type=F32).astype(BF)
            )
        m = jnp.concatenate(maxes, axis=0)
        t = jnp.concatenate(totals, axis=0)
        m_lane = jnp.sum(jnp.where(diag_l, m, 0.0), axis=0, keepdims=True)
        t_lane = jnp.sum(jnp.where(diag_l, t, 0.0), axis=0, keepdims=True)
        stats = jnp.where(iota((8, L), 0) == 0, m_lane, t_lane)
        return stats, jnp.concatenate(values, axis=0)

    def remote_block(d):
        src = down(d)
        stats, values = block_part(src)
        st_send[d] = stats
        val_send[d] = values
        stat_copy(d).start()
        val_copy(d).start()

    stats, values = block_part(me)
    st_recv[0] = stats
    val_recv[0] = values
    gather_pass(3, q_view)
    each(nh, lambda e: remote_block(2 * e))

    def mate_block(e, c):
        gather_wait(3, e, q_view)
        remote_block(lax.rem(me - mate_chunk(e) + n, n))
        return c

    lax.fori_loop(0, nh, mate_block, 0)
    own_kv = half[me // 2].astype(F32)
    for e in range(1, nh):
        rs2_copy(e).wait_recv()
        own_kv = own_kv + rs2[e].astype(F32)
    kvown[...] = own_kv.astype(BF)
    for i in range(2):
        for h in range(heads):
            flat[pl.ds(h, R, stride=heads), :] = own_kv[:, i * hw + h * hd : i * hw + (h + 1) * hd]
        kvflat[i, lrow(me)] = flat[...].astype(BF)
    gather_start(5, k_view)

    fold_h = iota((rows, hp), 0)
    tmax, ttot, tval = [], [], []
    for j in range(sp):
        s = me * sp + j
        q = heads_of(qall[pl.ds(pl.multiple_of(s * prop, prop), prop), :])
        k = heads_of(kvown[j * prop : (j + 1) * prop, 0:hw])
        v = heads_of(kvown[j * prop : (j + 1) * prop, hw : 2 * hw])
        arows = anc[pl.ds(pl.multiple_of(s * prop, prop), prop), :]
        sel = hot(fold_h == s * prop + iota((rows, hp), 1) % prop).astype(BF)
        am = jnp.dot(arows.astype(BF), sel, preferred_element_type=F32)
        am = jnp.concatenate([am] * heads, axis=0)
        mask = (am > 0.5) & (iota((hp, hp), 0) // prop == iota((hp, hp), 1) // prop)
        sc = lax.dot_general(q, k, NT, preferred_element_type=F32) * scale
        sc = jnp.where(mask, sc - tpath[pl.ds(s, 1), 0:hp], floor_value)
        m = jnp.max(sc, axis=1, keepdims=True)
        w = jnp.where(mask, jnp.exp(sc - m), 0.0)
        tmax.append(m)
        ttot.append(jnp.sum(w, axis=1, keepdims=True))
        tval.append(jnp.dot(w.astype(BF), v, preferred_element_type=F32))
    tree_max = jnp.concatenate(tmax, axis=0)
    tree_tot = jnp.concatenate(ttot, axis=0)
    tree_val = jnp.concatenate(tval, axis=0)

    last_lane = cand_send[...]
    for d in range(1, n):
        cand_copy(d).wait_recv()
        last_lane = jnp.maximum(last_lane, cand_recv[d])
    last_col = jnp.sum(jnp.where(diag, last_lane[0:1], 0.0), axis=1, keepdims=True)
    own_rows = iota((L, 128), 0)
    own_pick = iota((L, 128), 1) == (me * sp + own_rows // hp) * heads + (own_rows % hp) // prop
    last_own = jnp.sum(jnp.where(own_pick, last_lane[0:1], 0.0), axis=1, keepdims=True)

    shifted_path = ptile[...]
    for b in range((span - 1).bit_length()):
        moved = pltpu.roll(shifted_path, 1 << b, 1)
        shifted_path = jnp.where((rel64 >> b) & 1 == 1, moved, shifted_path)
    off = lane - rel64
    cum_out[...] = jnp.where((off >= 0) & (off < prop), last_col + shifted_path, cum[...])

    for d in range(1, n):
        stat_copy(d).wait_recv()
    top = st_recv[0]
    for d in range(1, n):
        top = jnp.maximum(top, st_recv[d])
    top = top[0:1]

    def col(x):
        return jnp.sum(jnp.where(diag_l, x, 0.0), axis=1, keepdims=True)

    cache_tot = jnp.zeros((1, L), F32)
    scales = []
    for d in range(n):
        sd = jnp.exp(st_recv[d, 0:1] - top)
        scales.append(col(sd))
        cache_tot = cache_tot + st_recv[d, 1:2] * sd
    shifted = col(top) + last_own
    both = jnp.maximum(shifted, tree_max)
    cscale = jnp.exp(shifted - both)
    tscale = jnp.exp(tree_max - both)
    denom = col(cache_tot) * cscale + tree_tot * tscale
    vals = jnp.zeros((L, hd), F32)
    for d in range(n):
        if d > 0:
            val_copy(d).wait_recv()
        vals = vals + val_recv[d].astype(F32) * scales[d]
    attended = ((vals * cscale + tree_val * tscale) / denom).astype(BF)
    for j in range(sp):
        for h in range(heads):
            att[pl.ds(pl.multiple_of(me * R + j * prop, prop), prop), h * hd : (h + 1) * hd] = (
                attended[j * hp + h * prop : j * hp + (h + 1) * prop]
            )
    gather_start(4, att_view)
    ins[13].wait()
    ins[14].wait()
    gather_pass(4, att_view)
    gather_start(11, v_view)
    gather_pass(5, k_view)
    for e in range(nh):
        gather_wait(4, e, att_view)
    full = jnp.dot(att[...], wov[...], preferred_element_type=F32).astype(BF)
    oc = o_send.shape[2]
    for t in range(nt):
        o_send[t] = full[:, t * oc : (t + 1) * oc]

    def o_copy(d):
        return to_tp(0, d, o_send.at[lax.rem(mt + d, nt)], o_recv.at[d])

    each(nt, lambda d: o_copy(d).start())
    gather_pass(11, v_view)
    mixed = o_send[mt].astype(F32)
    for d in range(1, nt):
        o_copy(d).wait_recv()
        mixed = mixed + o_recv[d].astype(F32)
    sq_send[...] = dot_hi(jnp.ones((8, oc), F32), mixed * mixed, NT)[0:1]
    each(count, lambda d: sq_copy(d).start())
    for e in range(nh):
        gather_wait(5, e, k_view)
        gather_wait(11, e, v_view)
    out_kv = pltpu.make_async_copy(kvflat, kv_out, loc.at[15])
    out_kv.start()
    each(count, lambda d: sq_copy(d).wait_recv())
    sq_recv[0] = sq_send[...]
    sq = jnp.sum(sq_recv[...], axis=0)
    ssum = dot_hi(jnp.broadcast_to(sq, (8, rows)), jnp.full((8, oc), 0.125, F32), (((0,), (0,)), ((), ())))
    mixed_out[...] = (mixed * lax.rsqrt(ssum / width + epsilon) * gpost[...]).astype(BF)

    def drain(d):
        rsq_copy(d).wait_send()
        stat_copy(d).wait_send()
        val_copy(d).wait_send()
        cand_copy(d).wait_send()

    each(n, drain)
    each(count, lambda d: sq_copy(d).wait_send())
    rs1_copy().wait_send()
    each(nh, lambda e: rs2_copy(e).wait_send())
    gather_drain(3, q_view)
    gather_drain(4, att_view)
    gather_drain(5, k_view)
    gather_drain(11, v_view)

    def drain_t(d):
        o_copy(d).wait_send()

    each(nt, drain_t)
    out_kv.wait()


def write_kernel(
    num_seqs,
    prop,
    span,
    kc,
    vc,
    kv_new,
    mixed,
    cum,
    lens_h,
    accs_h,
    k_out,
    v_out,
    mixed_out,
    cum_out,
    buf,
    fresh,
    lens,
    accs,
    sem,
    sin,
    sout,
):
    base = lax.axis_index("kv") * span
    small = [
        pltpu.make_async_copy(lens_h, lens, sem.at[0]),
        pltpu.make_async_copy(accs_h, accs, sem.at[1]),
        pltpu.make_async_copy(kv_new, fresh, sem.at[2]),
        pltpu.make_async_copy(mixed, mixed_out, sem.at[3]),
        pltpu.make_async_copy(cum, cum_out, sem.at[4]),
    ]
    cut = sin.shape[1]
    step = num_seqs // cut
    arrays = ((kc, k_out), (vc, v_out))

    def part(c):
        return pl.ds(c * step, step)

    def come(c, i):
        return pltpu.make_async_copy(arrays[i][0].at[part(c)], buf.at[i, part(c)], sin.at[i, c])

    def leave(c, i):
        return pltpu.make_async_copy(buf.at[i, part(c)], arrays[i][1].at[part(c)], sout.at[i, c])

    for c in small[:3]:
        c.start()
    for c in range(cut):
        for i in range(2):
            come(c, i).start()
    for c in small[3:]:
        c.start()
    for c in small[:3]:
        c.wait()

    def place(i, s):
        rel = lens[s] + accs[s] - base
        whole = (rel >= 0) & (rel <= span - prop)
        partly = (rel > -prop) & (rel < span) & jnp.logical_not(whole)

        @pl.when(whole)
        def _():
            buf[i, s, pl.ds(rel, prop)] = fresh[i, s]

        @pl.when(partly)
        def _():
            def one(j, c):
                buf[i, s, pl.ds(rel + j, 1)] = fresh[i, s, pl.ds(j, 1)]
                return c

            lax.fori_loop(jnp.maximum(-rel, 0), jnp.minimum(span - rel, prop), one, 0)

    for c in range(cut):
        for i in range(2):
            come(c, i).wait()
            for s in range(c * step, (c + 1) * step):
                place(i, s)
            leave(c, i).start()
    for c in range(cut):
        for i in range(2):
            leave(c, i).wait()
    for c in small[3:]:
        c.wait()


def fast_device(
    n,
    nt,
    tokens,
    gain_pre,
    w_query,
    w_key,
    w_value,
    w_forget,
    b_forget,
    w_out,
    gain_post,
    key_cache,
    value_cache,
    cum_cache,
    lengths,
    accepted,
    parent,
):
    num_seqs, prop, width = tokens.shape
    span, heads, hd = key_cache.shape[1:]
    rows = num_seqs * prop
    hw = heads * hd
    cols = heads * span
    sp = num_seqs // n
    R = sp * prop
    L = sp * heads * prop
    oc = gain_post.shape[0]
    kc = key_cache.reshape(num_seqs, cols, hd)
    vc = value_cache.reshape(num_seqs, cols, hd)
    cum = jnp.swapaxes(cum_cache, 1, 2).reshape(num_seqs * heads, span)
    vmem = pl.BlockSpec(memory_space=pltpu.VMEM)
    V = pltpu.VMEM
    D = pltpu.SemaphoreType.DMA
    hbm = pl.BlockSpec(memory_space=pltpu.HBM)
    S = pltpu.SMEM
    nh = n // 2
    mixed, kv_new, cum_new = pl.pallas_call(
        functools.partial(layer_kernel, n, nt, num_seqs, prop, heads, hd, span),
        out_shape=(
            jax.ShapeDtypeStruct((rows, oc), BF),
            jax.ShapeDtypeStruct((2, rows * heads, hd), BF),
            jax.ShapeDtypeStruct(cum.shape, F32),
        ),
        in_specs=[hbm] * 15,
        out_specs=(vmem, hbm, vmem),
        scratch_shapes=[
            V((rows, width), BF),
            V((rows, width), BF),
            V((rows, w_query.shape[0]), BF),
            V((rows, 128), F32),
            V((1, width), F32),
            V((3,) + w_query.shape, BF),
            V(w_forget.T.shape, BF),
            V(w_out.shape, BF),
            V((1, oc), F32),
            V(kc.shape, BF),
            V(vc.shape, BF),
            V(cum.shape, F32),
            V(parent.shape, jnp.int32),
            S(b_forget.shape, F32),
            S(lengths.shape, jnp.int32),
            S(accepted.shape, jnp.int32),
            V((rows, hw), BF),
            V((n, R, hw), BF),
            V((2, nh, R, 2 * hw), BF),
            V((nh, R, 2 * hw), BF),
            V((nh, R, 2 * hw), BF),
            V((nh, R, 2 * hw), BF),
            V((R, 2 * hw), BF),
            V((L, hd), F32),
            V((2, rows * heads, hd), BF),
            V((rows, hw), BF),
            V((n, 8, L), F32),
            V((n, L, hd), BF),
            V((n, 8, L), F32),
            V((n, L, hd), BF),
            V((8, 128), F32),
            V((n, 8, 128), F32),
            V((num_seqs, cols), F32),
            V((rows, rows), F32),
            V((num_seqs, 128), F32),
            V((num_seqs * heads, 128), F32),
            V((rows, hw), BF),
            V((nt, rows, oc), BF),
            V((nt, rows, oc), BF),
            V((1, rows), F32),
            V((n * nt, 1, rows), F32),
            D((20,)),
            D((12, n)),
            D((12, n)),
            D((1, nt)),
            D((1, nt)),
            D((n * nt,)),
            D((n * nt,)),
        ],
        compiler_params=pltpu.CompilerParams(
            collective_id=0, has_side_effects=True, vmem_limit_bytes=67043328
        ),
        name="layer",
    )(
        tokens.reshape(rows, width),
        gain_pre.reshape(1, width),
        w_query,
        w_key,
        w_value,
        w_forget.T,
        b_forget,
        w_out,
        gain_post.reshape(1, oc),
        kc,
        vc,
        cum,
        lengths,
        accepted,
        parent,
    )
    key_out, value_out, mixed, cum_new = pl.pallas_call(
        functools.partial(write_kernel, num_seqs, prop, span),
        out_shape=(
            jax.ShapeDtypeStruct(key_cache.shape, BF),
            jax.ShapeDtypeStruct(value_cache.shape, BF),
            jax.ShapeDtypeStruct(mixed.shape, BF),
            jax.ShapeDtypeStruct(cum_new.shape, F32),
        ),
        in_specs=[hbm] * 7,
        out_specs=(hbm,) * 4,
        scratch_shapes=[
            V((2,) + key_cache.shape, BF),
            V((2, num_seqs, prop, heads, hd), BF),
            S(lengths.shape, jnp.int32),
            S(accepted.shape, jnp.int32),
            D((5,)),
            D((2, 4)),
            D((2, 4)),
        ],
        compiler_params=pltpu.CompilerParams(vmem_limit_bytes=67043328),
        name="cache_write",
    )(
        key_cache,
        value_cache,
        kv_new.reshape(2, num_seqs, prop, heads, hd),
        mixed,
        cum_new,
        lengths,
        accepted,
    )
    cum_out = jnp.swapaxes(cum_new.reshape(num_seqs, heads, span), 1, 2)
    return (
        mixed.reshape(num_seqs, prop, oc),
        key_out,
        value_out,
        cum_out,
    )


def choose(mesh):
    n, nt = mesh.shape["kv"], mesh.shape["tp"]

    def body(*args):
        tokens, key_cache = args[0], args[9]
        num_seqs, prop = tokens.shape[:2]
        span, heads = key_cache.shape[1:3]
        fits = (
            num_seqs % n == 0
            and n % 2 == 0
            and num_seqs % 4 == 0
            and (num_seqs // n) * heads * prop == 128
            and span == 128
            and num_seqs * heads <= 128
            and prop % 16 == 0
        )
        if fits:
            return fast_device(n, nt, *args)
        return per_device(*args)

    return body


def solution(mesh):
    return jax.shard_map(
        choose(mesh),
        mesh=mesh,
        in_specs=(
            P(),
            P(),
            P("kv", "tp"),
            P("kv", "tp"),
            P("kv", "tp"),
            P(),
            P(),
            P("tp", "kv"),
            P(("kv", "tp")),
            P(None, "kv", "tp", None),
            P(None, "kv", "tp", None),
            P(None, "kv", "tp"),
            P(),
            P(),
            P(),
        ),
        out_specs=(
            P(None, None, ("kv", "tp")),
            P(None, "kv", "tp", None),
            P(None, "kv", "tp", None),
            P(None, "kv", "tp"),
        ),
        check_vma=False,
    )
```
